32 devices in a mesh: sp: 8 (over z, y), dp: 4 (over x, core).
Axes of the slice: x: 2, y: 2, z: 4, core: 2. Of those that a mesh axis runs over, the one named last changes fastest.
Arguments:
- queries: bfloat16 [4, 2048, 1280], P('dp', None, 'sp'), may hold values from -6 to 6
- keys: bfloat16 [4, 1024, 1280], P('dp', None, 'sp'), may hold values from -6 to 6
- values: bfloat16 [4, 1024, 1280], P('dp', None, 'sp'), may hold values from -48 to 48
- q_gain: float32 [64], replicated, may hold values from 0.5 to 10
- k_gain: float32 [64], replicated, may hold values from 0.5 to 10
- w_out: bfloat16 [2048, 2048], P(None, 'dp'), may hold values from -0.125 to 0.125
Outputs:
- mixed: bfloat16 [4, 1280, 2048], P('dp', 'sp')
The draws below stay inside these ranges and needn't reach their ends.
All inputs are finite; a program needn't handle non-finite values.
Results may differ from the reference program's by a relative error of at most 0.0038.
The reference program's roundings to bfloat16 on the way count: a program that leaves them out, or rounds other values in their place, can miss the bound.
Values may be sent and summed in bfloat16 or wider, within the bound.
A program may use at most 64 MiB of HBM per device.

```python
import jax
import jax.numpy as jnp
from jax import lax

HD = 64
QH = 32
KV = 16
D = 2048
GRID_W = 64
QW = 2048
KVW = 1024
TOKENS = 1280
SEQ_GROUPS = 4


def shared_keys(key):
    key_draw = jax.random.normal(jax.random.fold_in(key, 11), (SEQ_GROUPS, KVW, TOKENS), jnp.float32)
    return jnp.clip(key_draw, -6.0, 6.0)


def draw_keys(key, part):
    return shared_keys(key).astype(jnp.bfloat16)


def draw_queries(key, part):
    fresh_draw = jax.random.normal(jax.random.fold_in(key, 12), (SEQ_GROUPS, QW, TOKENS), jnp.float32)
    fresh_draw = jnp.clip(fresh_draw, -6.0, 6.0)
    return fresh_draw.astype(jnp.bfloat16)


def gain_draw(key, salt):
    noise_draw = jnp.clip(jax.random.normal(jax.random.fold_in(key, salt), (HD,), jnp.float32), -3.0, 3.0)
    return 1.25 * (1.0 + 0.18 * noise_draw)


def draw_q_gain(key, part):
    return gain_draw(key, 21)


def draw_k_gain(key, part):
    return gain_draw(key, 22)


def steps_of(rng, dims, split, least, top_value):
    level = 1.0
    for axis_at, parts in split:
        draws = jax.random.uniform(jax.random.fold_in(jax.random.fold_in(rng, 6), axis_at), (parts,), jnp.float32, least / len(split), top_value / len(split))
        level = level * jnp.repeat(jnp.exp(draws), dims[axis_at] // parts).reshape((-1,) + (1,) * (len(dims) - 1 - axis_at))
    return level


def noise(rng, shape, spread, reach, split=(), held_as=jnp.bfloat16):
    result = jax.random.normal(rng, shape, jnp.float32) * spread
    if len(split) > 0:
        result = steps_of(rng, shape, split, -0.22, 0.18) * result
    return jnp.clip(result, min=-reach, max=reach).astype(held_as)


def setup_inputs(seed: int = 0) -> dict:
    key_list = jax.random.split(jax.random.key(seed), 7)
    queries = draw_queries(jax.random.fold_in(key_list[6], 71), 0)
    keys = draw_keys(jax.random.fold_in(key_list[6], 71), 0)
    values = noise(key_list[2], (SEQ_GROUPS, KVW, TOKENS), 8.0, 48.0, ((0, 4), (2, 8)))
    q_gain = draw_q_gain(jax.random.fold_in(key_list[6], 71), 0)
    k_gain = draw_k_gain(jax.random.fold_in(key_list[6], 71), 0)
    w_out = noise(key_list[5], (QW, D), QW ** -0.5, 0.125, ((1, 4),))
    return dict(queries=queries, keys=keys, values=values, q_gain=q_gain, k_gain=k_gain, w_out=w_out)


epsilon = 1e-06
rotary_base = 10000.0

def rotary_tables(row_count):
    position = jnp.arange(row_count, dtype=jnp.int32)
    grid_row = (position // GRID_W).astype(jnp.float32)
    grid_col = (position % GRID_W).astype(jnp.float32)
    quarter = HD // 4
    inv_freq = rotary_base ** (-(2.0 * jnp.arange(quarter, dtype=jnp.float32)) / (HD // 2))
    row_angle = inv_freq[:, None] * grid_row[None, :]
    col_angle = inv_freq[:, None] * grid_col[None, :]
    cos_table = jnp.concatenate([jnp.cos(row_angle), jnp.cos(row_angle), jnp.cos(col_angle), jnp.cos(col_angle)], axis=0)
    sin_table = jnp.concatenate([jnp.sin(row_angle), jnp.sin(row_angle), jnp.sin(col_angle), jnp.sin(col_angle)], axis=0)
    return (cos_table, sin_table)

def normalize_turn(field, gain, cos_table, sin_table):
    head_count = field.shape[0] // HD
    values_f = field.astype(jnp.float32).reshape(head_count, HD, field.shape[1])
    normed = values_f * lax.rsqrt(lax.optimization_barrier(jnp.mean(values_f * values_f, axis=1, keepdims=True)) + epsilon) * gain[None, :, None]
    quarter = HD // 4
    quarters_of = normed.reshape(head_count, 4, quarter, field.shape[1])
    turned = jnp.concatenate([-quarters_of[:, 1], quarters_of[:, 0], -quarters_of[:, 3], quarters_of[:, 2]], axis=1)
    return (normed * cos_table[None] + turned * sin_table[None]).astype(jnp.bfloat16)

def reference(queries, keys, values, q_gain, k_gain, w_out):
    cos_table, sin_table = rotary_tables(TOKENS)
    group_size = QH // KV
    score_scale = HD ** (-0.5)

    def per_group(packed):
        query_rows, key_rows, value_rows = packed
        query_rot = normalize_turn(query_rows, q_gain, cos_table, sin_table)
        key_rot = normalize_turn(key_rows, k_gain, cos_table, sin_table)
        value_heads = value_rows.reshape(KV, HD, TOKENS)

        def per_head(head_index):
            query_one = lax.dynamic_index_in_dim(query_rot, head_index, 0, keepdims=False)
            key_one = lax.dynamic_index_in_dim(key_rot, head_index // group_size, 0, keepdims=False)
            value_one = lax.dynamic_index_in_dim(value_heads, head_index // group_size, 0, keepdims=False)
            scores = jnp.einsum('dq,dk->qk', query_one.astype(jnp.float32), key_one.astype(jnp.float32)) * score_scale
            row_max = lax.optimization_barrier(jnp.max(scores, axis=-1, keepdims=True))
            weights = jnp.exp(scores - row_max)
            weights = (weights / lax.optimization_barrier(jnp.sum(weights, axis=-1, keepdims=True))).astype(jnp.bfloat16)
            attended = jnp.einsum('qk,dk->dq', weights.astype(jnp.float32), value_one.astype(jnp.float32))
            return attended.astype(jnp.bfloat16)
        attended = lax.map(per_head, jnp.arange(QH, dtype=jnp.int32)).reshape(QW, TOKENS)
        return jnp.dot(attended.T, w_out, preferred_element_type=jnp.float32).astype(jnp.bfloat16)
    return lax.map(per_group, (queries, keys, values))
```

```python
import functools

import jax
import jax.numpy as jnp
import numpy as np
from jax import lax
from jax.experimental import pallas as pl
from jax.experimental.pallas import tpu as pltpu
from jax.sharding import PartitionSpec as P

HD = 64
QH = 32
KV = 16
GRID_W = 64


epsilon = 1e-06
rotary_base = 10000.0
block_count = 8


def swapped(block, axis, apart):
    count = lax.axis_size(axis)
    route = []
    for low in range(count):
        high = low | 1 << apart
        if high != low and high < count:
            route += [(low, high), (high, low)]
    return lax.ppermute(block, axis, route)


def rotary_tables(first_row, row_count):
    position = first_row + lax.iota(jnp.int32, row_count)
    grid_row = (position // GRID_W).astype(jnp.float32)
    grid_col = (position % GRID_W).astype(jnp.float32)
    quarter = HD // 4
    inv_freq = rotary_base ** (-(2.0 * lax.iota(jnp.float32, quarter)) / (HD // 2))
    row_angle = inv_freq[:, None] * grid_row[None, :]
    col_angle = inv_freq[:, None] * grid_col[None, :]
    cos_table = jnp.concatenate(
        [jnp.cos(row_angle), jnp.cos(row_angle), jnp.cos(col_angle), jnp.cos(col_angle)], axis=0
    )
    sin_table = jnp.concatenate(
        [jnp.sin(row_angle), jnp.sin(row_angle), jnp.sin(col_angle), jnp.sin(col_angle)], axis=0
    )
    return (cos_table, sin_table)


def normalize_turn(field, gain, cos_table, sin_table):
    head_count = field.shape[0] // HD
    values_f = field.astype(jnp.float32).reshape(head_count, HD, field.shape[1])
    normed = (
        values_f
        * lax.rsqrt(jnp.mean(values_f * values_f, axis=1, keepdims=True) + epsilon)
        * gain[None, :, None]
    )
    quarter = HD // 4
    quarters_of = normed.reshape(head_count, 4, quarter, field.shape[1])
    turned = jnp.concatenate(
        [-quarters_of[:, 1], quarters_of[:, 0], -quarters_of[:, 3], quarters_of[:, 2]], axis=1
    )
    return (normed * cos_table[None] + turned * sin_table[None]).astype(jnp.bfloat16)


def attention_heads(query_heads, key_heads, value_heads, seq_len):
    kv_local = key_heads.shape[0]
    group_local = query_heads.shape[0] // kv_local
    query_split = query_heads.reshape(kv_local, group_local, HD, seq_len)
    score_scale = HD ** (-0.5)
    block_rows = seq_len // block_count

    def one_block(block_index, result):
        row_start = block_index * block_rows
        query_block = lax.dynamic_slice_in_dim(query_split, row_start, block_rows, 3)
        scores = (
            jnp.einsum("hgdq,hdk->hgqk", query_block, key_heads, preferred_element_type=jnp.float32)
            * score_scale
        )
        row_max = jnp.max(scores, axis=-1, keepdims=True)
        weights = jnp.exp(scores - row_max)
        weights = (weights / jnp.sum(weights, axis=-1, keepdims=True)).astype(jnp.bfloat16)
        attended = jnp.einsum(
            "hgqk,hdk->hgdq", weights, value_heads, preferred_element_type=jnp.float32
        )
        return lax.dynamic_update_slice_in_dim(result, attended.astype(jnp.bfloat16), row_start, 3)

    result = jnp.zeros(query_split.shape, jnp.bfloat16)
    result = lax.fori_loop(0, block_count, one_block, result)
    return result.reshape(query_heads.shape)


def on_device_plain(queries, keys, values, q_gain, k_gain, w_out):
    sp_count = lax.axis_size("sp")
    tok_rows = queries.shape[2]
    seq_len = tok_rows * sp_count
    cos_table, sin_table = rotary_tables(lax.axis_index("sp") * tok_rows, tok_rows)
    query_rot = normalize_turn(queries[0], q_gain, cos_table, sin_table)
    key_rot = normalize_turn(keys[0], k_gain, cos_table, sin_table)
    value_rows = values[0].reshape(KV, HD, tok_rows)
    query_heads = lax.all_to_all(query_rot, "sp", split_axis=0, concat_axis=2, tiled=True)
    share_count = max(sp_count // KV, 1)
    part_rows = tok_rows // share_count
    key_cut = (
        key_rot.reshape(KV, HD, share_count, part_rows)
        .transpose(0, 2, 1, 3)
        .reshape(KV * share_count, HD, part_rows)
    )
    value_cut = (
        value_rows.reshape(KV, HD, share_count, part_rows)
        .transpose(0, 2, 1, 3)
        .reshape(KV * share_count, HD, part_rows)
    )
    key_got, value_got = (
        lax.all_to_all(key_cut, "sp", split_axis=0, concat_axis=2, tiled=True),
        lax.all_to_all(value_cut, "sp", split_axis=0, concat_axis=2, tiled=True),
    )
    kv_local = key_got.shape[0]
    key_got = key_got.reshape(kv_local, HD, sp_count, part_rows)
    value_got = value_got.reshape(kv_local, HD, sp_count, part_rows)
    for bit_index in range(share_count.bit_length() - 1):
        key_other, value_other = swapped((key_got, value_got), "sp", bit_index)
        key_got = jnp.concatenate([key_got, key_other], axis=3)
        value_got = jnp.concatenate([value_got, value_other], axis=3)
    key_heads = key_got.reshape(kv_local, HD, seq_len)
    value_heads = value_got.reshape(kv_local, HD, seq_len)
    attended = attention_heads(query_heads, key_heads, value_heads, seq_len)
    token_heads = lax.all_to_all(attended, "sp", split_axis=2, concat_axis=0, tiled=True)
    token_rows = token_heads.reshape(QH * HD, tok_rows)
    product = lax.dot_general(
        token_rows,
        lax.all_gather(w_out, "dp", axis=1, tiled=True),
        (((0,), (0,)), ((), ())),
        preferred_element_type=jnp.float32,
    )
    mixed_rows = product.astype(jnp.bfloat16)
    return mixed_rows[None]


MESH = pl.DeviceIdType.MESH
LOG2E = 1.4426950408889634
LANES = 128
TRANSPOSED = (((1,), (1,)), ((), ()))


def layer_kernel(
    m, q_ref, k_ref, v_ref, qg_ref, kg_ref, cos_ref, sin_ref, w_ref, out_ref,
    q_raw, k_raw, q_gain_in, k_gain_in, cos_in, sin_in, k_out, q_out, kv_in, q_in, a_out, a_in,
    w_all, score, peak, inv_sum,
    load, v_own, k_side, v_side, q_side, k_got, v_got, q_got, kv_up, q_up, kv_mid, kv_got,
    a_send, a_got, w_x, w_y, w_core, w_got, w_local,
):
    me = lax.axis_index("sp")
    dp = lax.axis_index("dp")
    z, y = me // 2, me % 2
    half = z // 2
    z_in, z_out = 1 + half, 3 * half
    inner = z == z_in
    outer = jnp.logical_not(inner)
    base = jnp.where(inner, 0, 2)
    mine, beside = base + y, base + 1 - y
    sibling = z * 2 + 1 - y
    in_same = z_in * 2 + y
    across = (3 - z_in) * 2 + y
    core = lax.rem(dp, 2)
    x_at = dp // 2
    x_peer = (1 - x_at) * 2 + core
    core_peer = x_at * 2 + 1 - core
    x_other = (1 - x_at) * 2 + 1 - core
    rows = k_raw.shape[0]
    pairs = kv_in.shape[0]
    parts = 2 * pairs
    w_rows = w_ref.shape[0] // parts

    barrier = pltpu.get_barrier_semaphore()

    def greet(**there):
        pl.semaphore_signal(barrier, inc=1, device_id=there, device_id_type=MESH)

    greet(sp=sibling)
    greet(dp=x_peer)
    greet(dp=core_peer)
    z_other = jnp.where(inner, z_out, z_in)
    greet(sp=z_other * 2 + y)
    greet(sp=z_other * 2 + 1 - y)

    @pl.when(inner)
    def _():
        greet(sp=across)

    def kv_lanes(side, j):
        return pl.ds(pl.multiple_of((side * pairs + j) * LANES, LANES), LANES)

    first = pl.multiple_of(me * rows, rows)
    loads = [
        pltpu.make_async_copy(k_ref, k_raw, load.at[0]),
        pltpu.make_async_copy(cos_ref.at[pl.ds(first, rows)], cos_in, load.at[1]),
        pltpu.make_async_copy(sin_ref.at[pl.ds(first, rows)], sin_in, load.at[2]),
        pltpu.make_async_copy(kg_ref, k_gain_in, load.at[3]),
        pltpu.make_async_copy(qg_ref, q_gain_in, load.at[4]),
        pltpu.make_async_copy(q_ref, q_raw, load.at[5]),
    ]
    for one in loads:
        one.start()

    def own_values(j):
        return pltpu.make_async_copy(
            v_ref.at[:, kv_lanes(y, j)], kv_in.at[j, mine, 1], v_own.at[j]
        )

    for j in range(pairs):
        own_values(j).start()
    own_w = pltpu.make_async_copy(w_ref, w_all.at[dp], w_local)
    own_w.start()

    def remote(src, dst, sent, got, **there):
        return pltpu.make_async_remote_copy(
            src_ref=src, dst_ref=dst, send_sem=sent, recv_sem=got,
            device_id=there, device_id_type=MESH,
        )

    def k_aside(j, to=None):
        to = mine if to is None else to
        return remote(k_out.at[j], kv_in.at[j, to, 0], k_side.at[j], k_got.at[j], sp=sibling)

    def v_aside(j, to=None):
        to = mine if to is None else to
        return remote(
            v_ref.at[:, kv_lanes(1 - y, j)], kv_in.at[j, to, 1], v_side.at[j], v_got.at[j],
            sp=sibling,
        )

    def q_aside(j, to=None):
        to = mine if to is None else to
        return remote(q_out.at[j], q_in.at[j, to], q_side.at[j], q_got.at[j, to], sp=sibling)

    def kv_upward(j, s):
        return remote(
            kv_in.at[j, s], kv_in.at[j, s], kv_up.at[j, s], kv_got.at[j, s], sp=in_same
        )

    def q_upward(j, s):
        return remote(q_in.at[j, s], q_in.at[j, s], q_up.at[j, s], q_got.at[j, s], sp=in_same)

    def kv_across(j, s):
        return remote(
            kv_in.at[j, s], kv_in.at[j, 4 + s], kv_mid.at[j, s], kv_got.at[j, 4 + s], sp=across
        )

    def kv_came(j, s):
        remote(
            kv_in.at[j, s], kv_in.at[j, s], kv_up.at[j, 0], kv_got.at[j, s], sp=across
        ).wait_recv()

    def q_came(j, s):
        remote(q_in.at[j, s], q_in.at[j, s], q_up.at[j, 0], q_got.at[j, s], sp=sibling).wait_recv()

    def w_piece(ref, c):
        return ref.at[pl.ds(pl.multiple_of(c * w_rows, w_rows), w_rows)]

    def w_held(shard, c):
        return w_all.at[shard, pl.ds(pl.multiple_of(c * w_rows, w_rows), w_rows)]

    direct = parts - 2

    def part_at(i):
        if i < 2:
            return y * pairs + i
        return (i % 2) * pairs + 1 + i // 2

    def w_cross(i):
        c = part_at(i)
        return remote(w_piece(w_ref, c), w_held(dp, c), w_x.at[i], w_got.at[dp, c], dp=x_peer)

    def w_own_core():
        return remote(w_ref, w_all.at[dp], w_core.at[parts], w_got.at[dp, parts], dp=core_peer)

    def w_to_core(c):
        return remote(
            w_held(x_peer, c), w_held(x_peer, c), w_core.at[c], w_got.at[x_peer, c], dp=core_peer
        )

    def w_aside(i):
        c = part_at(i)
        return remote(
            w_held(x_peer, c), w_held(x_peer, c), w_y.at[i], w_got.at[x_peer, c], sp=sibling
        )

    def w_came(shard, c):
        remote(
            w_held(shard, c), w_held(shard, c), w_y.at[0], w_got.at[shard, c], dp=core_peer
        ).wait_recv()

    def pass_w(i):
        c = part_at(i)
        w_came(x_peer, c)
        w_to_core(c).start()
        if i < 2:
            w_aside(i).start()

    def pass_w_aside(i):
        c = (1 - y) * pairs + i
        w_came(x_peer, c)
        w_to_core(c).start()

    lane = lax.broadcasted_iota(jnp.int32, (rows, LANES), 1)
    low = lane < HD
    even = (lane // (HD // 4)) % 2 == 0

    def turn(tile, gain):
        u = tile.astype(jnp.float32)
        square = u * u
        sum_low = jnp.sum(jnp.where(low, square, 0.0), axis=1, keepdims=True)
        sum_high = jnp.sum(jnp.where(low, 0.0, square), axis=1, keepdims=True)
        inverse = jnp.where(
            low, lax.rsqrt(sum_low * (1.0 / HD) + epsilon), lax.rsqrt(sum_high * (1.0 / HD) + epsilon)
        )
        normed = u * inverse * gain
        part = HD // 4
        turned = jnp.where(even, pltpu.roll(normed, LANES - part, 1), pltpu.roll(normed, part, 1))
        return normed * cos_in[...] + turned * sin_in[...]

    def crossed(one, two):
        return (
            jnp.where(low, one, pltpu.roll(two, HD, 1)),
            jnp.where(low, pltpu.roll(one, HD, 1), two),
        )

    def turn_keys(j, side):
        return turn(k_raw[:, kv_lanes(side, j)], k_gain).astype(jnp.bfloat16)

    def turn_queries(j, side):
        at = (side * pairs + j) * 2 * LANES
        natural = [
            turn(q_raw[:, pl.ds(pl.multiple_of(at + i * LANES, LANES), LANES)], q_gain)
            for i in range(2)
        ]
        return jnp.concatenate(crossed(*natural), axis=1).astype(jnp.bfloat16)

    for one in loads[:5]:
        one.wait()
    q_gain, k_gain = (
        jnp.concatenate([g[...], g[...]], axis=1) for g in (q_gain_in, k_gain_in)
    )

    def key_step(j):
        k_out[j] = turn_keys(j, 1 - y)
        kv_in[j, mine, 0] = turn_keys(j, y)

    def query_step(j):
        q_out[j] = turn_queries(j, 1 - y)
        q_in[j, mine] = turn_queries(j, y)

    key_step(0)
    pl.semaphore_wait(barrier, jnp.where(inner, 6, 5))
    loads[5].wait()

    def send_step(j, carry):
        v_aside(j).start()

        @pl.when(j > 0)
        def _():
            key_step(j)

        k_aside(j).start()
        own_values(j).wait()

        @pl.when(jnp.logical_and(outer, j == 0))
        def _():
            kv_upward(j, mine).start()

        @pl.when(jnp.logical_and(inner, j < 2))
        def _():
            kv_across(j, mine).start()

        query_step(j)
        q_aside(j).start()

        @pl.when(jnp.logical_and(outer, j == 0))
        def _():
            q_upward(j, mine).start()

        return carry

    w_cross(0).start()
    w_cross(1).start()
    lax.fori_loop(0, pairs, send_step, 0)
    for i in range(2, direct):
        w_cross(i).start()
    w_own_core().start()

    def beside_came(j):
        k_aside(j, beside).wait_recv()
        v_aside(j, beside).wait_recv()

    @pl.when(outer)
    def _():
        def kv(j):
            if j:
                kv_upward(j, mine).start()
            beside_came(j)
            kv_upward(j, beside).start()

        def query(j):
            if j:
                q_upward(j, mine).start()
            q_came(j, beside)
            q_upward(j, beside).start()

        kv(0)
        query(0)
        for j in range(1, pairs):
            kv(j)
            if j > 1:
                query(j - 1)
        query(pairs - 1)
        for i in range(direct):
            pass_w(i)
            if i in (2, 3):
                pass_w_aside(i - 2)

    scale = HD ** (-0.5) * LOG2E
    step = 2 * LANES
    seq_len = 8 * rows
    tiles = [(t, min(step, seq_len - t)) for t in range(0, seq_len, step)]

    def halves(tile, op):
        parts_of = [tile[:, i : i + LANES] for i in range(0, tile.shape[1], LANES)]
        return functools.reduce(op, parts_of)

    def wide(column, size):
        return jnp.concatenate([column] * (size // LANES), axis=1)

    def multiply_scores(j, s, at):
        stack = []
        for g in range(2):
            pair = q_in[j, s, :, g * LANES : (g + 1) * LANES]
            zero = jnp.zeros_like(pair)
            stack += [jnp.where(low, pair, zero), jnp.where(low, zero, pair)]
        stack = jnp.concatenate(stack, axis=0)
        keys = kv_in[j, :, 0].reshape(seq_len, LANES)
        top = None
        for t, size in tiles:
            tile = lax.dot_general(
                stack, keys[t : t + size], TRANSPOSED, preferred_element_type=jnp.float32
            )
            score[at, :, t : t + size] = tile
            most = halves(tile, jnp.maximum)
            top = most if top is None else jnp.maximum(top, most)
        peak[at] = jnp.broadcast_to(jnp.max(top, axis=1, keepdims=True), top.shape)

    def exponents(at):
        top = peak[at]
        total = None
        for t, size in tiles:
            p = jnp.exp2((score[at, :, t : t + size] - wide(top, size)) * scale)
            score[at, :, t : t + size] = p
            more = halves(p, jnp.add)
            total = more if total is None else total + more
        inv_sum[at] = jnp.broadcast_to(1.0 / jnp.sum(total, axis=1, keepdims=True), total.shape)

    def weigh(j, at):
        inv = inv_sum[at]
        p = jnp.concatenate(
            [
                (score[at, :, t : t + size] * wide(inv, size)).astype(jnp.bfloat16)
                for t, size in tiles
            ],
            axis=1,
        )
        vals = kv_in[j, :, 1].reshape(seq_len, LANES)
        o = jnp.dot(p, vals, preferred_element_type=jnp.float32)
        cut = [o[i * rows : (i + 1) * rows] for i in range(4)]
        mixed = [jnp.where(low, cut[2 * g], cut[2 * g + 1]) for g in range(2)]
        return jnp.concatenate(crossed(*mixed), axis=1).astype(jnp.bfloat16)

    def a_copy(j, s):
        there = jnp.where(s < 2, z_in, z_out) * 2 + s % 2
        c = y * pairs + j
        return remote(a_out.at[j, s], a_in.at[c], a_send.at[j, s], a_got.at[c], sp=there)

    def relay_first(j):
        beside_came(j)
        kv_across(j, beside).start()
        kv_came(j, 2 + y)
        kv_across(j, 2 + y).start()

    def relay_last(j):
        kv_came(j, 3 - y)
        kv_across(j, 3 - y).start()

        @pl.when(j + 2 < pairs)
        def _():
            kv_across(j + 2, mine).start()

    @pl.when(inner)
    def _():
        relay_first(0)
        relay_last(0)

        def attend(j, carry):
            more = j + 1 < pairs

            @pl.when(more)
            def _():
                relay_first(j + 1)

            for i in range(pairs):
                @pl.when(j == i)
                def _():
                    pass_w(i)
                    if i >= 2:
                        pass_w_aside(i - 2)

            q_came(j, 1 - y)
            q_came(j, 2)
            q_came(j, 3)
            for s in range(4, 8):
                kv_came(j, s)
            order = [2, 3, 1 - y, y]
            multiply_scores(j, order[0], 0)
            for u in range(4):
                if u == 2:
                    @pl.when(more)
                    def _():
                        relay_last(j + 1)

                if u < 3:
                    multiply_scores(j, order[u + 1], (u + 1) % 2)
                exponents(u % 2)
                tile = weigh(j, u % 2)
                if u < 3:
                    a_out[j, order[u]] = tile
                    a_copy(j, order[u]).start()
                else:
                    a_in[y * pairs + j] = tile
            return carry

        lax.fori_loop(0, pairs, attend, 0)
        for i in range(pairs, direct):
            pass_w(i)

    own_w.wait()
    remote(w_ref, w_all.at[core_peer], w_core.at[parts], w_got.at[core_peer, parts], dp=core_peer).wait_recv()

    def a_came(c):
        remote(a_in.at[c], a_in.at[c], a_send.at[0, 0], a_got.at[c], sp=sibling).wait_recv()

    for j in range(pairs):
        a_came((1 - y) * pairs + j)

        @pl.when(outer)
        def _():
            a_came(y * pairs + j)

    for c in range(parts):
        w_came(x_other, c)
    width = w_ref.shape[1]

    def product(shard):
        total = jnp.zeros((rows, width), jnp.float32)
        for c in range(parts):
            total += jnp.dot(
                a_in[c], w_all[shard, c * w_rows : (c + 1) * w_rows, :],
                preferred_element_type=jnp.float32,
            )
        out_ref[:, pl.ds(pl.multiple_of(shard * width, width), width)] = total.astype(jnp.bfloat16)

    for shard in range(m):
        product(shard)

    def sent(j, carry):
        k_aside(j).wait_send()
        v_aside(j).wait_send()
        q_aside(j).wait_send()

        @pl.when(outer)
        def _():
            for s in (mine, beside):
                kv_upward(j, s).wait_send()
                q_upward(j, s).wait_send()

        @pl.when(inner)
        def _():
            for s in range(4):
                kv_across(j, s).wait_send()
            for s in (1 - y, 2, 3):
                a_copy(j, s).wait_send()

        return carry

    lax.fori_loop(0, pairs, sent, 0)
    for i in range(direct):
        w_cross(i).wait_send()
    for i in range(2):
        w_aside(i).wait_send()
    for c in range(parts):
        w_to_core(c).wait_send()
    w_own_core().wait_send()


def rotary_lanes(row_count):
    position = np.arange(row_count)[:, None]
    lane = np.arange(LANES)[None, :]
    place = np.where(lane % HD < HD // 2, position // GRID_W, position % GRID_W).astype(np.float32)
    quarter = HD // 4
    step = (lane % quarter).astype(np.float32)
    inv_freq = np.power(np.float32(rotary_base), -(np.float32(2.0) * step) / np.float32(HD // 2))
    angle = inv_freq.astype(np.float32) * place
    sign = np.where((lane // quarter) % 2 == 0, np.float32(-1.0), np.float32(1.0))
    return np.cos(angle).astype(np.float32), (np.sin(angle) * sign).astype(np.float32)


def on_device(queries, keys, values, q_gain, k_gain, w_out):
    n, m = lax.axis_size("sp"), lax.axis_size("dp")
    rows = queries.shape[2]
    kv_width = keys.shape[1] // 2
    pairs = kv_width // LANES
    if n != 8 or m != 4 or kv_width % LANES or pairs < 2 or rows % 16 or QH != 2 * KV:
        return on_device_plain(queries, keys, values, q_gain, k_gain, w_out)
    seq_len = n * rows
    cos_table, sin_table = rotary_lanes(seq_len)
    hbm = pl.BlockSpec(memory_space=pltpu.HBM)
    bf16, f32 = jnp.bfloat16, jnp.float32
    dma = pltpu.SemaphoreType.DMA
    parts = 2 * pairs
    mixed = pl.pallas_call(
        functools.partial(layer_kernel, m),
        out_shape=jax.ShapeDtypeStruct((rows, w_out.shape[1] * m), bf16),
        in_specs=[hbm] * 8,
        out_specs=pl.BlockSpec(memory_space=pltpu.VMEM),
        scratch_shapes=[
            pltpu.VMEM((rows, queries.shape[1]), bf16),
            pltpu.VMEM((rows, keys.shape[1]), bf16),
            pltpu.VMEM((1, HD), f32),
            pltpu.VMEM((1, HD), f32),
            pltpu.VMEM((rows, LANES), f32),
            pltpu.VMEM((rows, LANES), f32),
            pltpu.VMEM((pairs, rows, LANES), bf16),
            pltpu.VMEM((pairs, rows, 2 * LANES), bf16),
            pltpu.VMEM((pairs, 8, 2, rows, LANES), bf16),
            pltpu.VMEM((pairs, 4, rows, 2 * LANES), bf16),
            pltpu.VMEM((pairs, 4, rows, 2 * LANES), bf16),
            pltpu.VMEM((parts, rows, 2 * LANES), bf16),
            pltpu.VMEM((m, w_out.shape[0], w_out.shape[1]), bf16),
            pltpu.VMEM((2, 4 * rows, seq_len), f32),
            pltpu.VMEM((2, 4 * rows, LANES), f32),
            pltpu.VMEM((2, 4 * rows, LANES), f32),
            dma((6,)), dma((pairs,)), dma((pairs,)), dma((pairs,)), dma((pairs,)),
            dma((pairs,)), dma((pairs,)), dma((pairs, 4)), dma((pairs, 4)), dma((pairs, 4)),
            dma((pairs, 4)), dma((pairs, 8)), dma((pairs, 4)), dma((parts,)),
            dma((parts - 2,)), dma((2,)), dma((parts + 1,)), dma((m, parts + 1)), dma,
        ],
        compiler_params=pltpu.CompilerParams(
            collective_id=0, has_side_effects=True, vmem_limit_bytes=62 * 1024 * 1024
        ),
    )(
        queries[0].T, keys[0].T, values[0].T, q_gain[None], k_gain[None],
        cos_table, sin_table, w_out,
    )
    return mixed[None]


def solution(mesh):
    placed = (
        P("dp", None, "sp"),
        P("dp", None, "sp"),
        P("dp", None, "sp"),
        P(),
        P(),
        P(None, "dp"),
    )
    return jax.shard_map(
        on_device, mesh=mesh, in_specs=placed, out_specs=P("dp", "sp", None), check_vma=False
    )
```

```python
import functools

import jax
import jax.numpy as jnp
import numpy as np
from jax import lax
from jax.experimental import pallas as pl
from jax.experimental.pallas import tpu as pltpu
from jax.sharding import PartitionSpec as P

HD = 64
QH = 32
KV = 16
GRID_W = 64


epsilon = 1e-06
rotary_base = 10000.0
block_count = 8


def swapped(block, axis, apart):
    count = lax.axis_size(axis)
    route = []
    for low in range(count):
        high = low | 1 << apart
        if high != low and high < count:
            route += [(low, high), (high, low)]
    return lax.ppermute(block, axis, route)


def rotary_tables(first_row, row_count):
    position = first_row + lax.iota(jnp.int32, row_count)
    grid_row = (position // GRID_W).astype(jnp.float32)
    grid_col = (position % GRID_W).astype(jnp.float32)
    quarter = HD // 4
    inv_freq = rotary_base ** (-(2.0 * lax.iota(jnp.float32, quarter)) / (HD // 2))
    row_angle = inv_freq[:, None] * grid_row[None, :]
    col_angle = inv_freq[:, None] * grid_col[None, :]
    cos_table = jnp.concatenate(
        [jnp.cos(row_angle), jnp.cos(row_angle), jnp.cos(col_angle), jnp.cos(col_angle)], axis=0
    )
    sin_table = jnp.concatenate(
        [jnp.sin(row_angle), jnp.sin(row_angle), jnp.sin(col_angle), jnp.sin(col_angle)], axis=0
    )
    return (cos_table, sin_table)


def normalize_turn(field, gain, cos_table, sin_table):
    head_count = field.shape[0] // HD
    values_f = field.astype(jnp.float32).reshape(head_count, HD, field.shape[1])
    normed = (
        values_f
        * lax.rsqrt(jnp.mean(values_f * values_f, axis=1, keepdims=True) + epsilon)
        * gain[None, :, None]
    )
    quarter = HD // 4
    quarters_of = normed.reshape(head_count, 4, quarter, field.shape[1])
    turned = jnp.concatenate(
        [-quarters_of[:, 1], quarters_of[:, 0], -quarters_of[:, 3], quarters_of[:, 2]], axis=1
    )
    return (normed * cos_table[None] + turned * sin_table[None]).astype(jnp.bfloat16)


def attention_heads(query_heads, key_heads, value_heads, seq_len):
    kv_local = key_heads.shape[0]
    group_local = query_heads.shape[0] // kv_local
    query_split = query_heads.reshape(kv_local, group_local, HD, seq_len)
    score_scale = HD ** (-0.5)
    block_rows = seq_len // block_count

    def one_block(block_index, result):
        row_start = block_index * block_rows
        query_block = lax.dynamic_slice_in_dim(query_split, row_start, block_rows, 3)
        scores = (
            jnp.einsum("hgdq,hdk->hgqk", query_block, key_heads, preferred_element_type=jnp.float32)
            * score_scale
        )
        row_max = jnp.max(scores, axis=-1, keepdims=True)
        weights = jnp.exp(scores - row_max)
        weights = (weights / jnp.sum(weights, axis=-1, keepdims=True)).astype(jnp.bfloat16)
        attended = jnp.einsum(
            "hgqk,hdk->hgdq", weights, value_heads, preferred_element_type=jnp.float32
        )
        return lax.dynamic_update_slice_in_dim(result, attended.astype(jnp.bfloat16), row_start, 3)

    result = jnp.zeros(query_split.shape, jnp.bfloat16)
    result = lax.fori_loop(0, block_count, one_block, result)
    return result.reshape(query_heads.shape)


def on_device_plain(queries, keys, values, q_gain, k_gain, w_out):
    sp_count = lax.axis_size("sp")
    tok_rows = queries.shape[2]
    seq_len = tok_rows * sp_count
    cos_table, sin_table = rotary_tables(lax.axis_index("sp") * tok_rows, tok_rows)
    query_rot = normalize_turn(queries[0], q_gain, cos_table, sin_table)
    key_rot = normalize_turn(keys[0], k_gain, cos_table, sin_table)
    value_rows = values[0].reshape(KV, HD, tok_rows)
    query_heads = lax.all_to_all(query_rot, "sp", split_axis=0, concat_axis=2, tiled=True)
    share_count = max(sp_count // KV, 1)
    part_rows = tok_rows // share_count
    key_cut = (
        key_rot.reshape(KV, HD, share_count, part_rows)
        .transpose(0, 2, 1, 3)
        .reshape(KV * share_count, HD, part_rows)
    )
    value_cut = (
        value_rows.reshape(KV, HD, share_count, part_rows)
        .transpose(0, 2, 1, 3)
        .reshape(KV * share_count, HD, part_rows)
    )
    key_got, value_got = (
        lax.all_to_all(key_cut, "sp", split_axis=0, concat_axis=2, tiled=True),
        lax.all_to_all(value_cut, "sp", split_axis=0, concat_axis=2, tiled=True),
    )
    kv_local = key_got.shape[0]
    key_got = key_got.reshape(kv_local, HD, sp_count, part_rows)
    value_got = value_got.reshape(kv_local, HD, sp_count, part_rows)
    for bit_index in range(share_count.bit_length() - 1):
        key_other, value_other = swapped((key_got, value_got), "sp", bit_index)
        key_got = jnp.concatenate([key_got, key_other], axis=3)
        value_got = jnp.concatenate([value_got, value_other], axis=3)
    key_heads = key_got.reshape(kv_local, HD, seq_len)
    value_heads = value_got.reshape(kv_local, HD, seq_len)
    attended = attention_heads(query_heads, key_heads, value_heads, seq_len)
    token_heads = lax.all_to_all(attended, "sp", split_axis=2, concat_axis=0, tiled=True)
    token_rows = token_heads.reshape(QH * HD, tok_rows)
    product = lax.dot_general(
        token_rows,
        lax.all_gather(w_out, "dp", axis=1, tiled=True),
        (((0,), (0,)), ((), ())),
        preferred_element_type=jnp.float32,
    )
    mixed_rows = product.astype(jnp.bfloat16)
    return mixed_rows[None]


MESH = pl.DeviceIdType.MESH
LOG2E = 1.4426950408889634
LANES = 128
TRANSPOSED = (((1,), (1,)), ((), ()))


def layer_kernel(
    m, q_ref, k_ref, v_ref, qg_ref, kg_ref, cos_ref, sin_ref, w_ref, out_ref,
    q_raw, k_raw, q_gain_in, k_gain_in, cos_in, sin_in, k_out, q_out, kv_in, q_in, a_out, a_in,
    w_all, score, v_turned, summed,
    load, v_own, k_side, v_side, q_side, k_got, v_got, q_got, kv_up, q_up, kv_mid, kv_got,
    a_send, a_got, w_x, w_y, w_core, w_got, w_local,
):
    me = lax.axis_index("sp")
    dp = lax.axis_index("dp")
    z, y = me // 2, me % 2
    half = z // 2
    z_in, z_out = 1 + half, 3 * half
    inner = z == z_in
    outer = jnp.logical_not(inner)
    base = jnp.where(inner, 0, 2)
    mine, beside = base + y, base + 1 - y
    sibling = z * 2 + 1 - y
    in_same = z_in * 2 + y
    across = (3 - z_in) * 2 + y
    core = lax.rem(dp, 2)
    x_at = dp // 2
    x_peer = (1 - x_at) * 2 + core
    core_peer = x_at * 2 + 1 - core
    x_other = (1 - x_at) * 2 + 1 - core
    rows = k_raw.shape[0]
    pairs = kv_in.shape[0]
    parts = 2 * pairs
    w_rows = w_ref.shape[0] // parts

    barrier = pltpu.get_barrier_semaphore()

    def greet(**there):
        pl.semaphore_signal(barrier, inc=1, device_id=there, device_id_type=MESH)

    greet(sp=sibling)
    greet(dp=x_peer)
    greet(dp=core_peer)
    z_other = jnp.where(inner, z_out, z_in)
    greet(sp=z_other * 2 + y)
    greet(sp=z_other * 2 + 1 - y)

    @pl.when(inner)
    def _():
        greet(sp=across)

    def kv_lanes(side, j):
        return pl.ds(pl.multiple_of((side * pairs + j) * LANES, LANES), LANES)

    first = pl.multiple_of(me * rows, rows)
    loads = [
        pltpu.make_async_copy(k_ref, k_raw, load.at[0]),
        pltpu.make_async_copy(cos_ref.at[pl.ds(first, rows)], cos_in, load.at[1]),
        pltpu.make_async_copy(sin_ref.at[pl.ds(first, rows)], sin_in, load.at[2]),
        pltpu.make_async_copy(kg_ref, k_gain_in, load.at[3]),
        pltpu.make_async_copy(qg_ref, q_gain_in, load.at[4]),
        pltpu.make_async_copy(q_ref, q_raw, load.at[5]),
    ]
    for one in loads:
        one.start()

    def own_values(j):
        return pltpu.make_async_copy(
            v_ref.at[:, kv_lanes(y, j)], kv_in.at[j, mine, 1], v_own.at[j]
        )

    for j in range(pairs):
        own_values(j).start()
    own_w = pltpu.make_async_copy(w_ref, w_all.at[dp], w_local)
    own_w.start()

    def remote(src, dst, sent, got, **there):
        return pltpu.make_async_remote_copy(
            src_ref=src, dst_ref=dst, send_sem=sent, recv_sem=got,
            device_id=there, device_id_type=MESH,
        )

    def k_aside(j, to=None):
        to = mine if to is None else to
        return remote(k_out.at[j], kv_in.at[j, to, 0], k_side.at[j], k_got.at[j], sp=sibling)

    def v_aside(j, to=None):
        to = mine if to is None else to
        return remote(
            v_ref.at[:, kv_lanes(1 - y, j)], kv_in.at[j, to, 1], v_side.at[j], v_got.at[j],
            sp=sibling,
        )

    def q_aside(j, to=None):
        to = mine if to is None else to
        return remote(q_out.at[j], q_in.at[j, to], q_side.at[j], q_got.at[j, to], sp=sibling)

    def kv_upward(j, s):
        return remote(
            kv_in.at[j, s], kv_in.at[j, s], kv_up.at[j, s], kv_got.at[j, s], sp=in_same
        )

    def q_upward(j, s):
        return remote(q_in.at[j, s], q_in.at[j, s], q_up.at[j, s], q_got.at[j, s], sp=in_same)

    def kv_across(j, s):
        return remote(
            kv_in.at[j, s], kv_in.at[j, 4 + s], kv_mid.at[j, s], kv_got.at[j, 4 + s], sp=across
        )

    def kv_came(j, s):
        remote(
            kv_in.at[j, s], kv_in.at[j, s], kv_up.at[j, 0], kv_got.at[j, s], sp=across
        ).wait_recv()

    def q_came(j, s):
        remote(q_in.at[j, s], q_in.at[j, s], q_up.at[j, 0], q_got.at[j, s], sp=sibling).wait_recv()

    def w_piece(ref, c):
        return ref.at[pl.ds(pl.multiple_of(c * w_rows, w_rows), w_rows)]

    def w_held(shard, c):
        return w_all.at[shard, pl.ds(pl.multiple_of(c * w_rows, w_rows), w_rows)]

    aside = pairs - 1
    direct = aside + 2

    def part_at(i):
        if i < aside:
            return y * pairs + i
        return (i - aside + 1) * pairs - 1

    def w_cross(i):
        c = part_at(i)
        return remote(w_piece(w_ref, c), w_held(dp, c), w_x.at[i], w_got.at[dp, c], dp=x_peer)

    def w_own_core():
        return remote(w_ref, w_all.at[dp], w_core.at[parts], w_got.at[dp, parts], dp=core_peer)

    def w_to_core(c):
        return remote(
            w_held(x_peer, c), w_held(x_peer, c), w_core.at[c], w_got.at[x_peer, c], dp=core_peer
        )

    def w_aside(i):
        c = part_at(i)
        return remote(
            w_held(x_peer, c), w_held(x_peer, c), w_y.at[i], w_got.at[x_peer, c], sp=sibling
        )

    def w_came(shard, c):
        remote(
            w_held(shard, c), w_held(shard, c), w_y.at[0], w_got.at[shard, c], dp=core_peer
        ).wait_recv()

    def pass_w(i):
        c = part_at(i)
        w_came(x_peer, c)
        w_to_core(c).start()
        if i < aside:
            w_aside(i).start()

    def pass_w_aside(i):
        c = (1 - y) * pairs + i
        w_came(x_peer, c)
        w_to_core(c).start()

    lane = lax.broadcasted_iota(jnp.int32, (rows, LANES), 1)
    low = lane < HD
    even = (lane // (HD // 4)) % 2 == 0

    def turn(tile, gain):
        u = tile.astype(jnp.float32)
        square = u * u
        sum_low = jnp.sum(jnp.where(low, square, 0.0), axis=1, keepdims=True)
        sum_high = jnp.sum(jnp.where(low, 0.0, square), axis=1, keepdims=True)
        inverse = jnp.where(
            low, lax.rsqrt(sum_low * (1.0 / HD) + epsilon), lax.rsqrt(sum_high * (1.0 / HD) + epsilon)
        )
        normed = u * inverse * gain
        part = HD // 4
        turned = jnp.where(even, pltpu.roll(normed, LANES - part, 1), pltpu.roll(normed, part, 1))
        return normed * cos_in[...] + turned * sin_in[...]

    def crossed(one, two):
        return (
            jnp.where(low, one, pltpu.roll(two, HD, 1)),
            jnp.where(low, pltpu.roll(one, HD, 1), two),
        )

    def turn_keys(j, side):
        return turn(k_raw[:, kv_lanes(side, j)], k_gain).astype(jnp.bfloat16)

    def turn_queries(j, side):
        at = (side * pairs + j) * 2 * LANES
        natural = [
            turn(q_raw[:, pl.ds(pl.multiple_of(at + i * LANES, LANES), LANES)], q_gain)
            for i in range(2)
        ]
        return jnp.concatenate(crossed(*natural), axis=1).astype(jnp.bfloat16)

    for one in loads[:5]:
        one.wait()
    q_gain, k_gain = (
        jnp.concatenate([g[...], g[...]], axis=1) for g in (q_gain_in, k_gain_in)
    )

    def key_step(j):
        k_out[j] = turn_keys(j, 1 - y)
        kv_in[j, mine, 0] = turn_keys(j, y)

    def query_step(j):
        q_out[j] = turn_queries(j, 1 - y)
        q_in[j, mine] = turn_queries(j, y)

    key_step(0)
    pl.semaphore_wait(barrier, jnp.where(inner, 6, 5))
    loads[5].wait()

    def send_step(j, carry):
        v_aside(j).start()

        @pl.when(j > 0)
        def _():
            key_step(j)

        k_aside(j).start()
        own_values(j).wait()

        @pl.when(jnp.logical_and(outer, j == 0))
        def _():
            kv_upward(j, mine).start()

        @pl.when(jnp.logical_and(inner, j < 2))
        def _():
            kv_across(j, mine).start()

        query_step(j)
        q_aside(j).start()

        @pl.when(jnp.logical_and(outer, j == 0))
        def _():
            q_upward(j, mine).start()

        return carry

    w_cross(0).start()
    w_cross(1).start()
    lax.fori_loop(0, pairs, send_step, 0)
    for i in range(2, direct):
        w_cross(i).start()
    w_own_core().start()

    def beside_came(j):
        k_aside(j, beside).wait_recv()
        v_aside(j, beside).wait_recv()

    @pl.when(outer)
    def _():
        def kv(j):
            if j:
                kv_upward(j, mine).start()
            beside_came(j)
            kv_upward(j, beside).start()

        def query(j):
            if j:
                q_upward(j, mine).start()
            q_came(j, beside)
            q_upward(j, beside).start()

        kv(0)
        query(0)
        for j in range(1, pairs):
            kv(j)
            if j > 1:
                query(j - 1)
        query(pairs - 1)
        for i in range(direct):
            pass_w(i)
            if i >= 2:
                pass_w_aside(i - 2)

    scale = HD ** (-0.5) * LOG2E
    step = 2 * LANES
    seq_len = 8 * rows
    tiles = [(t, min(step, seq_len - t)) for t in range(0, seq_len, step)]

    def by_sublane(tile):
        return tile.reshape(tile.shape[0] // 8, 8, tile.shape[1])

    def multiply_scores(j, s, at):
        pair = [q_in[j, s, :, g * LANES : (g + 1) * LANES] for g in range(2)]
        zero = jnp.zeros_like(pair[0])
        stack = [jnp.where(low, one, zero) for one in pair]
        stack += [jnp.where(low, zero, one) for one in pair]
        stack = jnp.concatenate(stack, axis=0)
        keys = kv_in[j, :, 0].reshape(seq_len, LANES)
        top = None
        for t, size in tiles:
            tile = lax.dot_general(
                keys[t : t + size], stack, TRANSPOSED, preferred_element_type=jnp.float32
            )
            score[at, t : t + size] = tile
            most = jnp.max(by_sublane(tile), axis=0)
            top = most if top is None else jnp.maximum(top, most)
        return jnp.max(top, axis=0, keepdims=True)

    def exponents(at, top):
        total = None
        for t, size in tiles:
            p = jnp.exp2((score[at, t : t + size] - top) * scale)
            score[at, t : t + size] = p
            more = jnp.sum(by_sublane(p), axis=0)
            total = more if total is None else total + more
        return 1.0 / jnp.sum(total, axis=0, keepdims=True)

    def weigh(at, inv):
        o = None
        for t, size in tiles:
            p = (score[at, t : t + size] * inv).astype(jnp.bfloat16)
            more = jnp.dot(v_turned[:, t : t + size], p, preferred_element_type=jnp.float32)
            o = more if o is None else o + more
        o = o.T
        cut = [o[i * rows : (i + 1) * rows] for i in range(4)]
        one = jnp.where(low, cut[0], pltpu.roll(cut[1], HD, 1))
        two = jnp.where(low, pltpu.roll(cut[2], HD, 1), cut[3])
        return jnp.concatenate([one, two], axis=1).astype(jnp.bfloat16)

    def a_copy(j, s):
        there = jnp.where(s < 2, z_in, z_out) * 2 + s % 2
        c = y * pairs + j
        return remote(a_out.at[j, s], a_in.at[c], a_send.at[j, s], a_got.at[c], sp=there)

    def relay_first(j):
        beside_came(j)
        kv_across(j, beside).start()
        kv_came(j, 2 + y)
        kv_across(j, 2 + y).start()

    def relay_last(j):
        kv_came(j, 3 - y)
        kv_across(j, 3 - y).start()

        @pl.when(j + 2 < pairs)
        def _():
            kv_across(j + 2, mine).start()

    def attend(j):
        q_came(j, 1 - y)
        q_came(j, 2)
        q_came(j, 3)
        for s in range(4, 8):
            kv_came(j, s)
        v_turned[...] = kv_in[j, :, 1].reshape(seq_len, LANES).T
        order = [2, 3, 1 - y, y]
        top = multiply_scores(j, order[0], 0)
        for u in range(4):
            if u < 3:
                later = multiply_scores(j, order[u + 1], (u + 1) % 2)
            inv = exponents(u % 2, top)
            tile = weigh(u % 2, inv)
            if u < 3:
                a_out[j, order[u]] = tile
                a_copy(j, order[u]).start()
                top = later
            else:
                a_in[y * pairs + j] = tile

    def a_came(c):
        remote(a_in.at[c], a_in.at[c], a_send.at[0, 0], a_got.at[c], sp=sibling).wait_recv()

    def a_ready(j):
        a_came((1 - y) * pairs + j)

        @pl.when(outer)
        def _():
            a_came(y * pairs + j)

    width = w_ref.shape[1]

    def project(which, first=False, last=False):
        for shard in range(m):
            at = slice(shard * width, (shard + 1) * width)
            total = None if first else summed[:, at]
            for j in which:
                for c in (j, pairs + j):
                    more = jnp.dot(
                        a_in[c], w_all[shard, c * w_rows : (c + 1) * w_rows, :],
                        preferred_element_type=jnp.float32,
                    )
                    total = more if total is None else total + more
            if last:
                out_ref[:, at] = total.astype(jnp.bfloat16)
            else:
                summed[:, at] = total

    def w_ready(which):
        for j in which:
            for c in (j, pairs + j):
                w_came(x_other, c)

    @pl.when(inner)
    def _():
        relay_first(0)
        relay_last(0)

        def one_pair(j, carry):
            relay_first(j + 1)
            relay_last(j + 1)
            for i in range(pairs - 1):
                @pl.when(j == i)
                def _():
                    pass_w(i)
                    if i >= 2:
                        pass_w_aside(i - 2)

            attend(j)
            return carry

        lax.fori_loop(0, pairs - 1, one_pair, 0)
        for i in range(1, aside - 1):
            pass_w_aside(i)

    own_w.wait()
    remote(
        w_ref, w_all.at[core_peer], w_core.at[parts], w_got.at[core_peer, parts], dp=core_peer
    ).wait_recv()
    early = list(range(pairs - 2))
    w_ready(early)
    for j in early:
        a_ready(j)
    project(early, first=True)

    @pl.when(inner)
    def _():
        pass_w(aside)
        pass_w_aside(aside - 1)
        attend(pairs - 1)
        pass_w(aside + 1)

    w_ready([pairs - 2])
    a_ready(pairs - 2)
    project([pairs - 2])
    w_ready([pairs - 1])
    a_ready(pairs - 1)
    project([pairs - 1], last=True)

    def sent(j, carry):
        k_aside(j).wait_send()
        v_aside(j).wait_send()
        q_aside(j).wait_send()

        @pl.when(outer)
        def _():
            for s in (mine, beside):
                kv_upward(j, s).wait_send()
                q_upward(j, s).wait_send()

        @pl.when(inner)
        def _():
            for s in range(4):
                kv_across(j, s).wait_send()
            for s in (1 - y, 2, 3):
                a_copy(j, s).wait_send()

        return carry

    lax.fori_loop(0, pairs, sent, 0)
    for i in range(direct):
        w_cross(i).wait_send()
    for i in range(aside):
        w_aside(i).wait_send()
    for c in range(parts):
        w_to_core(c).wait_send()
    w_own_core().wait_send()


def rotary_lanes(row_count):
    position = np.arange(row_count)[:, None]
    lane = np.arange(LANES)[None, :]
    place = np.where(lane % HD < HD // 2, position // GRID_W, position % GRID_W).astype(np.float32)
    quarter = HD // 4
    step = (lane % quarter).astype(np.float32)
    inv_freq = np.power(np.float32(rotary_base), -(np.float32(2.0) * step) / np.float32(HD // 2))
    angle = inv_freq.astype(np.float32) * place
    sign = np.where((lane // quarter) % 2 == 0, np.float32(-1.0), np.float32(1.0))
    return np.cos(angle).astype(np.float32), (np.sin(angle) * sign).astype(np.float32)


def on_device(queries, keys, values, q_gain, k_gain, w_out):
    n, m = lax.axis_size("sp"), lax.axis_size("dp")
    rows = queries.shape[2]
    kv_width = keys.shape[1] // 2
    pairs = kv_width // LANES
    if n != 8 or m != 4 or kv_width % LANES or pairs < 3 or rows % 16 or QH != 2 * KV:
        return on_device_plain(queries, keys, values, q_gain, k_gain, w_out)
    seq_len = n * rows
    cos_table, sin_table = rotary_lanes(seq_len)
    hbm = pl.BlockSpec(memory_space=pltpu.HBM)
    bf16, f32 = jnp.bfloat16, jnp.float32
    dma = pltpu.SemaphoreType.DMA
    parts = 2 * pairs
    mixed = pl.pallas_call(
        functools.partial(layer_kernel, m),
        out_shape=jax.ShapeDtypeStruct((rows, w_out.shape[1] * m), bf16),
        in_specs=[hbm] * 8,
        out_specs=pl.BlockSpec(memory_space=pltpu.VMEM),
        scratch_shapes=[
            pltpu.VMEM((rows, queries.shape[1]), bf16),
            pltpu.VMEM((rows, keys.shape[1]), bf16),
            pltpu.VMEM((1, HD), f32),
            pltpu.VMEM((1, HD), f32),
            pltpu.VMEM((rows, LANES), f32),
            pltpu.VMEM((rows, LANES), f32),
            pltpu.VMEM((pairs, rows, LANES), bf16),
            pltpu.VMEM((pairs, rows, 2 * LANES), bf16),
            pltpu.VMEM((pairs, 8, 2, rows, LANES), bf16),
            pltpu.VMEM((pairs, 4, rows, 2 * LANES), bf16),
            pltpu.VMEM((pairs, 4, rows, 2 * LANES), bf16),
            pltpu.VMEM((parts, rows, 2 * LANES), bf16),
            pltpu.VMEM((m, w_out.shape[0], w_out.shape[1]), bf16),
            pltpu.VMEM((2, seq_len, 4 * rows), f32),
            pltpu.VMEM((LANES, seq_len), bf16),
            pltpu.VMEM((rows, w_out.shape[1] * m), f32),
            dma((6,)), dma((pairs,)), dma((pairs,)), dma((pairs,)), dma((pairs,)),
            dma((pairs,)), dma((pairs,)), dma((pairs, 4)), dma((pairs, 4)), dma((pairs, 4)),
            dma((pairs, 4)), dma((pairs, 8)), dma((pairs, 4)), dma((parts,)),
            dma((pairs + 1,)), dma((pairs - 1,)), dma((parts + 1,)), dma((m, parts + 1)), dma,
        ],
        compiler_params=pltpu.CompilerParams(
            collective_id=0, has_side_effects=True, vmem_limit_bytes=44 * 1024 * 1024
        ),
    )(
        *(
            pltpu.with_memory_space_constraint(x, pltpu.HBM)
            for x in (
                queries[0].T, keys[0].T, values[0].T, q_gain[None], k_gain[None],
                jnp.asarray(cos_table), jnp.asarray(sin_table), w_out,
            )
        )
    )
    return mixed[None]


def solution(mesh):
    placed = (
        P("dp", None, "sp"),
        P("dp", None, "sp"),
        P("dp", None, "sp"),
        P(),
        P(),
        P(None, "dp"),
    )
    return jax.shard_map(
        on_device, mesh=mesh, in_specs=placed, out_specs=P("dp", "sp", None), check_vma=False
    )
```

```python
import functools

import jax
import jax.numpy as jnp
import numpy as np
from jax import lax
from jax.experimental import pallas as pl
from jax.experimental.pallas import tpu as pltpu
from jax.sharding import PartitionSpec as P

HD = 64
QH = 32
KV = 16
GRID_W = 64


epsilon = 1e-06
rotary_base = 10000.0
block_count = 8


def swapped(block, axis, apart):
    count = lax.axis_size(axis)
    route = []
    for low in range(count):
        high = low | 1 << apart
        if high != low and high < count:
            route += [(low, high), (high, low)]
    return lax.ppermute(block, axis, route)


def rotary_tables(first_row, row_count):
    position = first_row + lax.iota(jnp.int32, row_count)
    grid_row = (position // GRID_W).astype(jnp.float32)
    grid_col = (position % GRID_W).astype(jnp.float32)
    quarter = HD // 4
    inv_freq = rotary_base ** (-(2.0 * lax.iota(jnp.float32, quarter)) / (HD // 2))
    row_angle = inv_freq[:, None] * grid_row[None, :]
    col_angle = inv_freq[:, None] * grid_col[None, :]
    cos_table = jnp.concatenate(
        [jnp.cos(row_angle), jnp.cos(row_angle), jnp.cos(col_angle), jnp.cos(col_angle)], axis=0
    )
    sin_table = jnp.concatenate(
        [jnp.sin(row_angle), jnp.sin(row_angle), jnp.sin(col_angle), jnp.sin(col_angle)], axis=0
    )
    return (cos_table, sin_table)


def normalize_turn(field, gain, cos_table, sin_table):
    head_count = field.shape[0] // HD
    values_f = field.astype(jnp.float32).reshape(head_count, HD, field.shape[1])
    normed = (
        values_f
        * lax.rsqrt(jnp.mean(values_f * values_f, axis=1, keepdims=True) + epsilon)
        * gain[None, :, None]
    )
    quarter = HD // 4
    quarters_of = normed.reshape(head_count, 4, quarter, field.shape[1])
    turned = jnp.concatenate(
        [-quarters_of[:, 1], quarters_of[:, 0], -quarters_of[:, 3], quarters_of[:, 2]], axis=1
    )
    return (normed * cos_table[None] + turned * sin_table[None]).astype(jnp.bfloat16)


def attention_heads(query_heads, key_heads, value_heads, seq_len):
    kv_local = key_heads.shape[0]
    group_local = query_heads.shape[0] // kv_local
    query_split = query_heads.reshape(kv_local, group_local, HD, seq_len)
    score_scale = HD ** (-0.5)
    block_rows = seq_len // block_count

    def one_block(block_index, result):
        row_start = block_index * block_rows
        query_block = lax.dynamic_slice_in_dim(query_split, row_start, block_rows, 3)
        scores = (
            jnp.einsum("hgdq,hdk->hgqk", query_block, key_heads, preferred_element_type=jnp.float32)
            * score_scale
        )
        row_max = jnp.max(scores, axis=-1, keepdims=True)
        weights = jnp.exp(scores - row_max)
        weights = (weights / jnp.sum(weights, axis=-1, keepdims=True)).astype(jnp.bfloat16)
        attended = jnp.einsum(
            "hgqk,hdk->hgdq", weights, value_heads, preferred_element_type=jnp.float32
        )
        return lax.dynamic_update_slice_in_dim(result, attended.astype(jnp.bfloat16), row_start, 3)

    result = jnp.zeros(query_split.shape, jnp.bfloat16)
    result = lax.fori_loop(0, block_count, one_block, result)
    return result.reshape(query_heads.shape)


def on_device_plain(queries, keys, values, q_gain, k_gain, w_out):
    sp_count = lax.axis_size("sp")
    tok_rows = queries.shape[2]
    seq_len = tok_rows * sp_count
    cos_table, sin_table = rotary_tables(lax.axis_index("sp") * tok_rows, tok_rows)
    query_rot = normalize_turn(queries[0], q_gain, cos_table, sin_table)
    key_rot = normalize_turn(keys[0], k_gain, cos_table, sin_table)
    value_rows = values[0].reshape(KV, HD, tok_rows)
    query_heads = lax.all_to_all(query_rot, "sp", split_axis=0, concat_axis=2, tiled=True)
    share_count = max(sp_count // KV, 1)
    part_rows = tok_rows // share_count
    key_cut = (
        key_rot.reshape(KV, HD, share_count, part_rows)
        .transpose(0, 2, 1, 3)
        .reshape(KV * share_count, HD, part_rows)
    )
    value_cut = (
        value_rows.reshape(KV, HD, share_count, part_rows)
        .transpose(0, 2, 1, 3)
        .reshape(KV * share_count, HD, part_rows)
    )
    key_got, value_got = (
        lax.all_to_all(key_cut, "sp", split_axis=0, concat_axis=2, tiled=True),
        lax.all_to_all(value_cut, "sp", split_axis=0, concat_axis=2, tiled=True),
    )
    kv_local = key_got.shape[0]
    key_got = key_got.reshape(kv_local, HD, sp_count, part_rows)
    value_got = value_got.reshape(kv_local, HD, sp_count, part_rows)
    for bit_index in range(share_count.bit_length() - 1):
        key_other, value_other = swapped((key_got, value_got), "sp", bit_index)
        key_got = jnp.concatenate([key_got, key_other], axis=3)
        value_got = jnp.concatenate([value_got, value_other], axis=3)
    key_heads = key_got.reshape(kv_local, HD, seq_len)
    value_heads = value_got.reshape(kv_local, HD, seq_len)
    attended = attention_heads(query_heads, key_heads, value_heads, seq_len)
    token_heads = lax.all_to_all(attended, "sp", split_axis=2, concat_axis=0, tiled=True)
    token_rows = token_heads.reshape(QH * HD, tok_rows)
    product = lax.dot_general(
        token_rows,
        lax.all_gather(w_out, "dp", axis=1, tiled=True),
        (((0,), (0,)), ((), ())),
        preferred_element_type=jnp.float32,
    )
    mixed_rows = product.astype(jnp.bfloat16)
    return mixed_rows[None]


MESH = pl.DeviceIdType.MESH
LOG2E = 1.4426950408889634
LANES = 128
TRANSPOSED = (((1,), (1,)), ((), ()))


def layer_kernel(
    m, q_ref, k_ref, v_ref, qg_ref, kg_ref, cos_ref, sin_ref, w_ref, out_ref,
    q_raw, k_raw, q_gain_in, k_gain_in, cos_in, sin_in, k_out, q_out, kv_in, q_in, a_out, a_in,
    w_all, score, v_turned, summed,
    load, v_own, k_side, v_side, q_side, k_got, v_got, q_got, kv_up, q_up, kv_mid, kv_got, kv_low, kv_low_got,
    a_send, a_got, w_x, w_y, w_core, w_got, w_local,
):
    me = lax.axis_index("sp")
    dp = lax.axis_index("dp")
    z, y = me // 2, me % 2
    half = z // 2
    z_in, z_out = 1 + half, 3 * half
    inner = z == z_in
    outer = jnp.logical_not(inner)
    base = jnp.where(inner, 0, 2)
    mine, beside = base + y, base + 1 - y
    sibling = z * 2 + 1 - y
    in_same = z_in * 2 + y
    across = (3 - z_in) * 2 + y
    core = lax.rem(dp, 2)
    x_at = dp // 2
    x_peer = (1 - x_at) * 2 + core
    core_peer = x_at * 2 + 1 - core
    x_other = (1 - x_at) * 2 + 1 - core
    rows = k_raw.shape[0]
    pairs = kv_in.shape[0]
    parts = 2 * pairs
    shared = pairs // 2
    w_rows = w_ref.shape[0] // parts

    barrier = pltpu.get_barrier_semaphore()

    def greet(**there):
        pl.semaphore_signal(barrier, inc=1, device_id=there, device_id_type=MESH)

    greet(sp=sibling)
    greet(dp=x_peer)
    greet(dp=core_peer)
    z_other = jnp.where(inner, z_out, z_in)
    greet(sp=z_other * 2 + y)
    greet(sp=z_other * 2 + 1 - y)

    @pl.when(inner)
    def _():
        greet(sp=across)

    def kv_lanes(side, j):
        return pl.ds(pl.multiple_of((side * pairs + j) * LANES, LANES), LANES)

    first = pl.multiple_of(me * rows, rows)
    loads = [
        pltpu.make_async_copy(k_ref, k_raw, load.at[0]),
        pltpu.make_async_copy(cos_ref.at[pl.ds(first, rows)], cos_in, load.at[1]),
        pltpu.make_async_copy(sin_ref.at[pl.ds(first, rows)], sin_in, load.at[2]),
        pltpu.make_async_copy(kg_ref, k_gain_in, load.at[3]),
        pltpu.make_async_copy(qg_ref, q_gain_in, load.at[4]),
        pltpu.make_async_copy(q_ref, q_raw, load.at[5]),
    ]
    for one in loads:
        one.start()

    def own_values(j):
        return pltpu.make_async_copy(
            v_ref.at[:, kv_lanes(y, j)], kv_in.at[j, mine, 1], v_own.at[j]
        )

    for j in range(pairs):
        own_values(j).start()
    own_w = pltpu.make_async_copy(w_ref, w_all.at[dp], w_local)
    own_w.start()

    def remote(src, dst, sent, got, **there):
        return pltpu.make_async_remote_copy(
            src_ref=src, dst_ref=dst, send_sem=sent, recv_sem=got,
            device_id=there, device_id_type=MESH,
        )

    def k_aside(j, to=None):
        to = mine if to is None else to
        return remote(k_out.at[j], kv_in.at[j, to, 0], k_side.at[j], k_got.at[j], sp=sibling)

    def v_aside(j, to=None):
        to = mine if to is None else to
        return remote(
            v_ref.at[:, kv_lanes(1 - y, j)], kv_in.at[j, to, 1], v_side.at[j], v_got.at[j],
            sp=sibling,
        )

    def q_aside(j, to=None):
        to = mine if to is None else to
        return remote(q_out.at[j], q_in.at[j, to], q_side.at[j], q_got.at[j, to], sp=sibling)

    def kv_upward(j, s):
        return remote(
            kv_in.at[j, s], kv_in.at[j, s], kv_up.at[j, s], kv_got.at[j, s], sp=in_same
        )

    def q_upward(j, s):
        return remote(q_in.at[j, s], q_in.at[j, s], q_up.at[j, s], q_got.at[j, s], sp=in_same)

    def kv_across(j, s):
        return remote(
            kv_in.at[j, s], kv_in.at[j, 4 + s], kv_mid.at[j, s], kv_got.at[j, 4 + s], sp=across
        )

    out_same = z_out * 2 + y

    def kv_downward(j, part):
        at = pl.ds(4 * part, 2 + 2 * part)
        return remote(
            kv_in.at[j, at], kv_in.at[j, at], kv_low.at[j, part], kv_low_got.at[j, part],
            sp=out_same,
        )

    def kv_came(j, s):
        remote(
            kv_in.at[j, s], kv_in.at[j, s], kv_up.at[j, 0], kv_got.at[j, s], sp=across
        ).wait_recv()

    def q_came(j, s):
        remote(q_in.at[j, s], q_in.at[j, s], q_up.at[j, 0], q_got.at[j, s], sp=sibling).wait_recv()

    def w_piece(ref, c):
        return ref.at[pl.ds(pl.multiple_of(c * w_rows, w_rows), w_rows)]

    def w_held(shard, c):
        return w_all.at[shard, pl.ds(pl.multiple_of(c * w_rows, w_rows), w_rows)]

    aside = pairs - 1
    direct = aside + 2

    def part_at(i):
        if i < aside:
            return y * pairs + i
        return (i - aside + 1) * pairs - 1

    def w_cross(i):
        c = part_at(i)
        return remote(w_piece(w_ref, c), w_held(dp, c), w_x.at[i], w_got.at[dp, c], dp=x_peer)

    def w_own_core():
        return remote(w_ref, w_all.at[dp], w_core.at[parts], w_got.at[dp, parts], dp=core_peer)

    def w_to_core(c):
        return remote(
            w_held(x_peer, c), w_held(x_peer, c), w_core.at[c], w_got.at[x_peer, c], dp=core_peer
        )

    def w_aside(i):
        c = part_at(i)
        return remote(
            w_held(x_peer, c), w_held(x_peer, c), w_y.at[i], w_got.at[x_peer, c], sp=sibling
        )

    def w_came(shard, c):
        remote(
            w_held(shard, c), w_held(shard, c), w_y.at[0], w_got.at[shard, c], dp=core_peer
        ).wait_recv()

    def pass_w(i):
        c = part_at(i)
        w_came(x_peer, c)
        w_to_core(c).start()
        if i < aside:
            w_aside(i).start()

    def pass_w_aside(i):
        c = (1 - y) * pairs + i
        w_came(x_peer, c)
        w_to_core(c).start()

    lane = lax.broadcasted_iota(jnp.int32, (rows, LANES), 1)
    low = lane < HD
    even = (lane // (HD // 4)) % 2 == 0

    def turn(tile, gain):
        u = tile.astype(jnp.float32)
        square = u * u
        sum_low = jnp.sum(jnp.where(low, square, 0.0), axis=1, keepdims=True)
        sum_high = jnp.sum(jnp.where(low, 0.0, square), axis=1, keepdims=True)
        inverse = jnp.where(
            low, lax.rsqrt(sum_low * (1.0 / HD) + epsilon), lax.rsqrt(sum_high * (1.0 / HD) + epsilon)
        )
        normed = u * inverse * gain
        part = HD // 4
        turned = jnp.where(even, pltpu.roll(normed, LANES - part, 1), pltpu.roll(normed, part, 1))
        return normed * cos_in[...] + turned * sin_in[...]

    def crossed(one, two):
        return (
            jnp.where(low, one, pltpu.roll(two, HD, 1)),
            jnp.where(low, pltpu.roll(one, HD, 1), two),
        )

    def turn_keys(j, side):
        return turn(k_raw[:, kv_lanes(side, j)], k_gain).astype(jnp.bfloat16)

    def turn_queries(j, side):
        at = (side * pairs + j) * 2 * LANES
        natural = [
            turn(q_raw[:, pl.ds(pl.multiple_of(at + i * LANES, LANES), LANES)], q_gain)
            for i in range(2)
        ]
        return jnp.concatenate(crossed(*natural), axis=1).astype(jnp.bfloat16)

    for one in loads[:5]:
        one.wait()
    q_gain, k_gain = (
        jnp.concatenate([g[...], g[...]], axis=1) for g in (q_gain_in, k_gain_in)
    )

    def key_step(j):
        k_out[j] = turn_keys(j, 1 - y)
        kv_in[j, mine, 0] = turn_keys(j, y)

    def query_step(j):
        q_out[j] = turn_queries(j, 1 - y)
        q_in[j, mine] = turn_queries(j, y)

    key_step(0)
    pl.semaphore_wait(barrier, jnp.where(inner, 6, 5))
    loads[5].wait()

    def send_step(j, carry):
        v_aside(j).start()

        @pl.when(j > 0)
        def _():
            key_step(j)

        k_aside(j).start()
        own_values(j).wait()

        @pl.when(jnp.logical_and(outer, j == 0))
        def _():
            kv_upward(j, mine).start()

        @pl.when(jnp.logical_and(inner, j < 2))
        def _():
            kv_across(j, mine).start()

        query_step(j)
        q_aside(j).start()

        return carry

    w_cross(0).start()
    w_cross(1).start()
    lax.fori_loop(0, pairs, send_step, 0)
    for i in range(2, direct):
        w_cross(i).start()
    w_own_core().start()

    def beside_came(j):
        k_aside(j, beside).wait_recv()
        v_aside(j, beside).wait_recv()

    @pl.when(outer)
    def _():
        def kv(j):
            if j:
                kv_upward(j, mine).start()
            beside_came(j)
            kv_upward(j, beside).start()

        def query(j):
            if j:
                q_upward(j, mine).start()
            q_came(j, beside)
            q_upward(j, beside).start()

        for j in range(pairs):
            kv(j)
        for j in range(shared, pairs):
            query(j)

    scale = HD ** (-0.5) * LOG2E
    step = 2 * LANES
    seq_len = 8 * rows
    near_len = 4 * rows

    def tiles(far):
        start = near_len * far
        stop = start + near_len
        return [(t, min(step, stop - t)) for t in range(start, stop, step)]

    def by_sublane(tile):
        return tile.reshape(tile.shape[0] // 8, 8, tile.shape[1])

    def exponents(j, s, at, far):
        pair = [q_in[j, s, :, g * LANES : (g + 1) * LANES] for g in range(2)]
        zero = jnp.zeros_like(pair[0])
        stack = [jnp.where(low, one, zero) for one in pair]
        stack += [jnp.where(low, zero, one) for one in pair]
        stack = jnp.concatenate(stack, axis=0)
        keys = kv_in[j, 4 * far : 4 * far + 4, 0].reshape(near_len, LANES)
        top = None
        for t, size in tiles(far):
            tile = lax.dot_general(
                keys[t - near_len * far :][:size], stack, TRANSPOSED, preferred_element_type=jnp.float32
            )
            score[at, t : t + size] = tile
            most = jnp.max(by_sublane(tile), axis=0)
            top = most if top is None else jnp.maximum(top, most)
        top = jnp.max(top, axis=0, keepdims=True)

        def finish():
            total = None
            for t, size in tiles(far):
                p = jnp.exp2((score[at, t : t + size] - top) * scale)
                score[at, t : t + size] = p
                more = jnp.sum(by_sublane(p), axis=0)
                total = more if total is None else total + more
            return top, jnp.sum(total, axis=0, keepdims=True)

        return finish

    def staged(j, order, far):
        found = []
        ahead = exponents(j, order[0], 0, far)
        for u in range(len(order)):
            now = ahead
            if u + 1 < len(order):
                ahead = exponents(j, order[u + 1], u + 1, far)
            found.append(now())
        return found

    def weigh(at, near, far):
        top = jnp.maximum(near[0], far[0])
        shrink = [jnp.exp2((one[0] - top) * scale) for one in (near, far)]
        inv = 1.0 / (near[1] * shrink[0] + far[1] * shrink[1])
        o = None
        for side in range(2):
            factor = shrink[side] * inv
            for t, size in tiles(side):
                p = (score[at, t : t + size] * factor).astype(jnp.bfloat16)
                more = jnp.dot(v_turned[:, t : t + size], p, preferred_element_type=jnp.float32)
                o = more if o is None else o + more
        o = o.T
        cut = [o[i * rows : (i + 1) * rows] for i in range(4)]
        one = jnp.where(low, cut[0], pltpu.roll(cut[1], HD, 1))
        two = jnp.where(low, pltpu.roll(cut[2], HD, 1), cut[3])
        return jnp.concatenate([one, two], axis=1).astype(jnp.bfloat16)

    def a_copy(j, s):
        there = jnp.where(s < 2, z_in, z_out) * 2 + s % 2
        c = y * pairs + j
        return remote(a_out.at[j, s], a_in.at[c], a_send.at[j, s], a_got.at[c], sp=there)

    def relay_first(j):
        beside_came(j)
        kv_across(j, beside).start()

        @pl.when(j < shared)
        def _():
            kv_downward(j, 0).start()

        kv_came(j, 2 + y)
        kv_across(j, 2 + y).start()

    def relay_last(j):
        kv_came(j, 3 - y)
        kv_across(j, 3 - y).start()

        @pl.when(j + 2 < pairs)
        def _():
            kv_across(j + 2, mine).start()

    def turn_values(j, far):
        at = slice(near_len * far, near_len * (far + 1))
        v_turned[:, at] = kv_in[j, 4 * far : 4 * far + 4, 1].reshape(near_len, LANES).T

    def attend(j, order, await_far, eager):
        turn_values(j, 0)
        near = staged(j, order, 0)
        await_far()
        turn_values(j, 1)
        ready = exponents(j, order[0], 0, 1)
        for u in range(len(order)):
            far = ready()
            if u + 1 < len(order):
                ready = exponents(j, order[u + 1], u + 1, 1)
            tile = weigh(u, near[u], far)
            if u + 1 < len(order):
                a_out[j, order[u]] = tile
                if eager:
                    a_copy(j, order[u]).start()
            else:
                a_in[y * pairs + j] = tile
        if not eager:
            for s in order[:-1]:
                a_copy(j, s).start()

    def a_came(c):
        remote(a_in.at[c], a_in.at[c], a_send.at[0, 0], a_got.at[c], sp=sibling).wait_recv()

    def a_ready(j):
        a_came((1 - y) * pairs + j)

        if j >= shared:
            @pl.when(outer)
            def _():
                a_came(y * pairs + j)

    width = w_ref.shape[1]

    def project(which, first=False, last=False):
        for shard in range(m):
            at = slice(shard * width, (shard + 1) * width)
            total = None if first else summed[:, at]
            for j in which:
                for c in (j, pairs + j):
                    more = jnp.dot(
                        a_in[c], w_all[shard, c * w_rows : (c + 1) * w_rows, :],
                        preferred_element_type=jnp.float32,
                    )
                    total = more if total is None else total + more
            if last:
                out_ref[:, at] = total.astype(jnp.bfloat16)
            else:
                summed[:, at] = total

    def w_ready(which):
        for j in which:
            for c in (j, pairs + j):
                w_came(x_other, c)

    def far_came(j):
        for s in range(4, 8):
            kv_came(j, s)

    @pl.when(inner)
    def _():
        for j in range(shared):
            relay_first(j)
            relay_last(j)

    def shared_pair(j, carry):
        @pl.when(inner)
        def _():
            @pl.when(j + shared < pairs)
            def _():
                relay_first(j + shared)
                relay_last(j + shared)

        @pl.when(outer)
        def _():
            low_came(j, 0)

        for i in range(shared):
            @pl.when(j == i)
            def _():
                pass_w(i)

        @pl.when(inner)
        def _():
            q_came(j, beside)

        def await_far():
            @pl.when(inner)
            def _():
                far_came(j)
                kv_downward(j, 1).start()

            @pl.when(outer)
            def _():
                low_came(j, 1)

        attend(j, [beside, mine], await_far, False)
        return carry

    def low_came(j, part):
        kv_downward(j, part).wait_recv()

    @pl.when(outer)
    def _():
        for j in range(shared):
            q_came(j, beside)

    lax.fori_loop(0, shared, shared_pair, 0)
    order = [2, 3, 1 - y, y]

    def late_pair(j, eager):
        for s in (1 - y, 2, 3):
            q_came(j, s)
        attend(j, order, lambda: far_came(j), eager)

    for i in range(shared, aside):
        pass_w(i)
    pass_w_aside(0)

    @pl.when(inner)
    def _():
        for j in range(shared, pairs - 1):
            late_pair(j, False)

    for i in range(1, aside - 1):
        pass_w_aside(i)
    pass_w(aside)
    own_w.wait()
    remote(
        w_ref, w_all.at[core_peer], w_core.at[parts], w_got.at[core_peer, parts], dp=core_peer
    ).wait_recv()
    early = list(range(pairs - 2))
    w_ready(early)
    for j in early:
        a_ready(j)
    project(early, first=True)
    pass_w_aside(aside - 1)

    @pl.when(inner)
    def _():
        late_pair(pairs - 1, True)

    pass_w(aside + 1)
    w_ready([pairs - 2])
    a_ready(pairs - 2)
    project([pairs - 2])
    w_ready([pairs - 1])
    a_ready(pairs - 1)
    project([pairs - 1], last=True)

    def sent(j, carry):
        k_aside(j).wait_send()
        v_aside(j).wait_send()
        q_aside(j).wait_send()

        @pl.when(outer)
        def _():
            for s in (mine, beside):
                kv_upward(j, s).wait_send()

                @pl.when(j >= shared)
                def _():
                    q_upward(j, s).wait_send()

        @pl.when(inner)
        def _():
            for s in range(4):
                kv_across(j, s).wait_send()

            @pl.when(j < shared)
            def _():
                for part in range(2):
                    kv_downward(j, part).wait_send()

            @pl.when(j >= shared)
            def _():
                for s in (2, 3):
                    a_copy(j, s).wait_send()

        @pl.when(jnp.logical_or(inner, j < shared))
        def _():
            a_copy(j, beside).wait_send()

        return carry

    lax.fori_loop(0, pairs, sent, 0)
    for i in range(direct):
        w_cross(i).wait_send()
    for i in range(aside):
        w_aside(i).wait_send()
    for c in range(parts):
        w_to_core(c).wait_send()
    w_own_core().wait_send()


def rotary_lanes(row_count):
    position = np.arange(row_count)[:, None]
    lane = np.arange(LANES)[None, :]
    place = np.where(lane % HD < HD // 2, position // GRID_W, position % GRID_W).astype(np.float32)
    quarter = HD // 4
    step = (lane % quarter).astype(np.float32)
    inv_freq = np.power(np.float32(rotary_base), -(np.float32(2.0) * step) / np.float32(HD // 2))
    angle = inv_freq.astype(np.float32) * place
    sign = np.where((lane // quarter) % 2 == 0, np.float32(-1.0), np.float32(1.0))
    return np.cos(angle).astype(np.float32), (np.sin(angle) * sign).astype(np.float32)


def on_device(queries, keys, values, q_gain, k_gain, w_out):
    n, m = lax.axis_size("sp"), lax.axis_size("dp")
    rows = queries.shape[2]
    kv_width = keys.shape[1] // 2
    pairs = kv_width // LANES
    if n != 8 or m != 4 or kv_width % LANES or pairs < 4 or rows % 32 or QH != 2 * KV:
        return on_device_plain(queries, keys, values, q_gain, k_gain, w_out)
    seq_len = n * rows
    cos_table, sin_table = rotary_lanes(seq_len)
    hbm = pl.BlockSpec(memory_space=pltpu.HBM)
    bf16, f32 = jnp.bfloat16, jnp.float32
    dma = pltpu.SemaphoreType.DMA
    parts = 2 * pairs
    mixed = pl.pallas_call(
        functools.partial(layer_kernel, m),
        out_shape=jax.ShapeDtypeStruct((rows, w_out.shape[1] * m), bf16),
        in_specs=[hbm] * 8,
        out_specs=pl.BlockSpec(memory_space=pltpu.VMEM),
        scratch_shapes=[
            pltpu.VMEM((rows, queries.shape[1]), bf16),
            pltpu.VMEM((rows, keys.shape[1]), bf16),
            pltpu.VMEM((1, HD), f32),
            pltpu.VMEM((1, HD), f32),
            pltpu.VMEM((rows, LANES), f32),
            pltpu.VMEM((rows, LANES), f32),
            pltpu.VMEM((pairs, rows, LANES), bf16),
            pltpu.VMEM((pairs, rows, 2 * LANES), bf16),
            pltpu.VMEM((pairs, 8, 2, rows, LANES), bf16),
            pltpu.VMEM((pairs, 4, rows, 2 * LANES), bf16),
            pltpu.VMEM((pairs, 4, rows, 2 * LANES), bf16),
            pltpu.VMEM((parts, rows, 2 * LANES), bf16),
            pltpu.VMEM((m, w_out.shape[0], w_out.shape[1]), bf16),
            pltpu.VMEM((4, seq_len, 4 * rows), f32),
            pltpu.VMEM((LANES, seq_len), bf16),
            pltpu.VMEM((rows, w_out.shape[1] * m), f32),
            dma((6,)), dma((pairs,)), dma((pairs,)), dma((pairs,)), dma((pairs,)),
            dma((pairs,)), dma((pairs,)), dma((pairs, 4)), dma((pairs, 4)), dma((pairs, 4)),
            dma((pairs, 4)), dma((pairs, 8)), dma((pairs, 2)), dma((pairs, 2)), dma((pairs, 4)),
            dma((parts,)),
            dma((pairs + 1,)), dma((pairs - 1,)), dma((parts + 1,)), dma((m, parts + 1)), dma,
        ],
        compiler_params=pltpu.CompilerParams(
            collective_id=0, has_side_effects=True, vmem_limit_bytes=44 * 1024 * 1024
        ),
    )(
        *(
            pltpu.with_memory_space_constraint(x, pltpu.HBM)
            for x in (
                queries[0].T, keys[0].T, values[0].T, q_gain[None], k_gain[None],
                jnp.asarray(cos_table), jnp.asarray(sin_table), w_out,
            )
        )
    )
    return mixed[None]


def solution(mesh):
    placed = (
        P("dp", None, "sp"),
        P("dp", None, "sp"),
        P("dp", None, "sp"),
        P(),
        P(),
        P(None, "dp"),
    )
    return jax.shard_map(
        on_device, mesh=mesh, in_specs=placed, out_specs=P("dp", "sp", None), check_vma=False
    )
```

```python
import functools

import jax
import jax.numpy as jnp
import numpy as np
from jax import lax
from jax.experimental import pallas as pl
from jax.experimental.pallas import tpu as pltpu
from jax.sharding import PartitionSpec as P

HD = 64
QH = 32
KV = 16
GRID_W = 64


epsilon = 1e-06
rotary_base = 10000.0
block_count = 8


def swapped(block, axis, apart):
    count = lax.axis_size(axis)
    route = []
    for low in range(count):
        high = low | 1 << apart
        if high != low and high < count:
            route += [(low, high), (high, low)]
    return lax.ppermute(block, axis, route)


def rotary_tables(first_row, row_count):
    position = first_row + lax.iota(jnp.int32, row_count)
    grid_row = (position // GRID_W).astype(jnp.float32)
    grid_col = (position % GRID_W).astype(jnp.float32)
    quarter = HD // 4
    inv_freq = rotary_base ** (-(2.0 * lax.iota(jnp.float32, quarter)) / (HD // 2))
    row_angle = inv_freq[:, None] * grid_row[None, :]
    col_angle = inv_freq[:, None] * grid_col[None, :]
    cos_table = jnp.concatenate(
        [jnp.cos(row_angle), jnp.cos(row_angle), jnp.cos(col_angle), jnp.cos(col_angle)], axis=0
    )
    sin_table = jnp.concatenate(
        [jnp.sin(row_angle), jnp.sin(row_angle), jnp.sin(col_angle), jnp.sin(col_angle)], axis=0
    )
    return (cos_table, sin_table)


def normalize_turn(field, gain, cos_table, sin_table):
    head_count = field.shape[0] // HD
    values_f = field.astype(jnp.float32).reshape(head_count, HD, field.shape[1])
    normed = (
        values_f
        * lax.rsqrt(jnp.mean(values_f * values_f, axis=1, keepdims=True) + epsilon)
        * gain[None, :, None]
    )
    quarter = HD // 4
    quarters_of = normed.reshape(head_count, 4, quarter, field.shape[1])
    turned = jnp.concatenate(
        [-quarters_of[:, 1], quarters_of[:, 0], -quarters_of[:, 3], quarters_of[:, 2]], axis=1
    )
    return (normed * cos_table[None] + turned * sin_table[None]).astype(jnp.bfloat16)


def attention_heads(query_heads, key_heads, value_heads, seq_len):
    kv_local = key_heads.shape[0]
    group_local = query_heads.shape[0] // kv_local
    query_split = query_heads.reshape(kv_local, group_local, HD, seq_len)
    score_scale = HD ** (-0.5)
    block_rows = seq_len // block_count

    def one_block(block_index, result):
        row_start = block_index * block_rows
        query_block = lax.dynamic_slice_in_dim(query_split, row_start, block_rows, 3)
        scores = (
            jnp.einsum("hgdq,hdk->hgqk", query_block, key_heads, preferred_element_type=jnp.float32)
            * score_scale
        )
        row_max = jnp.max(scores, axis=-1, keepdims=True)
        weights = jnp.exp(scores - row_max)
        weights = (weights / jnp.sum(weights, axis=-1, keepdims=True)).astype(jnp.bfloat16)
        attended = jnp.einsum(
            "hgqk,hdk->hgdq", weights, value_heads, preferred_element_type=jnp.float32
        )
        return lax.dynamic_update_slice_in_dim(result, attended.astype(jnp.bfloat16), row_start, 3)

    result = jnp.zeros(query_split.shape, jnp.bfloat16)
    result = lax.fori_loop(0, block_count, one_block, result)
    return result.reshape(query_heads.shape)


def on_device_plain(queries, keys, values, q_gain, k_gain, w_out):
    sp_count = lax.axis_size("sp")
    tok_rows = queries.shape[2]
    seq_len = tok_rows * sp_count
    cos_table, sin_table = rotary_tables(lax.axis_index("sp") * tok_rows, tok_rows)
    query_rot = normalize_turn(queries[0], q_gain, cos_table, sin_table)
    key_rot = normalize_turn(keys[0], k_gain, cos_table, sin_table)
    value_rows = values[0].reshape(KV, HD, tok_rows)
    query_heads = lax.all_to_all(query_rot, "sp", split_axis=0, concat_axis=2, tiled=True)
    share_count = max(sp_count // KV, 1)
    part_rows = tok_rows // share_count
    key_cut = (
        key_rot.reshape(KV, HD, share_count, part_rows)
        .transpose(0, 2, 1, 3)
        .reshape(KV * share_count, HD, part_rows)
    )
    value_cut = (
        value_rows.reshape(KV, HD, share_count, part_rows)
        .transpose(0, 2, 1, 3)
        .reshape(KV * share_count, HD, part_rows)
    )
    key_got, value_got = (
        lax.all_to_all(key_cut, "sp", split_axis=0, concat_axis=2, tiled=True),
        lax.all_to_all(value_cut, "sp", split_axis=0, concat_axis=2, tiled=True),
    )
    kv_local = key_got.shape[0]
    key_got = key_got.reshape(kv_local, HD, sp_count, part_rows)
    value_got = value_got.reshape(kv_local, HD, sp_count, part_rows)
    for bit_index in range(share_count.bit_length() - 1):
        key_other, value_other = swapped((key_got, value_got), "sp", bit_index)
        key_got = jnp.concatenate([key_got, key_other], axis=3)
        value_got = jnp.concatenate([value_got, value_other], axis=3)
    key_heads = key_got.reshape(kv_local, HD, seq_len)
    value_heads = value_got.reshape(kv_local, HD, seq_len)
    attended = attention_heads(query_heads, key_heads, value_heads, seq_len)
    token_heads = lax.all_to_all(attended, "sp", split_axis=2, concat_axis=0, tiled=True)
    token_rows = token_heads.reshape(QH * HD, tok_rows)
    product = lax.dot_general(
        token_rows,
        lax.all_gather(w_out, "dp", axis=1, tiled=True),
        (((0,), (0,)), ((), ())),
        preferred_element_type=jnp.float32,
    )
    mixed_rows = product.astype(jnp.bfloat16)
    return mixed_rows[None]


MESH = pl.DeviceIdType.MESH
LOG2E = 1.4426950408889634
LANES = 128
TRANSPOSED = (((1,), (1,)), ((), ()))


def layer_kernel(
    m, q_ref, k_ref, v_ref, qg_ref, kg_ref, cos_ref, sin_ref, w_ref, out_ref,
    q_raw, k_raw, q_gain_in, k_gain_in, cos_in, sin_in, k_out, q_out, kv_in, q_in, a_out, a_in,
    w_all, score, v_turned, summed,
    load, v_own, k_side, v_side, q_side, k_got, v_got, q_got, kv_up, q_up, kv_mid, kv_got, kv_low, kv_low_got,
    a_send, a_got, w_x, w_y, w_core, w_got, w_local,
):
    me = lax.axis_index("sp")
    dp = lax.axis_index("dp")
    z, y = me // 2, me % 2
    half = z // 2
    z_in, z_out = 1 + half, 3 * half
    inner = z == z_in
    outer = jnp.logical_not(inner)
    base = jnp.where(inner, 0, 2)
    mine, beside = base + y, base + 1 - y
    sibling = z * 2 + 1 - y
    in_same = z_in * 2 + y
    across = (3 - z_in) * 2 + y
    core = lax.rem(dp, 2)
    x_at = dp // 2
    x_peer = (1 - x_at) * 2 + core
    core_peer = x_at * 2 + 1 - core
    x_other = (1 - x_at) * 2 + 1 - core
    rows = k_raw.shape[0]
    pairs = kv_in.shape[0]
    parts = 2 * pairs
    shared = pairs // 2
    w_rows = w_ref.shape[0] // parts

    barrier = pltpu.get_barrier_semaphore()

    def greet(**there):
        pl.semaphore_signal(barrier, inc=1, device_id=there, device_id_type=MESH)

    greet(sp=sibling)
    greet(dp=x_peer)
    greet(dp=core_peer)
    z_other = jnp.where(inner, z_out, z_in)
    greet(sp=z_other * 2 + y)
    greet(sp=z_other * 2 + 1 - y)

    @pl.when(inner)
    def _():
        greet(sp=across)

    def kv_lanes(side, j):
        return pl.ds(pl.multiple_of((side * pairs + j) * LANES, LANES), LANES)

    first = pl.multiple_of(me * rows, rows)
    loads = [
        pltpu.make_async_copy(k_ref, k_raw, load.at[0]),
        pltpu.make_async_copy(cos_ref.at[pl.ds(first, rows)], cos_in, load.at[1]),
        pltpu.make_async_copy(sin_ref.at[pl.ds(first, rows)], sin_in, load.at[2]),
        pltpu.make_async_copy(kg_ref, k_gain_in, load.at[3]),
        pltpu.make_async_copy(qg_ref, q_gain_in, load.at[4]),
        pltpu.make_async_copy(q_ref, q_raw, load.at[5]),
    ]
    for one in loads:
        one.start()

    def own_values(j):
        return pltpu.make_async_copy(
            v_ref.at[:, kv_lanes(y, j)], kv_in.at[j, mine, 1], v_own.at[j]
        )

    for j in range(pairs):
        own_values(j).start()
    own_w = pltpu.make_async_copy(w_ref, w_all.at[dp], w_local)
    own_w.start()

    def remote(src, dst, sent, got, **there):
        return pltpu.make_async_remote_copy(
            src_ref=src, dst_ref=dst, send_sem=sent, recv_sem=got,
            device_id=there, device_id_type=MESH,
        )

    def k_aside(j, to=None):
        to = mine if to is None else to
        return remote(k_out.at[j], kv_in.at[j, to, 0], k_side.at[j], k_got.at[j], sp=sibling)

    def v_aside(j, to=None):
        to = mine if to is None else to
        return remote(
            v_ref.at[:, kv_lanes(1 - y, j)], kv_in.at[j, to, 1], v_side.at[j], v_got.at[j],
            sp=sibling,
        )

    def q_aside(j, to=None):
        to = mine if to is None else to
        return remote(q_out.at[j], q_in.at[j, to], q_side.at[j], q_got.at[j, to], sp=sibling)

    def kv_upward(j, s):
        return remote(
            kv_in.at[j, s], kv_in.at[j, s], kv_up.at[j, s], kv_got.at[j, s], sp=in_same
        )

    def q_upward(j, s):
        return remote(q_in.at[j, s], q_in.at[j, s], q_up.at[j, s], q_got.at[j, s], sp=in_same)

    def kv_across(j, s):
        return remote(
            kv_in.at[j, s], kv_in.at[j, 4 + s], kv_mid.at[j, s], kv_got.at[j, 4 + s], sp=across
        )

    out_same = z_out * 2 + y

    def kv_downward(j, part):
        at = pl.ds(4 * part, 2 + 2 * part)
        return remote(
            kv_in.at[j, at], kv_in.at[j, at], kv_low.at[j, part], kv_low_got.at[j, part],
            sp=out_same,
        )

    def kv_came(j, s):
        remote(
            kv_in.at[j, s], kv_in.at[j, s], kv_up.at[j, 0], kv_got.at[j, s], sp=across
        ).wait_recv()

    def q_came(j, s):
        remote(q_in.at[j, s], q_in.at[j, s], q_up.at[j, 0], q_got.at[j, s], sp=sibling).wait_recv()

    def w_piece(ref, c):
        return ref.at[pl.ds(pl.multiple_of(c * w_rows, w_rows), w_rows)]

    def w_held(shard, c):
        return w_all.at[shard, pl.ds(pl.multiple_of(c * w_rows, w_rows), w_rows)]

    aside = pairs // 2
    direct = parts - aside

    def part_at(i):
        if i < aside:
            return y * pairs + i
        return (i % 2) * pairs + (aside + i) // 2

    def w_cross(i):
        c = part_at(i)
        return remote(w_piece(w_ref, c), w_held(dp, c), w_x.at[i], w_got.at[dp, c], dp=x_peer)

    def w_own_core():
        return remote(w_ref, w_all.at[dp], w_core.at[parts], w_got.at[dp, parts], dp=core_peer)

    def w_to_core(c):
        return remote(
            w_held(x_peer, c), w_held(x_peer, c), w_core.at[c], w_got.at[x_peer, c], dp=core_peer
        )

    def w_aside(i):
        c = part_at(i)
        return remote(
            w_held(x_peer, c), w_held(x_peer, c), w_y.at[i], w_got.at[x_peer, c], sp=sibling
        )

    def w_came(shard, c):
        remote(
            w_held(shard, c), w_held(shard, c), w_y.at[0], w_got.at[shard, c], dp=core_peer
        ).wait_recv()

    def pass_w(i):
        c = part_at(i)
        w_came(x_peer, c)
        w_to_core(c).start()
        if i < aside:
            w_aside(i).start()

    def pass_w_aside(i):
        c = (1 - y) * pairs + i
        w_came(x_peer, c)
        w_to_core(c).start()

    lane = lax.broadcasted_iota(jnp.int32, (rows, LANES), 1)
    low = lane < HD
    even = (lane // (HD // 4)) % 2 == 0

    def turn(tile, gain):
        u = tile.astype(jnp.float32)
        square = u * u
        sum_low = jnp.sum(jnp.where(low, square, 0.0), axis=1, keepdims=True)
        sum_high = jnp.sum(jnp.where(low, 0.0, square), axis=1, keepdims=True)
        inverse = jnp.where(
            low, lax.rsqrt(sum_low * (1.0 / HD) + epsilon), lax.rsqrt(sum_high * (1.0 / HD) + epsilon)
        )
        normed = u * inverse * gain
        part = HD // 4
        turned = jnp.where(even, pltpu.roll(normed, LANES - part, 1), pltpu.roll(normed, part, 1))
        return normed * cos_in[...] + turned * sin_in[...]

    def crossed(one, two):
        return (
            jnp.where(low, one, pltpu.roll(two, HD, 1)),
            jnp.where(low, pltpu.roll(one, HD, 1), two),
        )

    def turn_keys(j, side):
        return turn(k_raw[:, kv_lanes(side, j)], k_gain).astype(jnp.bfloat16)

    def turn_queries(j, side):
        at = (side * pairs + j) * 2 * LANES
        natural = [
            turn(q_raw[:, pl.ds(pl.multiple_of(at + i * LANES, LANES), LANES)], q_gain)
            for i in range(2)
        ]
        return jnp.concatenate(crossed(*natural), axis=1).astype(jnp.bfloat16)

    for one in loads[:5]:
        one.wait()
    q_gain, k_gain = (
        jnp.concatenate([g[...], g[...]], axis=1) for g in (q_gain_in, k_gain_in)
    )

    def key_step(j):
        k_out[j] = turn_keys(j, 1 - y)
        kv_in[j, mine, 0] = turn_keys(j, y)

    def query_step(j):
        q_out[j] = turn_queries(j, 1 - y)
        q_in[j, mine] = turn_queries(j, y)

    key_step(0)
    pl.semaphore_wait(barrier, jnp.where(inner, 6, 5))
    loads[5].wait()

    def send_step(j, carry):
        v_aside(j).start()

        @pl.when(j > 0)
        def _():
            key_step(j)

        k_aside(j).start()
        own_values(j).wait()

        @pl.when(jnp.logical_and(outer, j == 0))
        def _():
            kv_upward(j, mine).start()

        @pl.when(jnp.logical_and(inner, j < 2))
        def _():
            kv_across(j, mine).start()

        query_step(j)
        q_aside(j).start()

        return carry

    w_cross(0).start()
    w_cross(1).start()
    lax.fori_loop(0, pairs, send_step, 0)
    for i in range(2, direct):
        w_cross(i).start()
    w_own_core().start()

    def beside_came(j):
        k_aside(j, beside).wait_recv()
        v_aside(j, beside).wait_recv()

    @pl.when(outer)
    def _():
        def kv(j):
            if j:
                kv_upward(j, mine).start()
            beside_came(j)
            kv_upward(j, beside).start()

        def query(j):
            if j:
                q_upward(j, mine).start()
            q_came(j, beside)
            q_upward(j, beside).start()

        for j in range(pairs):
            kv(j)
        for j in range(shared, pairs):
            query(j)

    scale = HD ** (-0.5) * LOG2E
    step = 2 * LANES
    seq_len = 8 * rows
    near_len = 4 * rows

    def tiles(far):
        start = near_len * far
        stop = start + near_len
        return [(t, min(step, stop - t)) for t in range(start, stop, step)]

    def by_sublane(tile):
        return tile.reshape(tile.shape[0] // 8, 8, tile.shape[1])

    def exponents(j, s, at, far):
        pair = [q_in[j, s, :, g * LANES : (g + 1) * LANES] for g in range(2)]
        zero = jnp.zeros_like(pair[0])
        stack = [jnp.where(low, one, zero) for one in pair]
        stack += [jnp.where(low, zero, one) for one in pair]
        stack = jnp.concatenate(stack, axis=0)
        keys = kv_in[j, 4 * far : 4 * far + 4, 0].reshape(near_len, LANES)
        top = None
        for t, size in tiles(far):
            tile = lax.dot_general(
                keys[t - near_len * far :][:size], stack, TRANSPOSED, preferred_element_type=jnp.float32
            )
            score[at, t : t + size] = tile
            most = jnp.max(by_sublane(tile), axis=0)
            top = most if top is None else jnp.maximum(top, most)
        top = jnp.max(top, axis=0, keepdims=True)

        def finish():
            total = None
            for t, size in tiles(far):
                p = jnp.exp2((score[at, t : t + size] - top) * scale)
                score[at, t : t + size] = p
                more = jnp.sum(by_sublane(p), axis=0)
                total = more if total is None else total + more
            return top, jnp.sum(total, axis=0, keepdims=True)

        return finish

    def staged(j, order, far):
        found = []
        ahead = exponents(j, order[0], 0, far)
        for u in range(len(order)):
            now = ahead
            if u + 1 < len(order):
                ahead = exponents(j, order[u + 1], u + 1, far)
            found.append(now())
        return found

    def weigh(at, near, far):
        top = jnp.maximum(near[0], far[0])
        shrink = [jnp.exp2((one[0] - top) * scale) for one in (near, far)]
        inv = 1.0 / (near[1] * shrink[0] + far[1] * shrink[1])
        o = None
        for side in range(2):
            factor = shrink[side] * inv
            for t, size in tiles(side):
                p = (score[at, t : t + size] * factor).astype(jnp.bfloat16)
                more = jnp.dot(v_turned[:, t : t + size], p, preferred_element_type=jnp.float32)
                o = more if o is None else o + more
        o = o.T
        cut = [o[i * rows : (i + 1) * rows] for i in range(4)]
        one = jnp.where(low, cut[0], pltpu.roll(cut[1], HD, 1))
        two = jnp.where(low, pltpu.roll(cut[2], HD, 1), cut[3])
        return jnp.concatenate([one, two], axis=1).astype(jnp.bfloat16)

    def a_copy(j, s):
        there = jnp.where(s < 2, z_in, z_out) * 2 + s % 2
        c = y * pairs + j
        return remote(a_out.at[j, s], a_in.at[c], a_send.at[j, s], a_got.at[c], sp=there)

    def relay_first(j):
        beside_came(j)
        kv_across(j, beside).start()

        @pl.when(j < shared)
        def _():
            kv_downward(j, 0).start()

        kv_came(j, 2 + y)
        kv_across(j, 2 + y).start()

    def relay_last(j):
        kv_came(j, 3 - y)
        kv_across(j, 3 - y).start()

        @pl.when(j + 2 < pairs)
        def _():
            kv_across(j + 2, mine).start()

    def turn_values(j, far):
        at = slice(near_len * far, near_len * (far + 1))
        v_turned[:, at] = kv_in[j, 4 * far : 4 * far + 4, 1].reshape(near_len, LANES).T

    def attend(j, order, await_far, eager):
        turn_values(j, 0)
        near = staged(j, order, 0)
        await_far()
        turn_values(j, 1)
        ready = exponents(j, order[0], 0, 1)
        for u in range(len(order)):
            far = ready()
            if u + 1 < len(order):
                ready = exponents(j, order[u + 1], u + 1, 1)
            tile = weigh(u, near[u], far)
            if u + 1 < len(order):
                a_out[j, order[u]] = tile
                if eager:
                    a_copy(j, order[u]).start()
            else:
                a_in[y * pairs + j] = tile
        if not eager:
            for s in order[:-1]:
                a_copy(j, s).start()

    def a_came(c):
        remote(a_in.at[c], a_in.at[c], a_send.at[0, 0], a_got.at[c], sp=sibling).wait_recv()

    def a_ready(j):
        a_came((1 - y) * pairs + j)

        if j >= shared:
            @pl.when(outer)
            def _():
                a_came(y * pairs + j)

    width = w_ref.shape[1]

    def project(which, first=False, last=False):
        for shard in range(m):
            at = slice(shard * width, (shard + 1) * width)
            total = None if first else summed[:, at]
            for j in which:
                for c in (j, pairs + j):
                    more = jnp.dot(
                        a_in[c], w_all[shard, c * w_rows : (c + 1) * w_rows, :],
                        preferred_element_type=jnp.float32,
                    )
                    total = more if total is None else total + more
            if last:
                out_ref[:, at] = total.astype(jnp.bfloat16)
            else:
                summed[:, at] = total

    def w_ready(which):
        for j in which:
            for c in (j, pairs + j):
                w_came(x_other, c)

    def far_came(j):
        for s in range(4, 8):
            kv_came(j, s)

    @pl.when(inner)
    def _():
        for j in range(shared):
            relay_first(j)
            relay_last(j)

    def shared_pair(j, carry):
        @pl.when(inner)
        def _():
            @pl.when(j + shared < pairs)
            def _():
                relay_first(j + shared)
                relay_last(j + shared)

        @pl.when(outer)
        def _():
            low_came(j, 0)

        for i in range(shared):
            @pl.when(jnp.logical_and(inner, j == i))
            def _():
                pass_w(i)

        @pl.when(inner)
        def _():
            q_came(j, beside)

        def await_far():
            @pl.when(inner)
            def _():
                far_came(j)
                kv_downward(j, 1).start()

            @pl.when(outer)
            def _():
                low_came(j, 1)

        attend(j, [beside, mine], await_far, False)
        return carry

    def low_came(j, part):
        kv_downward(j, part).wait_recv()

    @pl.when(outer)
    def _():
        for j in range(shared):
            q_came(j, beside)
        for i in range(aside + 1):
            pass_w(i)

    lax.fori_loop(0, shared, shared_pair, 0)
    order = [2, 3, 1 - y, y]

    def late_pair(j, eager):
        for s in (1 - y, 2, 3):
            q_came(j, s)
        attend(j, order, lambda: far_came(j), eager)

    @pl.when(inner)
    def _():
        pass_w(aside)

    pass_w_aside(0)

    @pl.when(inner)
    def _():
        for j in range(shared, pairs - 1):
            late_pair(j, False)

    for i in range(1, aside):
        pass_w_aside(i)
    for i in range(aside + 1, direct - 2):
        pass_w(i)
    own_w.wait()
    remote(
        w_ref, w_all.at[core_peer], w_core.at[parts], w_got.at[core_peer, parts], dp=core_peer
    ).wait_recv()
    early = list(range(pairs - 2))
    w_ready(early)
    for j in early:
        a_ready(j)
    project(early, first=True)
    pass_w(direct - 2)

    @pl.when(inner)
    def _():
        late_pair(pairs - 1, True)

    pass_w(direct - 1)
    w_ready([pairs - 2])
    a_ready(pairs - 2)
    project([pairs - 2])
    w_ready([pairs - 1])
    a_ready(pairs - 1)
    project([pairs - 1], last=True)

    def sent(j, carry):
        k_aside(j).wait_send()
        v_aside(j).wait_send()
        q_aside(j).wait_send()

        @pl.when(outer)
        def _():
            for s in (mine, beside):
                kv_upward(j, s).wait_send()

                @pl.when(j >= shared)
                def _():
                    q_upward(j, s).wait_send()

        @pl.when(inner)
        def _():
            for s in range(4):
                kv_across(j, s).wait_send()

            @pl.when(j < shared)
            def _():
                for part in range(2):
                    kv_downward(j, part).wait_send()

            @pl.when(j >= shared)
            def _():
                for s in (2, 3):
                    a_copy(j, s).wait_send()

        @pl.when(jnp.logical_or(inner, j < shared))
        def _():
            a_copy(j, beside).wait_send()

        return carry

    lax.fori_loop(0, pairs, sent, 0)
    for i in range(direct):
        w_cross(i).wait_send()
    for i in range(aside):
        w_aside(i).wait_send()
    for c in range(parts):
        w_to_core(c).wait_send()
    w_own_core().wait_send()


def rotary_lanes(row_count):
    position = np.arange(row_count)[:, None]
    lane = np.arange(LANES)[None, :]
    place = np.where(lane % HD < HD // 2, position // GRID_W, position % GRID_W).astype(np.float32)
    quarter = HD // 4
    step = (lane % quarter).astype(np.float32)
    inv_freq = np.power(np.float32(rotary_base), -(np.float32(2.0) * step) / np.float32(HD // 2))
    angle = inv_freq.astype(np.float32) * place
    sign = np.where((lane // quarter) % 2 == 0, np.float32(-1.0), np.float32(1.0))
    return np.cos(angle).astype(np.float32), (np.sin(angle) * sign).astype(np.float32)


def on_device(queries, keys, values, q_gain, k_gain, w_out):
    n, m = lax.axis_size("sp"), lax.axis_size("dp")
    rows = queries.shape[2]
    kv_width = keys.shape[1] // 2
    pairs = kv_width // LANES
    if n != 8 or m != 4 or kv_width % LANES or pairs < 4 or rows % 32 or QH != 2 * KV:
        return on_device_plain(queries, keys, values, q_gain, k_gain, w_out)
    seq_len = n * rows
    cos_table, sin_table = rotary_lanes(seq_len)
    hbm = pl.BlockSpec(memory_space=pltpu.HBM)
    bf16, f32 = jnp.bfloat16, jnp.float32
    dma = pltpu.SemaphoreType.DMA
    parts = 2 * pairs
    mixed = pl.pallas_call(
        functools.partial(layer_kernel, m),
        out_shape=jax.ShapeDtypeStruct((rows, w_out.shape[1] * m), bf16),
        in_specs=[hbm] * 8,
        out_specs=pl.BlockSpec(memory_space=pltpu.VMEM),
        scratch_shapes=[
            pltpu.VMEM((rows, queries.shape[1]), bf16),
            pltpu.VMEM((rows, keys.shape[1]), bf16),
            pltpu.VMEM((1, HD), f32),
            pltpu.VMEM((1, HD), f32),
            pltpu.VMEM((rows, LANES), f32),
            pltpu.VMEM((rows, LANES), f32),
            pltpu.VMEM((pairs, rows, LANES), bf16),
            pltpu.VMEM((pairs, rows, 2 * LANES), bf16),
            pltpu.VMEM((pairs, 8, 2, rows, LANES), bf16),
            pltpu.VMEM((pairs, 4, rows, 2 * LANES), bf16),
            pltpu.VMEM((pairs, 4, rows, 2 * LANES), bf16),
            pltpu.VMEM((parts, rows, 2 * LANES), bf16),
            pltpu.VMEM((m, w_out.shape[0], w_out.shape[1]), bf16),
            pltpu.VMEM((4, seq_len, 4 * rows), f32),
            pltpu.VMEM((LANES, seq_len), bf16),
            pltpu.VMEM((rows, w_out.shape[1] * m), f32),
            dma((6,)), dma((pairs,)), dma((pairs,)), dma((pairs,)), dma((pairs,)),
            dma((pairs,)), dma((pairs,)), dma((pairs, 4)), dma((pairs, 4)), dma((pairs, 4)),
            dma((pairs, 4)), dma((pairs, 8)), dma((pairs, 2)), dma((pairs, 2)), dma((pairs, 4)),
            dma((parts,)),
            dma((parts,)), dma((pairs,)), dma((parts + 1,)), dma((m, parts + 1)), dma,
        ],
        compiler_params=pltpu.CompilerParams(
            collective_id=0, has_side_effects=True, vmem_limit_bytes=44 * 1024 * 1024
        ),
    )(
        *(
            pltpu.with_memory_space_constraint(x, pltpu.HBM)
            for x in (
                queries[0].T, keys[0].T, values[0].T, q_gain[None], k_gain[None],
                jnp.asarray(cos_table), jnp.asarray(sin_table), w_out,
            )
        )
    )
    return mixed[None]


def solution(mesh):
    placed = (
        P("dp", None, "sp"),
        P("dp", None, "sp"),
        P("dp", None, "sp"),
        P(),
        P(),
        P(None, "dp"),
    )
    return jax.shard_map(
        on_device, mesh=mesh, in_specs=placed, out_specs=P("dp", "sp", None), check_vma=False
    )
```

```python
import functools

import jax
import jax.numpy as jnp
import numpy as np
from jax import lax
from jax.experimental import pallas as pl
from jax.experimental.pallas import tpu as pltpu
from jax.sharding import PartitionSpec as P

HD = 64
QH = 32
KV = 16
GRID_W = 64


epsilon = 1e-06
rotary_base = 10000.0
block_count = 8


def swapped(block, axis, apart):
    count = lax.axis_size(axis)
    route = []
    for low in range(count):
        high = low | 1 << apart
        if high != low and high < count:
            route += [(low, high), (high, low)]
    return lax.ppermute(block, axis, route)


def rotary_tables(first_row, row_count):
    position = first_row + lax.iota(jnp.int32, row_count)
    grid_row = (position // GRID_W).astype(jnp.float32)
    grid_col = (position % GRID_W).astype(jnp.float32)
    quarter = HD // 4
    inv_freq = rotary_base ** (-(2.0 * lax.iota(jnp.float32, quarter)) / (HD // 2))
    row_angle = inv_freq[:, None] * grid_row[None, :]
    col_angle = inv_freq[:, None] * grid_col[None, :]
    cos_table = jnp.concatenate(
        [jnp.cos(row_angle), jnp.cos(row_angle), jnp.cos(col_angle), jnp.cos(col_angle)], axis=0
    )
    sin_table = jnp.concatenate(
        [jnp.sin(row_angle), jnp.sin(row_angle), jnp.sin(col_angle), jnp.sin(col_angle)], axis=0
    )
    return (cos_table, sin_table)


def normalize_turn(field, gain, cos_table, sin_table):
    head_count = field.shape[0] // HD
    values_f = field.astype(jnp.float32).reshape(head_count, HD, field.shape[1])
    normed = (
        values_f
        * lax.rsqrt(jnp.mean(values_f * values_f, axis=1, keepdims=True) + epsilon)
        * gain[None, :, None]
    )
    quarter = HD // 4
    quarters_of = normed.reshape(head_count, 4, quarter, field.shape[1])
    turned = jnp.concatenate(
        [-quarters_of[:, 1], quarters_of[:, 0], -quarters_of[:, 3], quarters_of[:, 2]], axis=1
    )
    return (normed * cos_table[None] + turned * sin_table[None]).astype(jnp.bfloat16)


def attention_heads(query_heads, key_heads, value_heads, seq_len):
    kv_local = key_heads.shape[0]
    group_local = query_heads.shape[0] // kv_local
    query_split = query_heads.reshape(kv_local, group_local, HD, seq_len)
    score_scale = HD ** (-0.5)
    block_rows = seq_len // block_count

    def one_block(block_index, result):
        row_start = block_index * block_rows
        query_block = lax.dynamic_slice_in_dim(query_split, row_start, block_rows, 3)
        scores = (
            jnp.einsum("hgdq,hdk->hgqk", query_block, key_heads, preferred_element_type=jnp.float32)
            * score_scale
        )
        row_max = jnp.max(scores, axis=-1, keepdims=True)
        weights = jnp.exp(scores - row_max)
        weights = (weights / jnp.sum(weights, axis=-1, keepdims=True)).astype(jnp.bfloat16)
        attended = jnp.einsum(
            "hgqk,hdk->hgdq", weights, value_heads, preferred_element_type=jnp.float32
        )
        return lax.dynamic_update_slice_in_dim(result, attended.astype(jnp.bfloat16), row_start, 3)

    result = jnp.zeros(query_split.shape, jnp.bfloat16)
    result = lax.fori_loop(0, block_count, one_block, result)
    return result.reshape(query_heads.shape)


def on_device_plain(queries, keys, values, q_gain, k_gain, w_out):
    sp_count = lax.axis_size("sp")
    tok_rows = queries.shape[2]
    seq_len = tok_rows * sp_count
    cos_table, sin_table = rotary_tables(lax.axis_index("sp") * tok_rows, tok_rows)
    query_rot = normalize_turn(queries[0], q_gain, cos_table, sin_table)
    key_rot = normalize_turn(keys[0], k_gain, cos_table, sin_table)
    value_rows = values[0].reshape(KV, HD, tok_rows)
    query_heads = lax.all_to_all(query_rot, "sp", split_axis=0, concat_axis=2, tiled=True)
    share_count = max(sp_count // KV, 1)
    part_rows = tok_rows // share_count
    key_cut = (
        key_rot.reshape(KV, HD, share_count, part_rows)
        .transpose(0, 2, 1, 3)
        .reshape(KV * share_count, HD, part_rows)
    )
    value_cut = (
        value_rows.reshape(KV, HD, share_count, part_rows)
        .transpose(0, 2, 1, 3)
        .reshape(KV * share_count, HD, part_rows)
    )
    key_got, value_got = (
        lax.all_to_all(key_cut, "sp", split_axis=0, concat_axis=2, tiled=True),
        lax.all_to_all(value_cut, "sp", split_axis=0, concat_axis=2, tiled=True),
    )
    kv_local = key_got.shape[0]
    key_got = key_got.reshape(kv_local, HD, sp_count, part_rows)
    value_got = value_got.reshape(kv_local, HD, sp_count, part_rows)
    for bit_index in range(share_count.bit_length() - 1):
        key_other, value_other = swapped((key_got, value_got), "sp", bit_index)
        key_got = jnp.concatenate([key_got, key_other], axis=3)
        value_got = jnp.concatenate([value_got, value_other], axis=3)
    key_heads = key_got.reshape(kv_local, HD, seq_len)
    value_heads = value_got.reshape(kv_local, HD, seq_len)
    attended = attention_heads(query_heads, key_heads, value_heads, seq_len)
    token_heads = lax.all_to_all(attended, "sp", split_axis=2, concat_axis=0, tiled=True)
    token_rows = token_heads.reshape(QH * HD, tok_rows)
    product = lax.dot_general(
        token_rows,
        lax.all_gather(w_out, "dp", axis=1, tiled=True),
        (((0,), (0,)), ((), ())),
        preferred_element_type=jnp.float32,
    )
    mixed_rows = product.astype(jnp.bfloat16)
    return mixed_rows[None]


MESH = pl.DeviceIdType.MESH
LOG2E = 1.4426950408889634
LANES = 128
TRANSPOSED = (((1,), (1,)), ((), ()))


def layer_kernel(
    m, q_ref, k_ref, v_ref, qg_ref, kg_ref, cos_ref, sin_ref, w_ref, out_ref,
    q_raw, k_raw, q_gain_in, k_gain_in, cos_in, sin_in, k_out, q_out, kv_in, q_in, a_out, a_in,
    w_all, score, v_turned, summed,
    load, v_own, k_side, v_side, q_side, k_got, v_got, q_got, kv_up, q_up, kv_mid, kv_got, kv_low, kv_low_got,
    a_send, a_got, w_x, w_y, w_core, w_got, w_local,
):
    me = lax.axis_index("sp")
    dp = lax.axis_index("dp")
    z, y = me // 2, me % 2
    half = z // 2
    z_in, z_out = 1 + half, 3 * half
    inner = z == z_in
    outer = jnp.logical_not(inner)
    base = jnp.where(inner, 0, 2)
    mine, beside = base + y, base + 1 - y
    sibling = z * 2 + 1 - y
    in_same = z_in * 2 + y
    across = (3 - z_in) * 2 + y
    core = lax.rem(dp, 2)
    x_at = dp // 2
    x_peer = (1 - x_at) * 2 + core
    core_peer = x_at * 2 + 1 - core
    x_other = (1 - x_at) * 2 + 1 - core
    rows = k_raw.shape[0]
    pairs = kv_in.shape[0]
    parts = 2 * pairs
    shared = pairs // 2
    w_rows = w_ref.shape[0] // parts

    barrier = pltpu.get_barrier_semaphore()

    def greet(**there):
        pl.semaphore_signal(barrier, inc=1, device_id=there, device_id_type=MESH)

    greet(sp=sibling)
    greet(dp=x_peer)
    greet(dp=core_peer)
    z_other = jnp.where(inner, z_out, z_in)
    greet(sp=z_other * 2 + y)
    greet(sp=z_other * 2 + 1 - y)

    @pl.when(inner)
    def _():
        greet(sp=across)

    def kv_lanes(side, j):
        return pl.ds(pl.multiple_of((side * pairs + j) * LANES, LANES), LANES)

    first = pl.multiple_of(me * rows, rows)
    loads = [
        pltpu.make_async_copy(k_ref, k_raw, load.at[0]),
        pltpu.make_async_copy(cos_ref.at[pl.ds(first, rows)], cos_in, load.at[1]),
        pltpu.make_async_copy(sin_ref.at[pl.ds(first, rows)], sin_in, load.at[2]),
        pltpu.make_async_copy(kg_ref, k_gain_in, load.at[3]),
        pltpu.make_async_copy(qg_ref, q_gain_in, load.at[4]),
        pltpu.make_async_copy(q_ref, q_raw, load.at[5]),
    ]
    for one in loads:
        one.start()

    def own_values(j):
        return pltpu.make_async_copy(
            v_ref.at[:, kv_lanes(y, j)], kv_in.at[j, mine, 1], v_own.at[j]
        )

    for j in range(pairs):
        own_values(j).start()
    own_w = pltpu.make_async_copy(w_ref, w_all.at[dp], w_local)
    own_w.start()

    def remote(src, dst, sent, got, **there):
        return pltpu.make_async_remote_copy(
            src_ref=src, dst_ref=dst, send_sem=sent, recv_sem=got,
            device_id=there, device_id_type=MESH,
        )

    def k_aside(j, to=None):
        to = mine if to is None else to
        return remote(k_out.at[j], kv_in.at[j, to, 0], k_side.at[j], k_got.at[j], sp=sibling)

    def v_aside(j, to=None):
        to = mine if to is None else to
        return remote(
            v_ref.at[:, kv_lanes(1 - y, j)], kv_in.at[j, to, 1], v_side.at[j], v_got.at[j],
            sp=sibling,
        )

    def q_aside(j, to=None):
        to = mine if to is None else to
        return remote(q_out.at[j], q_in.at[j, to], q_side.at[j], q_got.at[j, to], sp=sibling)

    def kv_upward(j, s):
        return remote(
            kv_in.at[j, s], kv_in.at[j, s], kv_up.at[j, s], kv_got.at[j, s], sp=in_same
        )

    def q_upward(j, s):
        return remote(q_in.at[j, s], q_in.at[j, s], q_up.at[j, s], q_got.at[j, s], sp=in_same)

    def kv_across(j, s):
        return remote(
            kv_in.at[j, s], kv_in.at[j, 4 + s], kv_mid.at[j, s], kv_got.at[j, 4 + s], sp=across
        )

    out_same = z_out * 2 + y

    def kv_downward(j, part):
        at = pl.ds(4 * part, 2 + 2 * part)
        return remote(
            kv_in.at[j, at], kv_in.at[j, at], kv_low.at[j, part], kv_low_got.at[j, part],
            sp=out_same,
        )

    def kv_came(j, s):
        remote(
            kv_in.at[j, s], kv_in.at[j, s], kv_up.at[j, 0], kv_got.at[j, s], sp=across
        ).wait_recv()

    def q_came(j, s):
        remote(q_in.at[j, s], q_in.at[j, s], q_up.at[j, 0], q_got.at[j, s], sp=sibling).wait_recv()

    def w_piece(ref, c):
        return ref.at[pl.ds(pl.multiple_of(c * w_rows, w_rows), w_rows)]

    def w_held(shard, c):
        return w_all.at[shard, pl.ds(pl.multiple_of(c * w_rows, w_rows), w_rows)]

    aside = pairs // 2
    direct = parts - aside

    def part_at(i):
        if i < aside:
            return y * pairs + i
        return (i % 2) * pairs + (aside + i) // 2

    def w_cross(i):
        c = part_at(i)
        return remote(w_piece(w_ref, c), w_held(dp, c), w_x.at[i], w_got.at[dp, c], dp=x_peer)

    def w_own_core():
        return remote(w_ref, w_all.at[dp], w_core.at[parts], w_got.at[dp, parts], dp=core_peer)

    def w_to_core(c):
        return remote(
            w_held(x_peer, c), w_held(x_peer, c), w_core.at[c], w_got.at[x_peer, c], dp=core_peer
        )

    def w_aside(i):
        c = part_at(i)
        return remote(
            w_held(x_peer, c), w_held(x_peer, c), w_y.at[i], w_got.at[x_peer, c], sp=sibling
        )

    def w_came(shard, c):
        remote(
            w_held(shard, c), w_held(shard, c), w_y.at[0], w_got.at[shard, c], dp=core_peer
        ).wait_recv()

    def pass_w(i):
        c = part_at(i)
        w_came(x_peer, c)
        w_to_core(c).start()
        if i < aside:
            w_aside(i).start()

    def pass_w_aside(i):
        c = (1 - y) * pairs + i
        w_came(x_peer, c)
        w_to_core(c).start()

    lane = lax.broadcasted_iota(jnp.int32, (rows, LANES), 1)
    low = lane < HD
    even = (lane // (HD // 4)) % 2 == 0

    def turn(tile, gain):
        u = tile.astype(jnp.float32)
        square = u * u
        sum_low = jnp.sum(jnp.where(low, square, 0.0), axis=1, keepdims=True)
        sum_high = jnp.sum(jnp.where(low, 0.0, square), axis=1, keepdims=True)
        inverse = jnp.where(
            low, lax.rsqrt(sum_low * (1.0 / HD) + epsilon), lax.rsqrt(sum_high * (1.0 / HD) + epsilon)
        )
        normed = u * inverse * gain
        part = HD // 4
        turned = jnp.where(even, pltpu.roll(normed, LANES - part, 1), pltpu.roll(normed, part, 1))
        return normed * cos_in[...] + turned * sin_in[...]

    def crossed(one, two):
        return (
            jnp.where(low, one, pltpu.roll(two, HD, 1)),
            jnp.where(low, pltpu.roll(one, HD, 1), two),
        )

    def turn_keys(j, side):
        return turn(k_raw[:, kv_lanes(side, j)], k_gain).astype(jnp.bfloat16)

    def turn_queries(j, side):
        at = (side * pairs + j) * 2 * LANES
        natural = [
            turn(q_raw[:, pl.ds(pl.multiple_of(at + i * LANES, LANES), LANES)], q_gain)
            for i in range(2)
        ]
        return jnp.concatenate(crossed(*natural), axis=1).astype(jnp.bfloat16)

    for one in loads[:5]:
        one.wait()
    q_gain, k_gain = (
        jnp.concatenate([g[...], g[...]], axis=1) for g in (q_gain_in, k_gain_in)
    )

    def key_step(j):
        k_out[j] = turn_keys(j, 1 - y)
        kv_in[j, mine, 0] = turn_keys(j, y)

    def query_step(j):
        q_out[j] = turn_queries(j, 1 - y)
        q_in[j, mine] = turn_queries(j, y)

    key_step(0)
    pl.semaphore_wait(barrier, jnp.where(inner, 6, 5))

    def key_send(j, carry):
        v_aside(j).start()

        @pl.when(j > 0)
        def _():
            key_step(j)

        k_aside(j).start()
        own_values(j).wait()

        @pl.when(jnp.logical_and(outer, j < 2))
        def _():
            kv_upward(j, mine).start()

        @pl.when(jnp.logical_and(inner, j < 2))
        def _():
            kv_across(j, mine).start()

        return carry

    def query_send(j, carry):
        query_step(j)
        q_aside(j).start()
        return carry

    w_cross(0).start()
    w_cross(1).start()
    lax.fori_loop(0, pairs, key_send, 0)
    loads[5].wait()
    lax.fori_loop(0, pairs, query_send, 0)
    for i in range(2, direct):
        w_cross(i).start()
    w_own_core().start()

    def beside_came(j):
        k_aside(j, beside).wait_recv()
        v_aside(j, beside).wait_recv()

    @pl.when(outer)
    def _():
        def kv(j):
            if j > 1:
                kv_upward(j, mine).start()
            beside_came(j)
            kv_upward(j, beside).start()

        def query(j):
            if j:
                q_upward(j, mine).start()
            q_came(j, beside)
            q_upward(j, beside).start()

        for j in range(pairs):
            kv(j)
        for j in range(shared, pairs):
            query(j)

    scale = HD ** (-0.5) * LOG2E
    step = 2 * LANES
    seq_len = 8 * rows
    near_len = 4 * rows

    def tiles(far):
        start = near_len * far
        stop = start + near_len
        return [(t, min(step, stop - t)) for t in range(start, stop, step)]

    def by_sublane(tile):
        return tile.reshape(tile.shape[0] // 8, 8, tile.shape[1])

    def exponents(j, s, at, far):
        pair = [q_in[j, s, :, g * LANES : (g + 1) * LANES] for g in range(2)]
        zero = jnp.zeros_like(pair[0])
        stack = [jnp.where(low, one, zero) for one in pair]
        stack += [jnp.where(low, zero, one) for one in pair]
        stack = jnp.concatenate(stack, axis=0)
        keys = kv_in[j, 4 * far : 4 * far + 4, 0].reshape(near_len, LANES)
        top = None
        for t, size in tiles(far):
            tile = lax.dot_general(
                keys[t - near_len * far :][:size], stack, TRANSPOSED, preferred_element_type=jnp.float32
            )
            score[at, t : t + size] = tile
            most = jnp.max(by_sublane(tile), axis=0)
            top = most if top is None else jnp.maximum(top, most)
        top = jnp.max(top, axis=0, keepdims=True)

        def finish():
            total = None
            for t, size in tiles(far):
                p = jnp.exp2((score[at, t : t + size] - top) * scale)
                score[at, t : t + size] = p
                more = jnp.sum(by_sublane(p), axis=0)
                total = more if total is None else total + more
            return top, jnp.sum(total, axis=0, keepdims=True)

        return finish

    def staged(j, order, far):
        found = []
        ahead = exponents(j, order[0], 0, far)
        for u in range(len(order)):
            now = ahead
            if u + 1 < len(order):
                ahead = exponents(j, order[u + 1], u + 1, far)
            found.append(now())
        return found

    def weigh(at, near, far):
        top = jnp.maximum(near[0], far[0])
        shrink = [jnp.exp2((one[0] - top) * scale) for one in (near, far)]
        inv = 1.0 / (near[1] * shrink[0] + far[1] * shrink[1])
        o = None
        for side in range(2):
            factor = shrink[side] * inv
            for t, size in tiles(side):
                p = (score[at, t : t + size] * factor).astype(jnp.bfloat16)
                more = jnp.dot(v_turned[:, t : t + size], p, preferred_element_type=jnp.float32)
                o = more if o is None else o + more
        o = o.T
        cut = [o[i * rows : (i + 1) * rows] for i in range(4)]
        one = jnp.where(low, cut[0], pltpu.roll(cut[1], HD, 1))
        two = jnp.where(low, pltpu.roll(cut[2], HD, 1), cut[3])
        return jnp.concatenate([one, two], axis=1).astype(jnp.bfloat16)

    def a_copy(j, s):
        there = jnp.where(s < 2, z_in, z_out) * 2 + s % 2
        c = y * pairs + j
        return remote(a_out.at[j, s], a_in.at[c], a_send.at[j, s], a_got.at[c], sp=there)

    def relay_first(j):
        @pl.when(j == pairs - 1)
        def _():
            kv_across(j, mine).start()

        beside_came(j)
        kv_across(j, beside).start()

        @pl.when(j < shared)
        def _():
            kv_downward(j, 0).start()

        kv_came(j, 2 + y)
        kv_across(j, 2 + y).start()

    def relay_last(j):
        kv_came(j, 3 - y)
        kv_across(j, 3 - y).start()

        @pl.when(j + 3 < pairs)
        def _():
            kv_across(j + 2, mine).start()

    def turn_values(j, far):
        at = slice(near_len * far, near_len * (far + 1))
        v_turned[:, at] = kv_in[j, 4 * far : 4 * far + 4, 1].reshape(near_len, LANES).T

    def attend(j, order, await_far, eager):
        turn_values(j, 0)
        near = staged(j, order, 0)
        await_far()
        turn_values(j, 1)
        ready = exponents(j, order[0], 0, 1)
        for u in range(len(order)):
            far = ready()
            if u + 1 < len(order):
                ready = exponents(j, order[u + 1], u + 1, 1)
            tile = weigh(u, near[u], far)
            if u + 1 < len(order):
                a_out[j, order[u]] = tile
                if eager:
                    a_copy(j, order[u]).start()
            else:
                a_in[y * pairs + j] = tile
        if not eager:
            for s in order[:-1]:
                a_copy(j, s).start()

    def a_came(c):
        remote(a_in.at[c], a_in.at[c], a_send.at[0, 0], a_got.at[c], sp=sibling).wait_recv()

    def a_ready(j):
        a_came((1 - y) * pairs + j)

        if j >= shared:
            @pl.when(outer)
            def _():
                a_came(y * pairs + j)

    width = w_ref.shape[1]

    def project(which, first=False, last=False):
        for shard in range(m):
            at = slice(shard * width, (shard + 1) * width)
            total = None if first else summed[:, at]
            for j in which:
                for c in (j, pairs + j):
                    more = jnp.dot(
                        a_in[c], w_all[shard, c * w_rows : (c + 1) * w_rows, :],
                        preferred_element_type=jnp.float32,
                    )
                    total = more if total is None else total + more
            if last:
                out_ref[:, at] = total.astype(jnp.bfloat16)
            else:
                summed[:, at] = total

    def w_ready(which):
        for j in which:
            for c in (j, pairs + j):
                w_came(x_other, c)

    def far_came(j):
        for s in range(4, 8):
            kv_came(j, s)

    @pl.when(inner)
    def _():
        for j in range(shared):
            relay_first(j)
            relay_last(j)

    def shared_pair(j, carry):
        @pl.when(inner)
        def _():
            @pl.when(j + shared < pairs)
            def _():
                relay_first(j + shared)
                relay_last(j + shared)

        @pl.when(outer)
        def _():
            low_came(j, 0)

        for i in range(shared):
            @pl.when(jnp.logical_and(inner, j == i))
            def _():
                pass_w(i)

        @pl.when(inner)
        def _():
            q_came(j, beside)

        def await_far():
            @pl.when(inner)
            def _():
                far_came(j)
                kv_downward(j, 1).start()

            @pl.when(outer)
            def _():
                low_came(j, 1)

        attend(j, [beside, mine], await_far, False)
        return carry

    def low_came(j, part):
        kv_downward(j, part).wait_recv()

    @pl.when(outer)
    def _():
        for j in range(shared):
            q_came(j, beside)
        for i in range(aside + 1):
            pass_w(i)

    lax.fori_loop(0, shared, shared_pair, 0)
    order = [2, 3, 1 - y, y]

    def late_pair(j, eager, await_far=None):
        for s in (1 - y, 2, 3):
            q_came(j, s)
        attend(j, order, await_far or (lambda: far_came(j)), eager)

    early = list(range(pairs - 2))

    def middle_passes():
        for i in range(aside):
            pass_w_aside(i)
        for i in range(aside + 1, direct - 2):
            pass_w(i)
        own_w.wait()
        remote(
            w_ref, w_all.at[core_peer], w_core.at[parts], w_got.at[core_peer, parts], dp=core_peer
        ).wait_recv()

    def early_project():
        w_ready(early)
        for j in early:
            a_ready(j)
        project(early, first=True)
        pass_w(direct - 2)

    @pl.when(inner)
    def _():
        pass_w(aside)
        for j in range(shared, pairs - 1):
            late_pair(j, False)
        middle_passes()

        def await_last():
            early_project()
            far_came(pairs - 1)

        late_pair(pairs - 1, True, await_last)

    @pl.when(outer)
    def _():
        middle_passes()
        early_project()

    pass_w(direct - 1)
    w_ready([pairs - 2])
    a_ready(pairs - 2)
    project([pairs - 2])
    w_ready([pairs - 1])
    a_ready(pairs - 1)
    project([pairs - 1], last=True)

    def sent(j, carry):
        k_aside(j).wait_send()
        v_aside(j).wait_send()
        q_aside(j).wait_send()

        @pl.when(outer)
        def _():
            for s in (mine, beside):
                kv_upward(j, s).wait_send()

                @pl.when(j >= shared)
                def _():
                    q_upward(j, s).wait_send()

        @pl.when(inner)
        def _():
            for s in range(4):
                kv_across(j, s).wait_send()

            @pl.when(j < shared)
            def _():
                for part in range(2):
                    kv_downward(j, part).wait_send()

            @pl.when(j >= shared)
            def _():
                for s in (2, 3):
                    a_copy(j, s).wait_send()

        @pl.when(jnp.logical_or(inner, j < shared))
        def _():
            a_copy(j, beside).wait_send()

        return carry

    lax.fori_loop(0, pairs, sent, 0)
    for i in range(direct):
        w_cross(i).wait_send()
    for i in range(aside):
        w_aside(i).wait_send()
    for c in range(parts):
        w_to_core(c).wait_send()
    w_own_core().wait_send()


def rotary_lanes(row_count):
    position = np.arange(row_count)[:, None]
    lane = np.arange(LANES)[None, :]
    place = np.where(lane % HD < HD // 2, position // GRID_W, position % GRID_W).astype(np.float32)
    quarter = HD // 4
    step = (lane % quarter).astype(np.float32)
    inv_freq = np.power(np.float32(rotary_base), -(np.float32(2.0) * step) / np.float32(HD // 2))
    angle = inv_freq.astype(np.float32) * place
    sign = np.where((lane // quarter) % 2 == 0, np.float32(-1.0), np.float32(1.0))
    return np.cos(angle).astype(np.float32), (np.sin(angle) * sign).astype(np.float32)


def on_device(queries, keys, values, q_gain, k_gain, w_out):
    n, m = lax.axis_size("sp"), lax.axis_size("dp")
    rows = queries.shape[2]
    kv_width = keys.shape[1] // 2
    pairs = kv_width // LANES
    if n != 8 or m != 4 or kv_width % LANES or pairs < 4 or rows % 32 or QH != 2 * KV:
        return on_device_plain(queries, keys, values, q_gain, k_gain, w_out)
    seq_len = n * rows
    cos_table, sin_table = rotary_lanes(seq_len)
    hbm = pl.BlockSpec(memory_space=pltpu.HBM)
    bf16, f32 = jnp.bfloat16, jnp.float32
    dma = pltpu.SemaphoreType.DMA
    parts = 2 * pairs
    mixed = pl.pallas_call(
        functools.partial(layer_kernel, m),
        out_shape=jax.ShapeDtypeStruct((rows, w_out.shape[1] * m), bf16),
        in_specs=[hbm] * 8,
        out_specs=pl.BlockSpec(memory_space=pltpu.VMEM),
        scratch_shapes=[
            pltpu.VMEM((rows, queries.shape[1]), bf16),
            pltpu.VMEM((rows, keys.shape[1]), bf16),
            pltpu.VMEM((1, HD), f32),
            pltpu.VMEM((1, HD), f32),
            pltpu.VMEM((rows, LANES), f32),
            pltpu.VMEM((rows, LANES), f32),
            pltpu.VMEM((pairs, rows, LANES), bf16),
            pltpu.VMEM((pairs, rows, 2 * LANES), bf16),
            pltpu.VMEM((pairs, 8, 2, rows, LANES), bf16),
            pltpu.VMEM((pairs, 4, rows, 2 * LANES), bf16),
            pltpu.VMEM((pairs, 4, rows, 2 * LANES), bf16),
            pltpu.VMEM((parts, rows, 2 * LANES), bf16),
            pltpu.VMEM((m, w_out.shape[0], w_out.shape[1]), bf16),
            pltpu.VMEM((4, seq_len, 4 * rows), f32),
            pltpu.VMEM((LANES, seq_len), bf16),
            pltpu.VMEM((rows, w_out.shape[1] * m), f32),
            dma((6,)), dma((pairs,)), dma((pairs,)), dma((pairs,)), dma((pairs,)),
            dma((pairs,)), dma((pairs,)), dma((pairs, 4)), dma((pairs, 4)), dma((pairs, 4)),
            dma((pairs, 4)), dma((pairs, 8)), dma((pairs, 2)), dma((pairs, 2)), dma((pairs, 4)),
            dma((parts,)),
            dma((parts,)), dma((pairs,)), dma((parts + 1,)), dma((m, parts + 1)), dma,
        ],
        compiler_params=pltpu.CompilerParams(
            collective_id=0, has_side_effects=True, vmem_limit_bytes=44 * 1024 * 1024
        ),
    )(
        *(
            pltpu.with_memory_space_constraint(x, pltpu.HBM)
            for x in (
                queries[0].T, keys[0].T, values[0].T, q_gain[None], k_gain[None],
                jnp.asarray(cos_table), jnp.asarray(sin_table), w_out,
            )
        )
    )
    return mixed[None]


def solution(mesh):
    placed = (
        P("dp", None, "sp"),
        P("dp", None, "sp"),
        P("dp", None, "sp"),
        P(),
        P(),
        P(None, "dp"),
    )
    return jax.shard_map(
        on_device, mesh=mesh, in_specs=placed, out_specs=P("dp", "sp", None), check_vma=False
    )
```

```python
import functools

import jax
import jax.numpy as jnp
import numpy as np
from jax import lax
from jax.experimental import pallas as pl
from jax.experimental.pallas import tpu as pltpu
from jax.sharding import PartitionSpec as P

HD = 64
QH = 32
KV = 16
GRID_W = 64


epsilon = 1e-06
rotary_base = 10000.0
block_count = 8


def swapped(block, axis, apart):
    count = lax.axis_size(axis)
    route = []
    for low in range(count):
        high = low | 1 << apart
        if high != low and high < count:
            route += [(low, high), (high, low)]
    return lax.ppermute(block, axis, route)


def rotary_tables(first_row, row_count):
    position = first_row + lax.iota(jnp.int32, row_count)
    grid_row = (position // GRID_W).astype(jnp.float32)
    grid_col = (position % GRID_W).astype(jnp.float32)
    quarter = HD // 4
    inv_freq = rotary_base ** (-(2.0 * lax.iota(jnp.float32, quarter)) / (HD // 2))
    row_angle = inv_freq[:, None] * grid_row[None, :]
    col_angle = inv_freq[:, None] * grid_col[None, :]
    cos_table = jnp.concatenate(
        [jnp.cos(row_angle), jnp.cos(row_angle), jnp.cos(col_angle), jnp.cos(col_angle)], axis=0
    )
    sin_table = jnp.concatenate(
        [jnp.sin(row_angle), jnp.sin(row_angle), jnp.sin(col_angle), jnp.sin(col_angle)], axis=0
    )
    return (cos_table, sin_table)


def normalize_turn(field, gain, cos_table, sin_table):
    head_count = field.shape[0] // HD
    values_f = field.astype(jnp.float32).reshape(head_count, HD, field.shape[1])
    normed = (
        values_f
        * lax.rsqrt(jnp.mean(values_f * values_f, axis=1, keepdims=True) + epsilon)
        * gain[None, :, None]
    )
    quarter = HD // 4
    quarters_of = normed.reshape(head_count, 4, quarter, field.shape[1])
    turned = jnp.concatenate(
        [-quarters_of[:, 1], quarters_of[:, 0], -quarters_of[:, 3], quarters_of[:, 2]], axis=1
    )
    return (normed * cos_table[None] + turned * sin_table[None]).astype(jnp.bfloat16)


def attention_heads(query_heads, key_heads, value_heads, seq_len):
    kv_local = key_heads.shape[0]
    group_local = query_heads.shape[0] // kv_local
    query_split = query_heads.reshape(kv_local, group_local, HD, seq_len)
    score_scale = HD ** (-0.5)
    block_rows = seq_len // block_count

    def one_block(block_index, result):
        row_start = block_index * block_rows
        query_block = lax.dynamic_slice_in_dim(query_split, row_start, block_rows, 3)
        scores = (
            jnp.einsum("hgdq,hdk->hgqk", query_block, key_heads, preferred_element_type=jnp.float32)
            * score_scale
        )
        row_max = jnp.max(scores, axis=-1, keepdims=True)
        weights = jnp.exp(scores - row_max)
        weights = (weights / jnp.sum(weights, axis=-1, keepdims=True)).astype(jnp.bfloat16)
        attended = jnp.einsum(
            "hgqk,hdk->hgdq", weights, value_heads, preferred_element_type=jnp.float32
        )
        return lax.dynamic_update_slice_in_dim(result, attended.astype(jnp.bfloat16), row_start, 3)

    result = jnp.zeros(query_split.shape, jnp.bfloat16)
    result = lax.fori_loop(0, block_count, one_block, result)
    return result.reshape(query_heads.shape)


def on_device_plain(queries, keys, values, q_gain, k_gain, w_out):
    sp_count = lax.axis_size("sp")
    tok_rows = queries.shape[2]
    seq_len = tok_rows * sp_count
    cos_table, sin_table = rotary_tables(lax.axis_index("sp") * tok_rows, tok_rows)
    query_rot = normalize_turn(queries[0], q_gain, cos_table, sin_table)
    key_rot = normalize_turn(keys[0], k_gain, cos_table, sin_table)
    value_rows = values[0].reshape(KV, HD, tok_rows)
    query_heads = lax.all_to_all(query_rot, "sp", split_axis=0, concat_axis=2, tiled=True)
    share_count = max(sp_count // KV, 1)
    part_rows = tok_rows // share_count
    key_cut = (
        key_rot.reshape(KV, HD, share_count, part_rows)
        .transpose(0, 2, 1, 3)
        .reshape(KV * share_count, HD, part_rows)
    )
    value_cut = (
        value_rows.reshape(KV, HD, share_count, part_rows)
        .transpose(0, 2, 1, 3)
        .reshape(KV * share_count, HD, part_rows)
    )
    key_got, value_got = (
        lax.all_to_all(key_cut, "sp", split_axis=0, concat_axis=2, tiled=True),
        lax.all_to_all(value_cut, "sp", split_axis=0, concat_axis=2, tiled=True),
    )
    kv_local = key_got.shape[0]
    key_got = key_got.reshape(kv_local, HD, sp_count, part_rows)
    value_got = value_got.reshape(kv_local, HD, sp_count, part_rows)
    for bit_index in range(share_count.bit_length() - 1):
        key_other, value_other = swapped((key_got, value_got), "sp", bit_index)
        key_got = jnp.concatenate([key_got, key_other], axis=3)
        value_got = jnp.concatenate([value_got, value_other], axis=3)
    key_heads = key_got.reshape(kv_local, HD, seq_len)
    value_heads = value_got.reshape(kv_local, HD, seq_len)
    attended = attention_heads(query_heads, key_heads, value_heads, seq_len)
    token_heads = lax.all_to_all(attended, "sp", split_axis=2, concat_axis=0, tiled=True)
    token_rows = token_heads.reshape(QH * HD, tok_rows)
    product = lax.dot_general(
        token_rows,
        lax.all_gather(w_out, "dp", axis=1, tiled=True),
        (((0,), (0,)), ((), ())),
        preferred_element_type=jnp.float32,
    )
    mixed_rows = product.astype(jnp.bfloat16)
    return mixed_rows[None]


MESH = pl.DeviceIdType.MESH
LOG2E = 1.4426950408889634
LANES = 128
TRANSPOSED = (((1,), (1,)), ((), ()))


def layer_kernel(
    m, q_ref, k_ref, v_ref, qg_ref, kg_ref, cos_ref, sin_ref, w_ref, out_ref,
    q_raw, k_raw, q_gain_in, k_gain_in, cos_in, sin_in, k_out, q_out, kv_in, q_in, a_out, a_in,
    w_all, score, v_turned, summed,
    load, v_own, k_side, v_side, q_side, k_got, v_got, q_got, kv_up, q_up, kv_mid, kv_got, kv_low, kv_low_got, v_mid, v_far,
    a_send, a_got, w_x, w_y, w_core, w_got, w_local,
):
    me = lax.axis_index("sp")
    dp = lax.axis_index("dp")
    z, y = me // 2, me % 2
    half = z // 2
    z_in, z_out = 1 + half, 3 * half
    inner = z == z_in
    outer = jnp.logical_not(inner)
    base = jnp.where(inner, 0, 2)
    mine, beside = base + y, base + 1 - y
    sibling = z * 2 + 1 - y
    in_same = z_in * 2 + y
    across = (3 - z_in) * 2 + y
    core = lax.rem(dp, 2)
    x_at = dp // 2
    x_peer = (1 - x_at) * 2 + core
    core_peer = x_at * 2 + 1 - core
    x_other = (1 - x_at) * 2 + 1 - core
    rows = k_raw.shape[0]
    pairs = kv_in.shape[0]
    parts = 2 * pairs
    shared = pairs // 2
    w_rows = w_ref.shape[0] // parts

    barrier = pltpu.get_barrier_semaphore()

    def greet(**there):
        pl.semaphore_signal(barrier, inc=1, device_id=there, device_id_type=MESH)

    greet(sp=sibling)
    greet(dp=x_peer)
    greet(dp=core_peer)
    z_other = jnp.where(inner, z_out, z_in)
    greet(sp=z_other * 2 + y)
    greet(sp=z_other * 2 + 1 - y)

    @pl.when(inner)
    def _():
        greet(sp=across)

    def kv_lanes(side, j):
        return pl.ds(pl.multiple_of((side * pairs + j) * LANES, LANES), LANES)

    first = pl.multiple_of(me * rows, rows)
    loads = [
        pltpu.make_async_copy(k_ref, k_raw, load.at[0]),
        pltpu.make_async_copy(cos_ref.at[pl.ds(first, rows)], cos_in, load.at[1]),
        pltpu.make_async_copy(sin_ref.at[pl.ds(first, rows)], sin_in, load.at[2]),
        pltpu.make_async_copy(kg_ref, k_gain_in, load.at[3]),
        pltpu.make_async_copy(qg_ref, q_gain_in, load.at[4]),
        pltpu.make_async_copy(q_ref, q_raw, load.at[5]),
    ]
    for one in loads:
        one.start()

    def own_values(j):
        return pltpu.make_async_copy(
            v_ref.at[:, kv_lanes(y, j)], kv_in.at[j, mine, 1], v_own.at[j]
        )

    for j in range(pairs):
        own_values(j).start()
    own_w = pltpu.make_async_copy(w_ref, w_all.at[dp], w_local)
    own_w.start()

    def remote(src, dst, sent, got, **there):
        return pltpu.make_async_remote_copy(
            src_ref=src, dst_ref=dst, send_sem=sent, recv_sem=got,
            device_id=there, device_id_type=MESH,
        )

    def k_aside(j, to=None):
        to = mine if to is None else to
        return remote(k_out.at[j], kv_in.at[j, to, 0], k_side.at[j], k_got.at[j], sp=sibling)

    def v_aside(j, to=None):
        to = mine if to is None else to
        return remote(
            v_ref.at[:, kv_lanes(1 - y, j)], kv_in.at[j, to, 1], v_side.at[j], v_got.at[j],
            sp=sibling,
        )

    def q_aside(j, to=None):
        to = mine if to is None else to
        return remote(q_out.at[j], q_in.at[j, to], q_side.at[j], q_got.at[j, to], sp=sibling)

    def kv_upward(j, s):
        return remote(
            kv_in.at[j, s], kv_in.at[j, s], kv_up.at[j, s], kv_got.at[j, s], sp=in_same
        )

    def q_upward(j, s):
        return remote(q_in.at[j, s], q_in.at[j, s], q_up.at[j, s], q_got.at[j, s], sp=in_same)

    def kv_across(j, s):
        return remote(
            kv_in.at[j, s], kv_in.at[j, 4 + s], kv_mid.at[j, s], kv_got.at[j, 4 + s], sp=across
        )

    out_same = z_out * 2 + y

    def kv_downward(j, part):
        at = pl.ds(4 * part, 2 + 2 * part)
        return remote(
            kv_in.at[j, at], kv_in.at[j, at], kv_low.at[j, part], kv_low_got.at[j, part],
            sp=out_same,
        )

    def kv_came(j, s):
        remote(
            kv_in.at[j, s], kv_in.at[j, s], kv_up.at[j, 0], kv_got.at[j, s], sp=across
        ).wait_recv()

    def q_came(j, s):
        remote(q_in.at[j, s], q_in.at[j, s], q_up.at[j, 0], q_got.at[j, s], sp=sibling).wait_recv()

    def w_piece(ref, c):
        return ref.at[pl.ds(pl.multiple_of(c * w_rows, w_rows), w_rows)]

    def w_held(shard, c):
        return w_all.at[shard, pl.ds(pl.multiple_of(c * w_rows, w_rows), w_rows)]

    aside = pairs // 2
    direct = parts - aside

    def part_at(i):
        if i < aside:
            return y * pairs + i
        return (i % 2) * pairs + (aside + i) // 2

    def w_cross(i):
        c = part_at(i)
        return remote(w_piece(w_ref, c), w_held(dp, c), w_x.at[i], w_got.at[dp, c], dp=x_peer)

    def w_own_core():
        return remote(w_ref, w_all.at[dp], w_core.at[parts], w_got.at[dp, parts], dp=core_peer)

    def w_to_core(c):
        return remote(
            w_held(x_peer, c), w_held(x_peer, c), w_core.at[c], w_got.at[x_peer, c], dp=core_peer
        )

    def w_aside(i):
        c = part_at(i)
        return remote(
            w_held(x_peer, c), w_held(x_peer, c), w_y.at[i], w_got.at[x_peer, c], sp=sibling
        )

    def w_came(shard, c):
        remote(
            w_held(shard, c), w_held(shard, c), w_y.at[0], w_got.at[shard, c], dp=core_peer
        ).wait_recv()

    def pass_w(i):
        c = part_at(i)
        w_came(x_peer, c)
        w_to_core(c).start()
        if i < aside:
            w_aside(i).start()

    def pass_w_aside(i):
        c = (1 - y) * pairs + i
        w_came(x_peer, c)
        w_to_core(c).start()

    lane = lax.broadcasted_iota(jnp.int32, (rows, LANES), 1)
    low = lane < HD
    even = (lane // (HD // 4)) % 2 == 0

    def turn(tile, gain):
        u = tile.astype(jnp.float32)
        square = u * u
        sum_low = jnp.sum(jnp.where(low, square, 0.0), axis=1, keepdims=True)
        sum_high = jnp.sum(jnp.where(low, 0.0, square), axis=1, keepdims=True)
        inverse = jnp.where(
            low, lax.rsqrt(sum_low * (1.0 / HD) + epsilon), lax.rsqrt(sum_high * (1.0 / HD) + epsilon)
        )
        normed = u * inverse * gain
        part = HD // 4
        turned = jnp.where(even, pltpu.roll(normed, LANES - part, 1), pltpu.roll(normed, part, 1))
        return normed * cos_in[...] + turned * sin_in[...]

    def crossed(one, two):
        return (
            jnp.where(low, one, pltpu.roll(two, HD, 1)),
            jnp.where(low, pltpu.roll(one, HD, 1), two),
        )

    def turn_keys(j, side):
        return turn(k_raw[:, kv_lanes(side, j)], k_gain).astype(jnp.bfloat16)

    def turn_queries(j, side):
        at = (side * pairs + j) * 2 * LANES
        natural = [
            turn(q_raw[:, pl.ds(pl.multiple_of(at + i * LANES, LANES), LANES)], q_gain)
            for i in range(2)
        ]
        return jnp.concatenate(crossed(*natural), axis=1).astype(jnp.bfloat16)

    for one in loads[:5]:
        one.wait()
    q_gain, k_gain = (
        jnp.concatenate([g[...], g[...]], axis=1) for g in (q_gain_in, k_gain_in)
    )

    def key_step(j):
        k_out[j] = turn_keys(j, 1 - y)
        kv_in[j, mine, 0] = turn_keys(j, y)

    def query_step(j):
        q_out[j] = turn_queries(j, 1 - y)
        q_in[j, mine] = turn_queries(j, y)

    key_step(0)
    pl.semaphore_wait(barrier, jnp.where(inner, 6, 5))

    def key_send(j, carry):
        v_aside(j).start()

        @pl.when(j > 0)
        def _():
            key_step(j)

        k_aside(j).start()
        own_values(j).wait()

        @pl.when(jnp.logical_and(outer, j < 2))
        def _():
            kv_upward(j, mine).start()

        @pl.when(jnp.logical_and(inner, j < 2))
        def _():
            kv_across(j, mine).start()

        return carry

    def query_send(j, carry):
        query_step(j)
        q_aside(j).start()
        return carry

    w_cross(0).start()
    w_cross(1).start()
    lax.fori_loop(0, pairs, key_send, 0)
    loads[5].wait()
    lax.fori_loop(0, pairs, query_send, 0)
    for i in range(2, direct):
        w_cross(i).start()
    w_own_core().start()

    def beside_came(j):
        k_aside(j, beside).wait_recv()
        v_aside(j, beside).wait_recv()

    @pl.when(outer)
    def _():
        def kv(j):
            if j > 1:
                kv_upward(j, mine).start()
            beside_came(j)
            kv_upward(j, beside).start()

        def query(j):
            if j:
                q_upward(j, mine).start()
            q_came(j, beside)
            q_upward(j, beside).start()

        for j in range(pairs):
            kv(j)
        for j in range(shared, pairs):
            query(j)

    scale = HD ** (-0.5) * LOG2E
    step = 2 * LANES
    seq_len = 8 * rows
    near_len = 4 * rows

    def tiles(far):
        start = near_len * far
        stop = start + near_len
        return [(t, min(step, stop - t)) for t in range(start, stop, step)]

    def by_sublane(tile):
        return tile.reshape(tile.shape[0] // 8, 8, tile.shape[1])

    def exponents(j, s, at, far):
        pair = [q_in[j, s, :, g * LANES : (g + 1) * LANES] for g in range(2)]
        zero = jnp.zeros_like(pair[0])
        stack = [jnp.where(low, one, zero) for one in pair]
        stack += [jnp.where(low, zero, one) for one in pair]
        stack = jnp.concatenate(stack, axis=0)
        keys = kv_in[j, 4 * far : 4 * far + 4, 0].reshape(near_len, LANES)
        top = None
        for t, size in tiles(far):
            tile = lax.dot_general(
                keys[t - near_len * far :][:size], stack, TRANSPOSED, preferred_element_type=jnp.float32
            )
            score[at, t : t + size] = tile
            most = jnp.max(by_sublane(tile), axis=0)
            top = most if top is None else jnp.maximum(top, most)
        top = jnp.max(top, axis=0, keepdims=True)

        def finish():
            total = None
            for t, size in tiles(far):
                p = jnp.exp2((score[at, t : t + size] - top) * scale)
                score[at, t : t + size] = p
                more = jnp.sum(by_sublane(p), axis=0)
                total = more if total is None else total + more
            return top, jnp.sum(total, axis=0, keepdims=True)

        return finish

    def staged(j, order, far):
        found = []
        ahead = exponents(j, order[0], 0, far)
        for u in range(len(order)):
            now = ahead
            if u + 1 < len(order):
                ahead = exponents(j, order[u + 1], u + 1, far)
            found.append(now())
        return found

    def weigh(at, near, far):
        top = jnp.maximum(near[0], far[0])
        shrink = [jnp.exp2((one[0] - top) * scale) for one in (near, far)]
        inv = 1.0 / (near[1] * shrink[0] + far[1] * shrink[1])
        o = None
        for side in range(2):
            factor = shrink[side] * inv
            for t, size in tiles(side):
                p = (score[at, t : t + size] * factor).astype(jnp.bfloat16)
                more = jnp.dot(v_turned[:, t : t + size], p, preferred_element_type=jnp.float32)
                o = more if o is None else o + more
        o = o.T
        cut = [o[i * rows : (i + 1) * rows] for i in range(4)]
        one = jnp.where(low, cut[0], pltpu.roll(cut[1], HD, 1))
        two = jnp.where(low, pltpu.roll(cut[2], HD, 1), cut[3])
        return jnp.concatenate([one, two], axis=1).astype(jnp.bfloat16)

    def a_copy(j, s):
        there = jnp.where(s < 2, z_in, z_out) * 2 + s % 2
        c = y * pairs + j
        return remote(a_out.at[j, s], a_in.at[c], a_send.at[j, s], a_got.at[c], sp=there)

    def relay_first(j):
        beside_came(j)
        kv_across(j, beside).start()

        @pl.when(j < shared)
        def _():
            kv_downward(j, 0).start()

        kv_came(j, 2 + y)
        kv_across(j, 2 + y).start()

    def relay_last(j):
        kv_came(j, 3 - y)
        kv_across(j, 3 - y).start()

        @pl.when(j + 3 < pairs)
        def _():
            kv_across(j + 2, mine).start()

    def turn_values(j, far):
        at = slice(near_len * far, near_len * (far + 1))
        v_turned[:, at] = kv_in[j, 4 * far : 4 * far + 4, 1].reshape(near_len, LANES).T

    def attend(j, order, await_far, eager):
        turn_values(j, 0)
        near = staged(j, order, 0)
        await_far()
        turn_values(j, 1)
        ready = exponents(j, order[0], 0, 1)
        for u in range(len(order)):
            far = ready()
            if u + 1 < len(order):
                ready = exponents(j, order[u + 1], u + 1, 1)
            tile = weigh(u, near[u], far)
            if u + 1 < len(order):
                a_out[j, order[u]] = tile
                if eager:
                    a_copy(j, order[u]).start()
            else:
                a_in[y * pairs + j] = tile
        if not eager:
            for s in order[:-1]:
                a_copy(j, s).start()

    def a_came(c):
        remote(a_in.at[c], a_in.at[c], a_send.at[0, 0], a_got.at[c], sp=sibling).wait_recv()

    def a_ready(j):
        a_came((1 - y) * pairs + j)

        if j >= shared:
            @pl.when(outer)
            def _():
                a_came(y * pairs + j)

    width = w_ref.shape[1]

    def project(which, first=False, last=False):
        for shard in range(m):
            at = slice(shard * width, (shard + 1) * width)
            total = None if first else summed[:, at]
            for j in which:
                for c in (j, pairs + j):
                    more = jnp.dot(
                        a_in[c], w_all[shard, c * w_rows : (c + 1) * w_rows, :],
                        preferred_element_type=jnp.float32,
                    )
                    total = more if total is None else total + more
            if last:
                out_ref[:, at] = total.astype(jnp.bfloat16)
            else:
                summed[:, at] = total

    def w_ready(which):
        for j in which:
            for c in (j, pairs + j):
                w_came(x_other, c)

    final = pairs - 1

    def k_across(s):
        return remote(
            kv_in.at[final, s, 0], kv_in.at[final, 4 + s, 0], kv_mid.at[final, s],
            kv_got.at[final, 4 + s], sp=across,
        )

    def v_across(s):
        return remote(
            kv_in.at[final, s, 1], kv_in.at[final, 4 + s, 1], v_mid.at[s], v_far.at[s], sp=across
        )

    def relay(j):
        if j < final:
            relay_first(j)
            relay_last(j)
            return
        k_across(mine).start()
        beside_came(j)
        k_across(beside).start()
        for s in (2 + y, 3 - y):
            kv_came(j, s)
            k_across(s).start()
        for s in (mine, beside, 2 + y, 3 - y):
            v_across(s).start()

    def far_came(j):
        for s in range(4, 8):
            kv_came(j, s)

    @pl.when(inner)
    def _():
        for j in range(shared):
            relay_first(j)
            relay_last(j)

    def shared_pair(j, carry):
        for i in range(pairs - shared):
            @pl.when(jnp.logical_and(inner, j == i))
            def _():
                relay(i + shared)

        @pl.when(outer)
        def _():
            low_came(j, 0)

        for i in range(shared):
            @pl.when(jnp.logical_and(inner, j == i))
            def _():
                pass_w(i)

        @pl.when(inner)
        def _():
            q_came(j, beside)

        def await_far():
            @pl.when(inner)
            def _():
                far_came(j)
                kv_downward(j, 1).start()

            @pl.when(outer)
            def _():
                low_came(j, 1)

        attend(j, [beside, mine], await_far, False)
        return carry

    def low_came(j, part):
        kv_downward(j, part).wait_recv()

    @pl.when(outer)
    def _():
        for j in range(shared):
            q_came(j, beside)
        for i in range(aside + 1):
            pass_w(i)

    lax.fori_loop(0, shared, shared_pair, 0)
    order = [2, 3, 1 - y, y]

    def late_pair(j, eager, await_far=None):
        for s in (1 - y, 2, 3):
            q_came(j, s)
        attend(j, order, await_far or (lambda: far_came(j)), eager)

    early = list(range(pairs - 2))

    def middle_passes():
        for i in range(aside):
            pass_w_aside(i)
        for i in range(aside + 1, direct - 2):
            pass_w(i)
        own_w.wait()
        remote(
            w_ref, w_all.at[core_peer], w_core.at[parts], w_got.at[core_peer, parts], dp=core_peer
        ).wait_recv()

    def early_project():
        w_ready(early)
        for j in early:
            a_ready(j)
        project(early, first=True)
        pass_w(direct - 2)

    @pl.when(inner)
    def _():
        pass_w(aside)
        for j in range(shared, pairs - 1):
            late_pair(j, False)
        middle_passes()

        for s in (1 - y, 2, 3):
            q_came(final, s)
        turn_values(final, 0)
        near = staged(final, order, 0)
        early_project()
        for s in range(4):
            k_across(s).wait_recv()
        far = staged(final, order, 1)
        for s in range(4):
            v_across(s).wait_recv()
        turn_values(final, 1)
        for u in range(4):
            tile = weigh(u, near[u], far[u])
            if u < 3:
                a_out[final, order[u]] = tile
                a_copy(final, order[u]).start()
            else:
                a_in[y * pairs + final] = tile

    @pl.when(outer)
    def _():
        middle_passes()
        early_project()

    pass_w(direct - 1)
    w_ready([pairs - 2])
    a_ready(pairs - 2)
    project([pairs - 2])
    w_ready([pairs - 1])
    a_ready(pairs - 1)
    project([pairs - 1], last=True)

    def sent(j, carry):
        k_aside(j).wait_send()
        v_aside(j).wait_send()
        q_aside(j).wait_send()

        @pl.when(outer)
        def _():
            for s in (mine, beside):
                kv_upward(j, s).wait_send()

                @pl.when(j >= shared)
                def _():
                    q_upward(j, s).wait_send()

        @pl.when(inner)
        def _():
            @pl.when(j < pairs - 1)
            def _():
                for s in range(4):
                    kv_across(j, s).wait_send()

            @pl.when(j < shared)
            def _():
                for part in range(2):
                    kv_downward(j, part).wait_send()

            @pl.when(j >= shared)
            def _():
                for s in (2, 3):
                    a_copy(j, s).wait_send()

        @pl.when(jnp.logical_or(inner, j < shared))
        def _():
            a_copy(j, beside).wait_send()

        return carry

    lax.fori_loop(0, pairs, sent, 0)

    @pl.when(inner)
    def _():
        for s in range(4):
            k_across(s).wait_send()
            v_across(s).wait_send()

    for i in range(direct):
        w_cross(i).wait_send()
    for i in range(aside):
        w_aside(i).wait_send()
    for c in range(parts):
        w_to_core(c).wait_send()
    w_own_core().wait_send()


def rotary_lanes(row_count):
    position = np.arange(row_count)[:, None]
    lane = np.arange(LANES)[None, :]
    place = np.where(lane % HD < HD // 2, position // GRID_W, position % GRID_W).astype(np.float32)
    quarter = HD // 4
    step = (lane % quarter).astype(np.float32)
    inv_freq = np.power(np.float32(rotary_base), -(np.float32(2.0) * step) / np.float32(HD // 2))
    angle = inv_freq.astype(np.float32) * place
    sign = np.where((lane // quarter) % 2 == 0, np.float32(-1.0), np.float32(1.0))
    return np.cos(angle).astype(np.float32), (np.sin(angle) * sign).astype(np.float32)


def on_device(queries, keys, values, q_gain, k_gain, w_out):
    n, m = lax.axis_size("sp"), lax.axis_size("dp")
    rows = queries.shape[2]
    kv_width = keys.shape[1] // 2
    pairs = kv_width // LANES
    if n != 8 or m != 4 or kv_width % LANES or pairs != 4 or rows % 32 or QH != 2 * KV:
        return on_device_plain(queries, keys, values, q_gain, k_gain, w_out)
    seq_len = n * rows
    cos_table, sin_table = rotary_lanes(seq_len)
    hbm = pl.BlockSpec(memory_space=pltpu.HBM)
    bf16, f32 = jnp.bfloat16, jnp.float32
    dma = pltpu.SemaphoreType.DMA
    parts = 2 * pairs
    mixed = pl.pallas_call(
        functools.partial(layer_kernel, m),
        out_shape=jax.ShapeDtypeStruct((rows, w_out.shape[1] * m), bf16),
        in_specs=[hbm] * 8,
        out_specs=pl.BlockSpec(memory_space=pltpu.VMEM),
        scratch_shapes=[
            pltpu.VMEM((rows, queries.shape[1]), bf16),
            pltpu.VMEM((rows, keys.shape[1]), bf16),
            pltpu.VMEM((1, HD), f32),
            pltpu.VMEM((1, HD), f32),
            pltpu.VMEM((rows, LANES), f32),
            pltpu.VMEM((rows, LANES), f32),
            pltpu.VMEM((pairs, rows, LANES), bf16),
            pltpu.VMEM((pairs, rows, 2 * LANES), bf16),
            pltpu.VMEM((pairs, 8, 2, rows, LANES), bf16),
            pltpu.VMEM((pairs, 4, rows, 2 * LANES), bf16),
            pltpu.VMEM((pairs, 4, rows, 2 * LANES), bf16),
            pltpu.VMEM((parts, rows, 2 * LANES), bf16),
            pltpu.VMEM((m, w_out.shape[0], w_out.shape[1]), bf16),
            pltpu.VMEM((4, seq_len, 4 * rows), f32),
            pltpu.VMEM((LANES, seq_len), bf16),
            pltpu.VMEM((rows, w_out.shape[1] * m), f32),
            dma((6,)), dma((pairs,)), dma((pairs,)), dma((pairs,)), dma((pairs,)),
            dma((pairs,)), dma((pairs,)), dma((pairs, 4)), dma((pairs, 4)), dma((pairs, 4)),
            dma((pairs, 4)), dma((pairs, 8)), dma((pairs, 2)), dma((pairs, 2)), dma((4,)), dma((4,)), dma((pairs, 4)),
            dma((parts,)),
            dma((parts,)), dma((pairs,)), dma((parts + 1,)), dma((m, parts + 1)), dma,
        ],
        compiler_params=pltpu.CompilerParams(
            collective_id=0, has_side_effects=True, vmem_limit_bytes=44 * 1024 * 1024
        ),
    )(
        *(
            pltpu.with_memory_space_constraint(x, pltpu.HBM)
            for x in (
                queries[0].T, keys[0].T, values[0].T, q_gain[None], k_gain[None],
                jnp.asarray(cos_table), jnp.asarray(sin_table), w_out,
            )
        )
    )
    return mixed[None]


def solution(mesh):
    placed = (
        P("dp", None, "sp"),
        P("dp", None, "sp"),
        P("dp", None, "sp"),
        P(),
        P(),
        P(None, "dp"),
    )
    return jax.shard_map(
        on_device, mesh=mesh, in_specs=placed, out_specs=P("dp", "sp", None), check_vma=False
    )
```

```python
import functools

import jax
import jax.numpy as jnp
import numpy as np
from jax import lax
from jax.experimental import pallas as pl
from jax.experimental.pallas import tpu as pltpu
from jax.sharding import PartitionSpec as P

HD = 64
QH = 32
KV = 16
GRID_W = 64


epsilon = 1e-06
rotary_base = 10000.0
block_count = 8


def swapped(block, axis, apart):
    count = lax.axis_size(axis)
    route = []
    for low in range(count):
        high = low | 1 << apart
        if high != low and high < count:
            route += [(low, high), (high, low)]
    return lax.ppermute(block, axis, route)


def rotary_tables(first_row, row_count):
    position = first_row + lax.iota(jnp.int32, row_count)
    grid_row = (position // GRID_W).astype(jnp.float32)
    grid_col = (position % GRID_W).astype(jnp.float32)
    quarter = HD // 4
    inv_freq = rotary_base ** (-(2.0 * lax.iota(jnp.float32, quarter)) / (HD // 2))
    row_angle = inv_freq[:, None] * grid_row[None, :]
    col_angle = inv_freq[:, None] * grid_col[None, :]
    cos_table = jnp.concatenate(
        [jnp.cos(row_angle), jnp.cos(row_angle), jnp.cos(col_angle), jnp.cos(col_angle)], axis=0
    )
    sin_table = jnp.concatenate(
        [jnp.sin(row_angle), jnp.sin(row_angle), jnp.sin(col_angle), jnp.sin(col_angle)], axis=0
    )
    return (cos_table, sin_table)


def normalize_turn(field, gain, cos_table, sin_table):
    head_count = field.shape[0] // HD
    values_f = field.astype(jnp.float32).reshape(head_count, HD, field.shape[1])
    normed = (
        values_f
        * lax.rsqrt(jnp.mean(values_f * values_f, axis=1, keepdims=True) + epsilon)
        * gain[None, :, None]
    )
    quarter = HD // 4
    quarters_of = normed.reshape(head_count, 4, quarter, field.shape[1])
    turned = jnp.concatenate(
        [-quarters_of[:, 1], quarters_of[:, 0], -quarters_of[:, 3], quarters_of[:, 2]], axis=1
    )
    return (normed * cos_table[None] + turned * sin_table[None]).astype(jnp.bfloat16)


def attention_heads(query_heads, key_heads, value_heads, seq_len):
    kv_local = key_heads.shape[0]
    group_local = query_heads.shape[0] // kv_local
    query_split = query_heads.reshape(kv_local, group_local, HD, seq_len)
    score_scale = HD ** (-0.5)
    block_rows = seq_len // block_count

    def one_block(block_index, result):
        row_start = block_index * block_rows
        query_block = lax.dynamic_slice_in_dim(query_split, row_start, block_rows, 3)
        scores = (
            jnp.einsum("hgdq,hdk->hgqk", query_block, key_heads, preferred_element_type=jnp.float32)
            * score_scale
        )
        row_max = jnp.max(scores, axis=-1, keepdims=True)
        weights = jnp.exp(scores - row_max)
        weights = (weights / jnp.sum(weights, axis=-1, keepdims=True)).astype(jnp.bfloat16)
        attended = jnp.einsum(
            "hgqk,hdk->hgdq", weights, value_heads, preferred_element_type=jnp.float32
        )
        return lax.dynamic_update_slice_in_dim(result, attended.astype(jnp.bfloat16), row_start, 3)

    result = jnp.zeros(query_split.shape, jnp.bfloat16)
    result = lax.fori_loop(0, block_count, one_block, result)
    return result.reshape(query_heads.shape)


def on_device_plain(queries, keys, values, q_gain, k_gain, w_out):
    sp_count = lax.axis_size("sp")
    tok_rows = queries.shape[2]
    seq_len = tok_rows * sp_count
    cos_table, sin_table = rotary_tables(lax.axis_index("sp") * tok_rows, tok_rows)
    query_rot = normalize_turn(queries[0], q_gain, cos_table, sin_table)
    key_rot = normalize_turn(keys[0], k_gain, cos_table, sin_table)
    value_rows = values[0].reshape(KV, HD, tok_rows)
    query_heads = lax.all_to_all(query_rot, "sp", split_axis=0, concat_axis=2, tiled=True)
    share_count = max(sp_count // KV, 1)
    part_rows = tok_rows // share_count
    key_cut = (
        key_rot.reshape(KV, HD, share_count, part_rows)
        .transpose(0, 2, 1, 3)
        .reshape(KV * share_count, HD, part_rows)
    )
    value_cut = (
        value_rows.reshape(KV, HD, share_count, part_rows)
        .transpose(0, 2, 1, 3)
        .reshape(KV * share_count, HD, part_rows)
    )
    key_got, value_got = (
        lax.all_to_all(key_cut, "sp", split_axis=0, concat_axis=2, tiled=True),
        lax.all_to_all(value_cut, "sp", split_axis=0, concat_axis=2, tiled=True),
    )
    kv_local = key_got.shape[0]
    key_got = key_got.reshape(kv_local, HD, sp_count, part_rows)
    value_got = value_got.reshape(kv_local, HD, sp_count, part_rows)
    for bit_index in range(share_count.bit_length() - 1):
        key_other, value_other = swapped((key_got, value_got), "sp", bit_index)
        key_got = jnp.concatenate([key_got, key_other], axis=3)
        value_got = jnp.concatenate([value_got, value_other], axis=3)
    key_heads = key_got.reshape(kv_local, HD, seq_len)
    value_heads = value_got.reshape(kv_local, HD, seq_len)
    attended = attention_heads(query_heads, key_heads, value_heads, seq_len)
    token_heads = lax.all_to_all(attended, "sp", split_axis=2, concat_axis=0, tiled=True)
    token_rows = token_heads.reshape(QH * HD, tok_rows)
    product = lax.dot_general(
        token_rows,
        lax.all_gather(w_out, "dp", axis=1, tiled=True),
        (((0,), (0,)), ((), ())),
        preferred_element_type=jnp.float32,
    )
    mixed_rows = product.astype(jnp.bfloat16)
    return mixed_rows[None]


MESH = pl.DeviceIdType.MESH
LOG2E = 1.4426950408889634
LANES = 128
TRANSPOSED = (((1,), (1,)), ((), ()))


def layer_kernel(
    m, q_ref, k_ref, v_ref, qg_ref, kg_ref, cos_ref, sin_ref, w_ref, out_ref,
    q_raw, k_raw, q_gain_in, k_gain_in, cos_in, sin_in, k_out, q_out, kv_in, q_in, a_out, a_in,
    w_all, score, v_turned, summed,
    load, v_own, k_side, v_side, q_side, k_got, v_got, q_got, kv_up, q_up, kv_mid, kv_got, kv_low, kv_low_got,
    a_send, a_got, w_x, w_y, w_core, w_got, w_local,
):
    me = lax.axis_index("sp")
    dp = lax.axis_index("dp")
    z, y = me // 2, me % 2
    half = z // 2
    z_in, z_out = 1 + half, 3 * half
    inner = z == z_in
    outer = jnp.logical_not(inner)
    base = jnp.where(inner, 0, 2)
    mine, beside = base + y, base + 1 - y
    sibling = z * 2 + 1 - y
    in_same = z_in * 2 + y
    across = (3 - z_in) * 2 + y
    core = lax.rem(dp, 2)
    x_at = dp // 2
    x_peer = (1 - x_at) * 2 + core
    core_peer = x_at * 2 + 1 - core
    x_other = (1 - x_at) * 2 + 1 - core
    rows = k_raw.shape[0]
    pairs = kv_in.shape[0]
    parts = 2 * pairs
    shared = pairs // 2
    w_rows = w_ref.shape[0] // parts

    barrier = pltpu.get_barrier_semaphore()

    def greet(**there):
        pl.semaphore_signal(barrier, inc=1, device_id=there, device_id_type=MESH)

    greet(sp=sibling)
    greet(dp=x_peer)
    greet(dp=core_peer)
    z_other = jnp.where(inner, z_out, z_in)
    greet(sp=z_other * 2 + y)
    greet(sp=z_other * 2 + 1 - y)

    @pl.when(inner)
    def _():
        greet(sp=across)

    def kv_lanes(side, j):
        return pl.ds(pl.multiple_of((side * pairs + j) * LANES, LANES), LANES)

    first = pl.multiple_of(me * rows, rows)
    loads = [
        pltpu.make_async_copy(k_ref, k_raw, load.at[0]),
        pltpu.make_async_copy(cos_ref.at[pl.ds(first, rows)], cos_in, load.at[1]),
        pltpu.make_async_copy(sin_ref.at[pl.ds(first, rows)], sin_in, load.at[2]),
        pltpu.make_async_copy(kg_ref, k_gain_in, load.at[3]),
        pltpu.make_async_copy(qg_ref, q_gain_in, load.at[4]),
        pltpu.make_async_copy(q_ref, q_raw, load.at[5]),
    ]
    for one in loads:
        one.start()

    def own_values(j):
        return pltpu.make_async_copy(
            v_ref.at[:, kv_lanes(y, j)], kv_in.at[j, mine, 1], v_own.at[j]
        )

    for j in range(pairs):
        own_values(j).start()
    own_w = pltpu.make_async_copy(w_ref, w_all.at[dp], w_local)

    def remote(src, dst, sent, got, **there):
        return pltpu.make_async_remote_copy(
            src_ref=src, dst_ref=dst, send_sem=sent, recv_sem=got,
            device_id=there, device_id_type=MESH,
        )

    def k_aside(j, to=None):
        to = mine if to is None else to
        return remote(k_out.at[j], kv_in.at[j, to, 0], k_side.at[j], k_got.at[j], sp=sibling)

    def v_aside(j, to=None):
        to = mine if to is None else to
        return remote(
            v_ref.at[:, kv_lanes(1 - y, j)], kv_in.at[j, to, 1], v_side.at[j], v_got.at[j],
            sp=sibling,
        )

    def q_aside(j, to=None):
        to = mine if to is None else to
        return remote(q_out.at[j], q_in.at[j, to], q_side.at[j], q_got.at[j, to], sp=sibling)

    def kv_upward(j, s):
        return remote(
            kv_in.at[j, s], kv_in.at[j, s], kv_up.at[j, s], kv_got.at[j, s], sp=in_same
        )

    def q_upward(j, s):
        return remote(q_in.at[j, s], q_in.at[j, s], q_up.at[j, s], q_got.at[j, s], sp=in_same)

    def kv_across(j, s):
        return remote(
            kv_in.at[j, s], kv_in.at[j, 4 + s], kv_mid.at[j, s], kv_got.at[j, 4 + s], sp=across
        )

    out_same = z_out * 2 + y

    def kv_downward(j, part):
        at = pl.ds(4 * part, 2 + 2 * part)
        return remote(
            kv_in.at[j, at], kv_in.at[j, at], kv_low.at[j, part], kv_low_got.at[j, part],
            sp=out_same,
        )

    def kv_came(j, s):
        remote(
            kv_in.at[j, s], kv_in.at[j, s], kv_up.at[j, 0], kv_got.at[j, s], sp=across
        ).wait_recv()

    def q_came(j, s):
        remote(q_in.at[j, s], q_in.at[j, s], q_up.at[j, 0], q_got.at[j, s], sp=sibling).wait_recv()

    def w_piece(ref, c):
        return ref.at[pl.ds(pl.multiple_of(c * w_rows, w_rows), w_rows)]

    def w_held(shard, c):
        return w_all.at[shard, pl.ds(pl.multiple_of(c * w_rows, w_rows), w_rows)]

    aside = pairs // 2
    direct = parts - aside

    def part_at(i):
        if i < aside:
            return y * pairs + i
        return (i % 2) * pairs + (aside + i) // 2

    def w_cross(i):
        c = part_at(i)
        return remote(w_piece(w_ref, c), w_held(dp, c), w_x.at[i], w_got.at[dp, c], dp=x_peer)

    def w_own_core():
        return remote(w_ref, w_all.at[dp], w_core.at[parts], w_got.at[dp, parts], dp=core_peer)

    def w_to_core(c):
        return remote(
            w_held(x_peer, c), w_held(x_peer, c), w_core.at[c], w_got.at[x_peer, c], dp=core_peer
        )

    def w_aside(i):
        c = part_at(i)
        return remote(
            w_held(x_peer, c), w_held(x_peer, c), w_y.at[i], w_got.at[x_peer, c], sp=sibling
        )

    def w_came(shard, c):
        remote(
            w_held(shard, c), w_held(shard, c), w_y.at[0], w_got.at[shard, c], dp=core_peer
        ).wait_recv()

    def pass_w(i):
        c = part_at(i)
        w_came(x_peer, c)
        w_to_core(c).start()
        if i < aside:
            w_aside(i).start()

    def pass_w_aside(i):
        c = (1 - y) * pairs + i
        w_came(x_peer, c)
        w_to_core(c).start()

    lane = lax.broadcasted_iota(jnp.int32, (rows, LANES), 1)
    low = lane < HD
    even = (lane // (HD // 4)) % 2 == 0

    def turn(tile, gain):
        u = tile.astype(jnp.float32)
        square = u * u
        sum_low = jnp.sum(jnp.where(low, square, 0.0), axis=1, keepdims=True)
        sum_high = jnp.sum(jnp.where(low, 0.0, square), axis=1, keepdims=True)
        inverse = jnp.where(
            low, lax.rsqrt(sum_low * (1.0 / HD) + epsilon), lax.rsqrt(sum_high * (1.0 / HD) + epsilon)
        )
        normed = u * inverse * gain
        part = HD // 4
        turned = jnp.where(even, pltpu.roll(normed, LANES - part, 1), pltpu.roll(normed, part, 1))
        return normed * cos_in[...] + turned * sin_in[...]

    def crossed(one, two):
        return (
            jnp.where(low, one, pltpu.roll(two, HD, 1)),
            jnp.where(low, pltpu.roll(one, HD, 1), two),
        )

    def turn_keys(j, side):
        return turn(k_raw[:, kv_lanes(side, j)], k_gain).astype(jnp.bfloat16)

    def turn_queries(j, side):
        at = (side * pairs + j) * 2 * LANES
        natural = [
            turn(q_raw[:, pl.ds(pl.multiple_of(at + i * LANES, LANES), LANES)], q_gain)
            for i in range(2)
        ]
        return jnp.concatenate(crossed(*natural), axis=1).astype(jnp.bfloat16)

    for one in loads[:5]:
        one.wait()
    q_gain, k_gain = (
        jnp.concatenate([g[...], g[...]], axis=1) for g in (q_gain_in, k_gain_in)
    )

    def key_step(j):
        k_out[j] = turn_keys(j, 1 - y)
        kv_in[j, mine, 0] = turn_keys(j, y)

    def query_step(j):
        q_out[j] = turn_queries(j, 1 - y)
        q_in[j, mine] = turn_queries(j, y)

    key_step(0)
    pl.semaphore_wait(barrier, jnp.where(inner, 6, 5))

    def key_send(j, carry):
        v_aside(j).start()

        @pl.when(j > 0)
        def _():
            key_step(j)

        k_aside(j).start()
        own_values(j).wait()

        @pl.when(jnp.logical_and(outer, j < 2))
        def _():
            kv_upward(j, mine).start()

        @pl.when(jnp.logical_and(inner, j < 2))
        def _():
            kv_across(j, mine).start()

        return carry

    def query_send(j, carry):
        query_step(j)
        q_aside(j).start()
        return carry

    w_cross(0).start()
    w_cross(1).start()
    lax.fori_loop(0, pairs, key_send, 0)
    loads[5].wait()
    lax.fori_loop(0, pairs, query_send, 0)
    for i in range(2, direct):
        w_cross(i).start()
    own_w.start()
    w_own_core().start()

    def beside_came(j):
        k_aside(j, beside).wait_recv()
        v_aside(j, beside).wait_recv()

    @pl.when(outer)
    def _():
        def kv(j):
            if j > 1:
                kv_upward(j, mine).start()
            beside_came(j)
            kv_upward(j, beside).start()

        def query(j):
            if j:
                q_upward(j, mine).start()
            q_came(j, beside)
            q_upward(j, beside).start()

        for j in range(pairs):
            kv(j)
        for j in range(shared, pairs):
            query(j)

    scale = HD ** (-0.5) * LOG2E
    step = 2 * LANES
    seq_len = 8 * rows
    near_len = 4 * rows

    def tiles(far):
        start = near_len * far
        stop = start + near_len
        return [(t, min(step, stop - t)) for t in range(start, stop, step)]

    def by_sublane(tile):
        return tile.reshape(tile.shape[0] // 8, 8, tile.shape[1])

    def exponents(j, s, at, far):
        pair = [q_in[j, s, :, g * LANES : (g + 1) * LANES] for g in range(2)]
        zero = jnp.zeros_like(pair[0])
        stack = [jnp.where(low, one, zero) for one in pair]
        stack += [jnp.where(low, zero, one) for one in pair]
        stack = jnp.concatenate(stack, axis=0)
        keys = kv_in[j, 4 * far : 4 * far + 4, 0].reshape(near_len, LANES)
        top = None
        for t, size in tiles(far):
            tile = lax.dot_general(
                keys[t - near_len * far :][:size], stack, TRANSPOSED, preferred_element_type=jnp.float32
            )
            score[at, t : t + size] = tile
            most = jnp.max(by_sublane(tile), axis=0)
            top = most if top is None else jnp.maximum(top, most)
        top = jnp.max(top, axis=0, keepdims=True)

        def finish():
            total = None
            for t, size in tiles(far):
                p = jnp.exp2((score[at, t : t + size] - top) * scale)
                score[at, t : t + size] = p
                more = jnp.sum(by_sublane(p), axis=0)
                total = more if total is None else total + more
            return top, jnp.sum(total, axis=0, keepdims=True)

        return finish

    def staged(j, order, far):
        found = []
        ahead = exponents(j, order[0], 0, far)
        for u in range(len(order)):
            now = ahead
            if u + 1 < len(order):
                ahead = exponents(j, order[u + 1], u + 1, far)
            found.append(now())
        return found

    def weigh(at, near, far):
        top = jnp.maximum(near[0], far[0])
        shrink = [jnp.exp2((one[0] - top) * scale) for one in (near, far)]
        inv = 1.0 / (near[1] * shrink[0] + far[1] * shrink[1])
        o = None
        for side in range(2):
            factor = shrink[side] * inv
            for t, size in tiles(side):
                p = (score[at, t : t + size] * factor).astype(jnp.bfloat16)
                more = jnp.dot(v_turned[:, t : t + size], p, preferred_element_type=jnp.float32)
                o = more if o is None else o + more
        o = o.T
        cut = [o[i * rows : (i + 1) * rows] for i in range(4)]
        one = jnp.where(low, cut[0], pltpu.roll(cut[1], HD, 1))
        two = jnp.where(low, pltpu.roll(cut[2], HD, 1), cut[3])
        return jnp.concatenate([one, two], axis=1).astype(jnp.bfloat16)

    def a_copy(j, s):
        there = jnp.where(s < 2, z_in, z_out) * 2 + s % 2
        c = y * pairs + j
        return remote(a_out.at[j, s], a_in.at[c], a_send.at[j, s], a_got.at[c], sp=there)

    def relay_first(j):
        @pl.when(j == pairs - 1)
        def _():
            kv_across(j, mine).start()

        beside_came(j)
        kv_across(j, beside).start()

        @pl.when(j < shared)
        def _():
            kv_downward(j, 0).start()

        kv_came(j, 2 + y)
        kv_across(j, 2 + y).start()

    def relay_last(j):
        kv_came(j, 3 - y)
        kv_across(j, 3 - y).start()

        @pl.when(j + 3 < pairs)
        def _():
            kv_across(j + 2, mine).start()

    def turn_values(j, far):
        at = slice(near_len * far, near_len * (far + 1))
        v_turned[:, at] = kv_in[j, 4 * far : 4 * far + 4, 1].reshape(near_len, LANES).T

    def attend(j, order, await_far, eager):
        turn_values(j, 0)
        near = staged(j, order, 0)
        await_far()
        turn_values(j, 1)
        ready = exponents(j, order[0], 0, 1)
        for u in range(len(order)):
            far = ready()
            if u + 1 < len(order):
                ready = exponents(j, order[u + 1], u + 1, 1)
            tile = weigh(u, near[u], far)
            if u + 1 < len(order):
                a_out[j, order[u]] = tile
                if eager:
                    a_copy(j, order[u]).start()
            else:
                a_in[y * pairs + j] = tile
        if not eager:
            for s in order[:-1]:
                a_copy(j, s).start()

    def a_came(c):
        remote(a_in.at[c], a_in.at[c], a_send.at[0, 0], a_got.at[c], sp=sibling).wait_recv()

    def a_ready(j):
        a_came((1 - y) * pairs + j)

        if j >= shared:
            @pl.when(outer)
            def _():
                a_came(y * pairs + j)

    width = w_ref.shape[1]

    def project(which, first=False, last=False):
        for shard in range(m):
            at = slice(shard * width, (shard + 1) * width)
            total = None if first else summed[:, at]
            for j in which:
                for c in (j, pairs + j):
                    more = jnp.dot(
                        a_in[c], w_all[shard, c * w_rows : (c + 1) * w_rows, :],
                        preferred_element_type=jnp.float32,
                    )
                    total = more if total is None else total + more
            if last:
                out_ref[:, at] = total.astype(jnp.bfloat16)
            else:
                summed[:, at] = total

    def w_ready(which):
        for j in which:
            for c in (j, pairs + j):
                w_came(x_other, c)

    def far_came(j):
        for s in range(4, 8):
            kv_came(j, s)

    @pl.when(inner)
    def _():
        for j in range(shared):
            relay_first(j)
            relay_last(j)

    def shared_pair(j, carry):
        @pl.when(inner)
        def _():
            @pl.when(j + shared < pairs)
            def _():
                relay_first(j + shared)
                relay_last(j + shared)

        @pl.when(outer)
        def _():
            low_came(j, 0)

        for i in range(shared):
            @pl.when(jnp.logical_and(inner, j == i))
            def _():
                pass_w(i)

        @pl.when(inner)
        def _():
            q_came(j, beside)

        def await_far():
            @pl.when(inner)
            def _():
                far_came(j)
                kv_downward(j, 1).start()

            @pl.when(outer)
            def _():
                low_came(j, 1)

        attend(j, [beside, mine], await_far, False)
        return carry

    def low_came(j, part):
        kv_downward(j, part).wait_recv()

    @pl.when(outer)
    def _():
        for j in range(shared):
            q_came(j, beside)
        for i in range(aside + 1):
            pass_w(i)

    lax.fori_loop(0, shared, shared_pair, 0)
    order = [2, 3, 1 - y, y]

    def late_pair(j, eager, await_far=None):
        for s in (1 - y, 2, 3):
            q_came(j, s)
        attend(j, order, await_far or (lambda: far_came(j)), eager)

    early = list(range(pairs - 2))

    def middle_passes():
        for i in range(aside):
            pass_w_aside(i)
        for i in range(aside + 1, direct - 2):
            pass_w(i)
        own_w.wait()
        remote(
            w_ref, w_all.at[core_peer], w_core.at[parts], w_got.at[core_peer, parts], dp=core_peer
        ).wait_recv()

    def early_project():
        w_ready(early)
        for j in early:
            a_ready(j)
        project(early, first=True)
        pass_w(direct - 2)

    @pl.when(inner)
    def _():
        pass_w(aside)
        for j in range(shared, pairs - 1):
            late_pair(j, False)
        middle_passes()

        def await_last():
            early_project()
            far_came(pairs - 1)

        late_pair(pairs - 1, True, await_last)

    @pl.when(outer)
    def _():
        middle_passes()
        early_project()

    pass_w(direct - 1)
    w_ready([pairs - 2])
    a_ready(pairs - 2)
    project([pairs - 2])
    w_ready([pairs - 1])
    a_ready(pairs - 1)
    project([pairs - 1], last=True)

    def sent(j, carry):
        k_aside(j).wait_send()
        v_aside(j).wait_send()
        q_aside(j).wait_send()

        @pl.when(outer)
        def _():
            for s in (mine, beside):
                kv_upward(j, s).wait_send()

                @pl.when(j >= shared)
                def _():
                    q_upward(j, s).wait_send()

        @pl.when(inner)
        def _():
            for s in range(4):
                kv_across(j, s).wait_send()

            @pl.when(j < shared)
            def _():
                for part in range(2):
                    kv_downward(j, part).wait_send()

            @pl.when(j >= shared)
            def _():
                for s in (2, 3):
                    a_copy(j, s).wait_send()

        @pl.when(jnp.logical_or(inner, j < shared))
        def _():
            a_copy(j, beside).wait_send()

        return carry

    lax.fori_loop(0, pairs, sent, 0)
    for i in range(direct):
        w_cross(i).wait_send()
    for i in range(aside):
        w_aside(i).wait_send()
    for c in range(parts):
        w_to_core(c).wait_send()
    w_own_core().wait_send()


def rotary_lanes(row_count):
    position = np.arange(row_count)[:, None]
    lane = np.arange(LANES)[None, :]
    place = np.where(lane % HD < HD // 2, position // GRID_W, position % GRID_W).astype(np.float32)
    quarter = HD // 4
    step = (lane % quarter).astype(np.float32)
    inv_freq = np.power(np.float32(rotary_base), -(np.float32(2.0) * step) / np.float32(HD // 2))
    angle = inv_freq.astype(np.float32) * place
    sign = np.where((lane // quarter) % 2 == 0, np.float32(-1.0), np.float32(1.0))
    return np.cos(angle).astype(np.float32), (np.sin(angle) * sign).astype(np.float32)


def on_device(queries, keys, values, q_gain, k_gain, w_out):
    n, m = lax.axis_size("sp"), lax.axis_size("dp")
    rows = queries.shape[2]
    kv_width = keys.shape[1] // 2
    pairs = kv_width // LANES
    if n != 8 or m != 4 or kv_width % LANES or pairs < 4 or rows % 32 or QH != 2 * KV:
        return on_device_plain(queries, keys, values, q_gain, k_gain, w_out)
    seq_len = n * rows
    cos_table, sin_table = rotary_lanes(seq_len)
    hbm = pl.BlockSpec(memory_space=pltpu.HBM)
    bf16, f32 = jnp.bfloat16, jnp.float32
    dma = pltpu.SemaphoreType.DMA
    parts = 2 * pairs
    mixed = pl.pallas_call(
        functools.partial(layer_kernel, m),
        out_shape=jax.ShapeDtypeStruct((rows, w_out.shape[1] * m), bf16),
        in_specs=[hbm] * 8,
        out_specs=pl.BlockSpec(memory_space=pltpu.VMEM),
        scratch_shapes=[
            pltpu.VMEM((rows, queries.shape[1]), bf16),
            pltpu.VMEM((rows, keys.shape[1]), bf16),
            pltpu.VMEM((1, HD), f32),
            pltpu.VMEM((1, HD), f32),
            pltpu.VMEM((rows, LANES), f32),
            pltpu.VMEM((rows, LANES), f32),
            pltpu.VMEM((pairs, rows, LANES), bf16),
            pltpu.VMEM((pairs, rows, 2 * LANES), bf16),
            pltpu.VMEM((pairs, 8, 2, rows, LANES), bf16),
            pltpu.VMEM((pairs, 4, rows, 2 * LANES), bf16),
            pltpu.VMEM((pairs, 4, rows, 2 * LANES), bf16),
            pltpu.VMEM((parts, rows, 2 * LANES), bf16),
            pltpu.VMEM((m, w_out.shape[0], w_out.shape[1]), bf16),
            pltpu.VMEM((4, seq_len, 4 * rows), f32),
            pltpu.VMEM((LANES, seq_len), bf16),
            pltpu.VMEM((rows, w_out.shape[1] * m), f32),
            dma((6,)), dma((pairs,)), dma((pairs,)), dma((pairs,)), dma((pairs,)),
            dma((pairs,)), dma((pairs,)), dma((pairs, 4)), dma((pairs, 4)), dma((pairs, 4)),
            dma((pairs, 4)), dma((pairs, 8)), dma((pairs, 2)), dma((pairs, 2)), dma((pairs, 4)),
            dma((parts,)),
            dma((parts,)), dma((pairs,)), dma((parts + 1,)), dma((m, parts + 1)), dma,
        ],
        compiler_params=pltpu.CompilerParams(
            collective_id=0, has_side_effects=True, vmem_limit_bytes=44 * 1024 * 1024
        ),
    )(
        *(
            pltpu.with_memory_space_constraint(x, pltpu.HBM)
            for x in (
                queries[0].T, keys[0].T, values[0].T, q_gain[None], k_gain[None],
                jnp.asarray(cos_table), jnp.asarray(sin_table), w_out,
            )
        )
    )
    return mixed[None]


def solution(mesh):
    placed = (
        P("dp", None, "sp"),
        P("dp", None, "sp"),
        P("dp", None, "sp"),
        P(),
        P(),
        P(None, "dp"),
    )
    return jax.shard_map(
        on_device, mesh=mesh, in_specs=placed, out_specs=P("dp", "sp", None), check_vma=False
    )
```
